128 devices in a mesh: sp: 16 (over z, x), tp: 8 (over y, core).
Axes of the slice: x: 4, y: 4, z: 4, core: 2. Of those that a mesh axis runs over, the one named last changes fastest.
Arguments:
- queries: bfloat16 [8192, 2048], P('sp', 'tp'), may hold values from -4.5 to 4.5
- keys: bfloat16 [8192, 2048], P('sp', 'tp'), may hold values from -4.5 to 4.5
- values: bfloat16 [8192, 2048], P('sp', 'tp'), may hold values from -6 to 6
- forget_logits: float32 [8192, 16], P('sp', 'tp'), may hold values from -1 to 20
- layer_input: bfloat16 [8192, 4096], P('sp', 'tp'), may hold values from -0.09375 to 0.09375
- out_grad: bfloat16 [8192, 2048], P('sp', 'tp'), may hold values from -6 to 6
Outputs:
- query_grad: float32 [8192, 2048], P('sp', 'tp')
- key_grad: float32 [8192, 2048], P('sp', 'tp')
- value_grad: float32 [8192, 2048], P('sp', 'tp')
- weight_grad: float32 [4096, 2048], P('sp', 'tp')
The draws below stay inside these ranges and needn't reach their ends.
All inputs are finite; a program needn't handle non-finite values.
Results may differ from the reference program's by a relative error of at most 0.04.
Values may be sent and summed in bfloat16 or wider, within the bound.
A program may use at most 64 MiB of HBM per device.

```python
import math
import jax
import jax.numpy as jnp
from jax import lax

DMODEL = 4096
HEADS = 16
HEAD = 128
TOK_DEV = 512
TOKENS = 8192


def drawn_pair(key):
    full_shape = (TOKENS, HEADS * HEAD)
    query_rows = jnp.clip(jax.random.normal(jax.random.fold_in(key, 101), full_shape, jnp.float32), -4.5, 4.5)
    key_rows = jnp.clip(jax.random.normal(jax.random.fold_in(key, 102), full_shape, jnp.float32), -4.5, 4.5)
    return (query_rows, key_rows)


def draw_queries(key, part):
    return drawn_pair(key)[0].astype(jnp.bfloat16)


def draw_keys(key, part):
    return drawn_pair(key)[1].astype(jnp.bfloat16)


def draw_forget_logits(key, part):
    ranks = jax.random.permutation(jax.random.fold_in(key, 201), HEADS)
    quick = ranks < HEADS // 2
    levels = jax.random.uniform(jax.random.fold_in(key, 202), (HEADS,), jnp.float32, -0.5, 0.5)
    base_level = jnp.where(quick, math.log(80.0), math.log(TOKENS) + 1.0) + levels
    span_rows = max(TOK_DEV // 2, 1)
    shifts = jax.random.uniform(jax.random.fold_in(key, 203), (TOKENS // span_rows + 1, 1), jnp.float32, -0.9, 0.9)
    span_shift = jnp.repeat(shifts, span_rows, axis=0)[:TOKENS]
    noise = jnp.clip(jax.random.normal(jax.random.fold_in(key, 204), (TOKENS, HEADS), jnp.float32), -3.0, 3.0)
    return base_level[None, :] + span_shift + noise


def raised(values, own_key, source, target, parts, factor):
    def block_of(position):
        return (jnp.arange(values.shape[position]) // (values.shape[position] // parts)).reshape((-1,) + (1,) * (values.ndim - 1 - position))

    one_side = jax.random.permutation(own_key, parts)[block_of(target)]
    other_side = (block_of(target) + parts // 2) % parts
    return jnp.where((block_of(source) == one_side) | (block_of(source) == other_side), factor * values, values)


def level_of(key, shape, cuts, smallest, top_value):
    factor_of = 1.0
    for axis_at, shards_of in cuts:
        heights = jax.random.uniform(jax.random.fold_in(jax.random.fold_in(key, 6), axis_at), (shards_of,), jnp.float32, smallest / len(cuts), top_value / len(cuts))
        factor_of = factor_of * jnp.repeat(jnp.exp(heights), shape[axis_at] // shards_of).reshape((-1,) + (1,) * (len(shape) - 1 - axis_at))
    return factor_of


def gaussian(own_key, extent, spread, bound, cuts=(), kind=jnp.bfloat16):
    drawn = spread * jax.random.normal(own_key, extent, jnp.float32)
    if cuts:
        drawn = drawn * level_of(own_key, extent, cuts, -0.22, 0.18)
    return jnp.clip(drawn, -bound, bound).astype(kind)


def heavy_noise(key, extent, width, reach, pieces, heavy, kind=jnp.bfloat16):
    entries = width * jax.random.normal(key, extent, jnp.float32)
    if pieces:
        entries = entries * level_of(key, extent, pieces, -0.22, 0.18)
    return jnp.clip(raised(entries, jax.random.fold_in(key, 3), *heavy), -reach, reach).astype(kind)


def setup_inputs(seed: int = 0) -> dict:
    key_list = jax.random.split(jax.random.key(seed), 7)
    return {
        "queries": draw_queries(jax.random.fold_in(key_list[6], 71), 0),
        "keys": draw_keys(jax.random.fold_in(key_list[6], 71), 0),
        "values": gaussian(key_list[2], (TOKENS, HEADS * HEAD), 1.0, 6.0, ((0, 16), (1, 8))),
        "forget_logits": draw_forget_logits(jax.random.fold_in(key_list[6], 71), 0),
        "layer_input": heavy_noise(key_list[4], (TOKENS, DMODEL), TOKENS ** -0.5, 0.09375, ((0, 16), (1, 8)), (0, 1, 16, 2.0)),
        "out_grad": heavy_noise(key_list[5], (TOKENS, HEADS * HEAD), 1.0, 6.0, ((0, 16), (1, 8)), (0, 1, 16, 2.0)),
    }


def query_block(row_count):
    block_size = row_count
    while block_size > 512 and block_size % 2 == 0:
        block_size //= 2
    return block_size


def reference(queries, keys, values, forget_logits, layer_input, out_grad):
    row_count = queries.shape[0]
    head_total = queries.shape[1] // HEAD
    score_scale = HEAD ** -0.5
    gate_sums = jnp.cumsum(jax.nn.log_sigmoid(forget_logits), axis=0)
    positions = jnp.arange(row_count, dtype=jnp.int32)
    block_size = query_block(row_count)
    block_count = row_count // block_size

    def by_head(array):
        return array.reshape(row_count, head_total, HEAD).transpose(1, 0, 2)

    def one_head(inputs):
        head_query, head_key, head_value, head_grad, head_gates = inputs

        def one_block(carry, number):
            key_total, value_total = carry
            begin_at = number * block_size
            query_rows = lax.dynamic_slice_in_dim(head_query, begin_at, block_size, 0)
            grad_rows = lax.dynamic_slice_in_dim(head_grad, begin_at, block_size, 0)
            gate_rows = lax.dynamic_slice_in_dim(head_gates, begin_at, block_size, 0)
            scores = jnp.dot(query_rows, head_key.T, preferred_element_type=jnp.float32) * score_scale
            scores = scores + gate_rows[:, None] - head_gates[None, :]
            query_pos = begin_at + jnp.arange(block_size, dtype=jnp.int32)
            visible = positions[None, :] <= query_pos[:, None]
            row_max = jnp.max(jnp.where(visible, scores, -1.0e30), axis=1)
            weights = jnp.where(visible, jnp.exp(scores - row_max[:, None]), 0.0)
            weight_sum = jnp.sum(weights, axis=1)
            mixed = jnp.dot(weights.astype(jnp.bfloat16), head_value, preferred_element_type=jnp.float32)
            attended = (mixed / weight_sum[:, None]).astype(jnp.bfloat16)
            log_sums = row_max + jnp.log(weight_sum)
            row_terms = jnp.sum(attended.astype(jnp.float32) * grad_rows.astype(jnp.float32), axis=1)
            probs = jnp.where(visible, jnp.exp(scores - log_sums[:, None]), 0.0)
            prob_grads = jnp.dot(grad_rows, head_value.T, preferred_element_type=jnp.float32)
            score_grads = (probs * (prob_grads - row_terms[:, None])).astype(jnp.bfloat16)
            query_part = score_scale * jnp.dot(score_grads, head_key, preferred_element_type=jnp.float32)
            key_total = key_total + score_scale * jnp.dot(score_grads.T, query_rows, preferred_element_type=jnp.float32)
            value_total = value_total + jnp.dot(probs.astype(jnp.bfloat16).T, grad_rows, preferred_element_type=jnp.float32)
            return (key_total, value_total), query_part

        zeros_head = jnp.zeros((row_count, HEAD), jnp.float32)
        (key_total, value_total), query_parts = lax.scan(one_block, (zeros_head, zeros_head), jnp.arange(block_count, dtype=jnp.int32))
        return query_parts.reshape(row_count, HEAD), key_total, value_total

    query_heads, key_heads, value_heads = lax.map(one_head, (by_head(queries), by_head(keys), by_head(values), by_head(out_grad), gate_sums.T))

    def back_rows(array):
        return array.transpose(1, 0, 2).reshape(row_count, head_total * HEAD)

    query_grad = back_rows(query_heads)
    weight_grad = jnp.dot(layer_input.T, query_grad.astype(jnp.bfloat16), preferred_element_type=jnp.float32)
    return query_grad, back_rows(key_heads), back_rows(value_heads), weight_grad
```

```python
import jax
import jax.numpy as jnp
from jax import lax
from jax.experimental import pallas as pl
from jax.experimental.pallas import tpu as pltpu
from jax.sharding import PartitionSpec as P

HEAD = 128
LOG2E = 1.4426950408889634
SCALE = HEAD ** (-0.5)
LOW = jnp.bfloat16
NX = 4
LAG = 2


def nt(a, b):
    return lax.dot_general(a, b, (((1,), (1,)), ((), ())), preferred_element_type=jnp.float32)


def nn(a, b):
    return lax.dot_general(a, b, (((1,), (0,)), ((), ())), preferred_element_type=jnp.float32)


def kernel_body(
    heads, wide,
    q_in, g_in, k_in, v_in, gate_in, x_in,
    dq_out, dk_out, dv_out, w_out,
    kv, qg, gates, kt, bias, wbuf, dpbuf, mrow, dk, dv, stat, stat_got,
    dq_stage, part_stage, red, fin, dq_got, kv_got,
    x_all, low, wa_stage, wb_stage, wa_red, wb_red, wa_own, wb_own, wa_fin, wb_fin, wa_got, wb_got,
    kv_recv, xs_send, col_send, x2_send, qg_recv, q_send, qf_send, gate_send, gate_recv, local_sem,
    stat_send, stat_recv, dq_send, dq_recv, part_send, red_recv, fin_send, fin_recv,
    x_send, xf_send, x_recv, wa_send, wb_send, wa_recv, wb_recv, wa_fsend, wb_fsend, wa_frecv, wb_frecv,
):
    blocks, _, hk, _ = kv.shape
    nx = NX
    nz = blocks // nx
    halves = nz // heads
    sub = qg.shape[2]
    tiles = blocks // 2
    span = w_out.shape[0]
    part_rows = span // 2
    x_width = x_in.shape[1]
    column = lax.axis_index("tp")
    me = lax.axis_index("sp")
    z = me // nx
    x = lax.rem(me, nx)
    head = z // halves
    half = lax.rem(z, halves)

    def at(zt, xt):
        return zt * nx + xt

    def near(r, c):
        return lax.rem(z + r, nz), lax.rem(x + c, nx)

    def remote(src, dst, send, recv, target):
        return pltpu.make_async_remote_copy(
            src_ref=src, dst_ref=dst, send_sem=send, recv_sem=recv, device_id={"sp": target}
        )

    def arrived(ref, recv):
        remote(ref, ref, dq_send.at[0], recv, me).wait_recv()

    barrier = pltpu.get_barrier_semaphore()
    for r in range(1, blocks):
        pl.semaphore_signal(barrier, inc=1, device_id={"sp": lax.rem(me + r, blocks)})
    for r in range(1, wide):
        pl.semaphore_signal(barrier, inc=1, device_id={"tp": lax.rem(column + r, wide)})
    pl.semaphore_wait(barrier, blocks + wide - 2)

    def lanes(h):
        return pl.ds(pl.multiple_of(h * HEAD, HEAD), HEAD)

    sent = []

    def go(copy):
        copy.start()
        sent.append(copy)

    kv_in = (k_in, v_in)
    qg_in = (q_in, g_in)

    def kv_source(i, zt):
        begin = pl.multiple_of(lax.rem(zt, halves) * hk, hk)
        return kv_in[i].at[pl.ds(begin, hk), lanes(zt // halves)]

    def q_source(i, zt, xt):
        begin = pl.multiple_of(xt * sub, sub)
        return qg_in[i].at[pl.ds(begin, sub), lanes(zt // halves)]

    for d, c in ((0, 1), (1, nx - 1)):
        for i in range(2):
            go(remote(kv_source(i, z), kv.at[me, i], xs_send.at[0, d, i], kv_recv.at[me, i], at(z, near(0, c)[1])))
    for r in (1, nz - 1, 2):
        zt = near(r, 0)[0]
        for i in range(2):
            go(remote(kv_source(i, zt), kv.at[me, i], col_send.at[r, i], kv_recv.at[me, i], at(zt, x)))

    across = nz - 1 - z
    partner = z + 1 - 2 * half

    def q_plane(r):
        return z if r == 0 else across

    for i in range(2):
        go(remote(q_source(i, z, x), qg.at[me, i], qf_send.at[0, 0, i], qg_recv.at[me, i], at(partner, x)))
    for r in range(heads):
        for c in range(nx):
            if (r, c) == (0, 0):
                continue
            zt, xt = q_plane(r), near(0, c)[1]
            for i in range(2):
                go(remote(q_source(i, zt, xt), qg.at[me, i], q_send.at[r, c, i], qg_recv.at[me, i], at(zt, xt)))
    for r in range(nz):
        for c in range(nx):
            if (r, c) == (0, 0):
                continue
            zt, xt = near(r, c)
            go(remote(gate_in.at[zt // halves], gates.at[me], gate_send.at[r, c], gate_recv.at[me], at(zt, xt)))

    def x_copy(src, source, target, send):
        return pltpu.make_async_remote_copy(
            src_ref=src, dst_ref=x_all.at[source], send_sem=send, recv_sem=x_recv.at[source], device_id={"tp": target}
        )

    core = lax.rem(column, 2)
    twin = column + 1 - 2 * core
    for r in range(1, wide // 2):
        go(x_copy(x_in, column, lax.rem(column + 2 * r, wide), x_send.at[r]))
    go(x_copy(x_in, column, twin, x_send.at[0]))

    own = [pltpu.make_async_copy(kv_source(i, z), kv.at[me, i], local_sem.at[i]) for i in range(2)]
    own += [pltpu.make_async_copy(q_source(i, z, x), qg.at[me, i], local_sem.at[2 + i]) for i in range(2)]
    own += [pltpu.make_async_copy(gate_in.at[head], gates.at[me], local_sem.at[4])]
    own += [pltpu.make_async_copy(x_in, x_all.at[column], local_sem.at[5])]
    for copy in own:
        copy.start()
    for copy in own:
        copy.wait()

    done = set()

    def kv_wait(r, c, i):
        if (r, c, i) in done:
            return
        done.add((r, c, i))
        j = at(*near(r, c))
        arrived(kv.at[j, i], kv_recv.at[j, i])

    def column_on(r):
        j = at(near(r, 0)[0], x)
        for i in range(2):
            kv_wait(r, 0, i)
            for d, c in ((0, 1), (1, nx - 1)):
                go(remote(kv.at[j, i], kv.at[j, i], xs_send.at[r, d, i], kv_recv.at[j, i], at(z, near(0, c)[1])))

    def second_on(r):
        for i, c in ((0, nx - 1), (1, 1)):
            kv_wait(r, c, i)
            j = at(*near(r, c))
            go(remote(kv.at[j, i], kv.at[j, i], x2_send.at[r, i], kv_recv.at[j, i], at(z, near(0, nx - c)[1])))

    def q_wait(j):
        for i in range(2):
            arrived(qg.at[j, i], qg_recv.at[j, i])

    def q_on(r, c):
        j = at(q_plane(r), near(0, c)[1])
        q_wait(j)
        for i in range(2):
            go(remote(qg.at[j, i], qg.at[j, i], qf_send.at[r, c, i], qg_recv.at[j, i], at(partner, x)))

    column_on(1)
    column_on(nz - 1)
    second_on(0)
    for c in range(1, nx):
        q_on(0, c)
    column_on(2)
    second_on(1)
    second_on(nz - 1)
    for c in range(nx):
        q_on(1, c)
    second_on(2)
    for plane in (partner, nz - 1 - partner):
        for c in range(nx):
            q_wait(at(plane, near(0, c)[1]))
    for r in range(nz):
        for c in range(nx):
            if (r, c) != (0, 0):
                j = at(*near(r, c))
                arrived(gates.at[j], gate_recv.at[j])

    def prepare(j, base):
        per = hk // HEAD
        table = gates[j]
        mine = table[0:per]
        for n in range(1, halves):
            mine = jnp.where(half == n, table[n * per : (n + 1) * per], mine)
        for n in range(per):
            row = mine[n : n + 1] + base
            bias[j, n * HEAD : (n + 1) * HEAD] = jnp.broadcast_to(row, (HEAD, HEAD)).T
        return base + table[halves * per : halves * per + 1]

    lax.fori_loop(0, blocks, prepare, jnp.zeros((1, HEAD), jnp.float32))
    for r in range(nz):
        for c in range(nx):
            if (r, c) != (0, 0):
                for i in range(2):
                    kv_wait(r, c, i)

    @pl.loop(0, tiles)
    def _(j):
        for n in range(2):
            kt[j, :, n * hk : (n + 1) * hk] = kv[2 * j + n, 0].T
        dk[j] = jnp.zeros((2 * hk, HEAD), jnp.float32)
        dv[j] = jnp.zeros((2 * hk, HEAD), jnp.float32)

    width = 2 * sub
    keys_wide = 2 * hk

    def forward(t):
        slot = lax.rem(t, 2)
        q = qg[pl.ds(2 * t, 2), 0].reshape(width, HEAD)
        g = qg[pl.ds(2 * t, 2), 1].reshape(width, HEAD)

        def block(j, state, mask):
            m, total, terms = state
            k = kv[pl.ds(2 * j, 2), 0].reshape(keys_wide, HEAD)
            v = kv[pl.ds(2 * j, 2), 1].reshape(keys_wide, HEAD)
            column_bias = bias[pl.ds(2 * j, 2)].reshape(keys_wide, HEAD)
            s = nt(k, q) * (SCALE * LOG2E) - jnp.concatenate([column_bias] * (width // HEAD), axis=1)
            if mask is not None:
                s = jnp.where(mask, s, -1e30)
            top = jnp.maximum(m, jnp.max(s, axis=0, keepdims=True))
            w = jnp.exp2(s - top)
            old = jnp.exp2(m - top)
            dp = nt(v, g)
            wbuf[slot, j] = w
            dpbuf[slot, j] = dp
            mrow[slot, j] = jnp.broadcast_to(top, (8, width))
            total = total * old + jnp.sum(w, axis=0, keepdims=True)
            terms = terms * old + jnp.sum(w * dp, axis=0, keepdims=True)
            return top, total, terms

        zero = jnp.zeros((1, width), jnp.float32)
        state = lax.fori_loop(
            0, t, lambda j, state: block(j, state, None), (jnp.full((1, width), -1e30, jnp.float32), zero, zero)
        )
        rows = halves * hk
        key_row = lax.broadcasted_iota(jnp.int32, (keys_wide, width), 0)
        query_row = lax.broadcasted_iota(jnp.int32, (keys_wide, width), 1)
        key_pos = jnp.where(key_row >= hk, key_row - hk + rows, key_row) + half * hk
        query_pos = jnp.where(query_row >= sub, query_row - sub + rows, query_row) + x * sub
        m, total, terms = block(t, state, key_pos <= query_pos)
        stat[t] = jnp.concatenate([m, total, terms, jnp.zeros((5, width), jnp.float32)], axis=0)

    def backward(t):
        slot = lax.rem(t, 2)
        q = qg[pl.ds(2 * t, 2), 0].reshape(width, HEAD)
        g = qg[pl.ds(2 * t, 2), 1].reshape(width, HEAD)
        arrived(stat_got.at[t], stat_recv.at[t])
        mine = stat[t]
        other = stat_got[t]
        top = jnp.maximum(mine[0:1], other[0:1])
        scale_mine = jnp.exp2(mine[0:1] - top)
        scale_other = jnp.exp2(other[0:1] - top)
        inverse = 1.0 / (mine[1:2] * scale_mine + other[1:2] * scale_other)
        terms = (mine[2:3] * scale_mine + other[2:3] * scale_other) * inverse

        def block(j, acc):
            factor = jnp.exp2(mrow[slot, j][0:1] - top) * inverse
            prob = wbuf[slot, j] * factor
            ds = (prob * (dpbuf[slot, j] - terms)).astype(LOW)
            dv[j] += nn(prob.astype(LOW), g)
            dk[j] += nn(ds, q)
            return acc + nn(kt[j], ds)

        acc = lax.fori_loop(0, t + 1, block, jnp.zeros((HEAD, width), jnp.float32))
        dq_t = (acc * SCALE).T.astype(LOW)
        for n in range(2):
            dq_stage[2 * t + n] = dq_t[n * sub : (n + 1) * sub]
            part_stage[2 * t + n, 0] = (dk[t, n * hk : (n + 1) * hk] * SCALE).astype(LOW)
            part_stage[2 * t + n, 1] = dv[t, n * hk : (n + 1) * hk].astype(LOW)

    def stat_copy(t):
        return remote(stat.at[t], stat_got.at[t], stat_send.at[t], stat_recv.at[t], at(partner, x))

    def dq_copy(n):
        return remote(dq_stage.at[n], dq_got.at[z, x], dq_send.at[n], dq_recv.at[me], n)

    def part_copy(n):
        return remote(
            part_stage.at[n], red.at[n // nx, x], part_send.at[n], red_recv.at[n // nx, x], at(z, lax.rem(n, nx))
        )

    def fin_copy(n):
        return remote(fin.at[n // nx], kv_got.at[z], fin_send.at[n // nx], fin_recv.at[z], n)

    def x_on(r):
        return x_copy(
            x_all.at[lax.rem(column + 2 * r, wide)], lax.rem(column + 2 * r, wide), twin, xf_send.at[r]
        )

    def step(s, carry):
        t = tiles - 1 - s

        @pl.when(s < tiles)
        def _():
            forward(t)

        @pl.when((s >= 2) & (s < tiles + 2))
        def _():
            for u in range(2):
                n = 2 * (t + 2) + u

                @pl.when(n == me)
                def _():
                    dq_got[z, x] = dq_stage[n]

                @pl.when(n != me)
                def _():
                    dq_copy(n).start()

                @pl.when(lax.rem(n, nx) != x)
                def _():
                    part_copy(n).start()

        @pl.when(s < tiles)
        def _():
            stat_copy(t).start()

        @pl.when((s >= 2 + LAG) & (s < tiles + 2 + LAG))
        def _():
            tile = t + 2 + LAG
            for u in range(2):
                n = 2 * tile + u

                @pl.when(lax.rem(n, nx) == x)
                def _():
                    zn = n // nx
                    for c in range(1, nx):
                        other = lax.rem(x + c, nx)
                        arrived(red.at[zn, other], red_recv.at[zn, other])
                    for i in range(2):
                        value = dk[tile, u * hk : (u + 1) * hk] * SCALE if i == 0 else dv[tile, u * hk : (u + 1) * hk]
                        for c in range(1, nx):
                            value = value + red[zn, lax.rem(x + c, nx), i].astype(jnp.float32)
                        fin[zn, i] = value.astype(LOW)

        @pl.when((s >= 1) & (s < tiles + 1))
        def _():
            backward(t + 1)

        @pl.when(s == 2)
        def _():
            for r in range(1, wide // 2):
                source = lax.rem(column + 2 * r, wide)
                pltpu.make_async_remote_copy(
                    src_ref=x_all.at[source], dst_ref=x_all.at[source], send_sem=xf_send.at[r],
                    recv_sem=x_recv.at[source], device_id={"tp": twin},
                ).wait_recv()
                x_on(r).start()

        @pl.when(s >= 3 + LAG)
        def _():
            for u in range(2):
                n = 2 * (t + 3 + LAG) + u

                @pl.when(lax.rem(n, nx) == x)
                def _():
                    @pl.when(n == me)
                    def _():
                        kv_got[z] = fin[n // nx]

                    @pl.when(n != me)
                    def _():
                        fin_copy(n).start()

        return carry

    lax.fori_loop(0, tiles + 3 + LAG, step, 0)

    for r in range(nz):
        for c in range(nx):
            if (r, c) != (0, 0):
                zs, xs = near(r, c)
                arrived(dq_got.at[zs, xs], dq_recv.at[at(zs, xs)])
    for h in range(heads):
        for n in range(nx):
            value = dq_got[h * halves, n].astype(jnp.float32)
            for m in range(1, halves):
                value = value + dq_got[h * halves + m, n].astype(jnp.float32)
            dq_out[n * sub : (n + 1) * sub, h * HEAD : (h + 1) * HEAD] = value
            low[n * sub : (n + 1) * sub, h * HEAD : (h + 1) * HEAD] = value.astype(LOW)
    for r in range(wide // 2):
        source = lax.rem(twin + 2 * r, wide)
        pltpu.make_async_remote_copy(
            src_ref=x_all.at[source], dst_ref=x_all.at[source], send_sem=x_send.at[0],
            recv_sem=x_recv.at[source], device_id={"tp": twin},
        ).wait_recv()

    def term(c):
        begin = c * span
        xs = x_all[begin // x_width, :, pl.ds(pl.multiple_of(lax.rem(begin, x_width), span), span)]
        return lax.dot_general(xs, low[...], (((0,), (0,)), ((), ())), preferred_element_type=jnp.float32)

    waiting = []

    def flush():
        for copy in waiting:
            go(copy)
        waiting.clear()

    order = [(r, c) for r in range(1, nz) for c in range(1, nx)]
    order += [(0, c) for c in range(1, nx)] + [(r, 0) for r in range(1, nz)] + [(0, 0)]
    for r, c in order:
        zt, xt = near(r, c)
        value = term(at(zt, xt))
        fresh = []
        if c:
            wa_stage[r, c] = value[:part_rows].astype(LOW)
            fresh.append(
                remote(wa_stage.at[r, c], wa_red.at[x, zt], wa_send.at[r, c], wa_recv.at[x, zt], at(z, xt))
            )
        else:
            wa_own[r] = value[:part_rows]
        if r:
            wb_stage[r, c] = value[part_rows:].astype(LOW)
            fresh.append(
                remote(wb_stage.at[r, c], wb_red.at[z, xt], wb_send.at[r, c], wb_recv.at[z, xt], at(zt, x))
            )
        else:
            wb_own[c] = value[part_rows:]
        flush()
        waiting.extend(fresh)
    flush()

    for n in list(range(1, nz)) + [0]:
        zt = near(n, 0)[0]
        value = wa_own[n]
        for c in range(1, nx):
            xs = near(0, c)[1]
            arrived(wa_red.at[xs, zt], wa_recv.at[xs, zt])
            value = value + wa_red[xs, zt].astype(jnp.float32)
        fresh = []
        if n:
            wa_fin[n] = value.astype(LOW)
            fresh.append(remote(wa_fin.at[n], wa_got.at[z], wa_fsend.at[n], wa_frecv.at[z], at(zt, x)))
        else:
            w_out[:part_rows] = value
        xt = near(0, n)[1]
        value = wb_own[n]
        for r in range(1, nz):
            zs = near(r, 0)[0]
            arrived(wb_red.at[zs, xt], wb_recv.at[zs, xt])
            value = value + wb_red[zs, xt].astype(jnp.float32)
        if n:
            wb_fin[n] = value.astype(LOW)
            fresh.append(remote(wb_fin.at[n], wb_got.at[x], wb_fsend.at[n], wb_frecv.at[x], at(z, xt)))
        else:
            w_out[part_rows:] = value
        flush()
        waiting.extend(fresh)
    flush()

    for r in range(1, nz):
        zs = near(r, 0)[0]
        arrived(kv_got.at[zs], fin_recv.at[zs])
    for h in range(heads):
        for m in range(halves):
            dk_out[m * hk : (m + 1) * hk, h * HEAD : (h + 1) * HEAD] = kv_got[h * halves + m, 0].astype(jnp.float32)
            dv_out[m * hk : (m + 1) * hk, h * HEAD : (h + 1) * HEAD] = kv_got[h * halves + m, 1].astype(jnp.float32)
    for n in range(1, nz):
        zs = near(n, 0)[0]
        arrived(wa_got.at[zs], wa_frecv.at[zs])
        w_out[:part_rows] += wa_got[zs].astype(jnp.float32)
        xs = near(0, n)[1]
        arrived(wb_got.at[xs], wb_frecv.at[xs])
        w_out[part_rows:] += wb_got[xs].astype(jnp.float32)

    for copy in sent:
        copy.wait_send()
    for r in range(1, wide // 2):
        x_on(r).wait_send()

    @pl.loop(0, tiles)
    def _(t):
        stat_copy(t).wait_send()

    @pl.loop(0, blocks)
    def _(n):
        @pl.when(n != me)
        def _():
            dq_copy(n).wait_send()

        @pl.when(lax.rem(n, nx) != x)
        def _():
            part_copy(n).wait_send()

        @pl.when((lax.rem(n, nx) == x) & (n != me))
        def _():
            fin_copy(n).wait_send()


def attention(blocks, wide, q, g, k, v, gate, x):
    rows, cols = k.shape
    heads = cols // HEAD
    nx = NX
    nz = blocks // nx
    halves = nz // heads
    hk = rows // halves
    sub = rows // nx
    tiles = blocks // 2
    vmem = pl.BlockSpec(memory_space=pltpu.VMEM)
    f32 = jnp.float32
    dma = pltpu.SemaphoreType.DMA
    span = x.shape[1] * wide // blocks
    part = span // 2
    grad = jax.ShapeDtypeStruct((rows, cols), f32)
    return pl.pallas_call(
        lambda *refs: kernel_body(heads, wide, *refs),
        out_shape=(grad, grad, grad, jax.ShapeDtypeStruct((span, cols), f32)),
        in_specs=[vmem] * 6,
        out_specs=(vmem,) * 4,
        scratch_shapes=[
            pltpu.VMEM((blocks, 2, hk, HEAD), LOW),
            pltpu.VMEM((blocks, 2, sub, HEAD), LOW),
            pltpu.VMEM((blocks, 8, HEAD), f32),
            pltpu.VMEM((tiles, HEAD, 2 * hk), LOW),
            pltpu.VMEM((blocks, hk, HEAD), f32),
            pltpu.VMEM((2, tiles, 2 * hk, 2 * sub), f32),
            pltpu.VMEM((2, tiles, 2 * hk, 2 * sub), f32),
            pltpu.VMEM((2, tiles, 8, 2 * sub), f32),
            pltpu.VMEM((tiles, 2 * hk, HEAD), f32),
            pltpu.VMEM((tiles, 2 * hk, HEAD), f32),
            pltpu.VMEM((tiles, 8, 2 * sub), f32),
            pltpu.VMEM((tiles, 8, 2 * sub), f32),
            pltpu.VMEM((blocks, sub, HEAD), LOW),
            pltpu.VMEM((blocks, 2, hk, HEAD), LOW),
            pltpu.VMEM((nz, nx, 2, hk, HEAD), LOW),
            pltpu.VMEM((nz, 2, hk, HEAD), LOW),
            pltpu.VMEM((nz, nx, sub, HEAD), LOW),
            pltpu.VMEM((nz, 2, hk, HEAD), LOW),
            pltpu.VMEM((wide, rows, x.shape[1]), LOW),
            pltpu.VMEM((rows, cols), LOW),
            pltpu.VMEM((nz, nx, part, cols), LOW),
            pltpu.VMEM((nz, nx, part, cols), LOW),
            pltpu.VMEM((nx, nz, part, cols), LOW),
            pltpu.VMEM((nz, nx, part, cols), LOW),
            pltpu.VMEM((nz, part, cols), f32),
            pltpu.VMEM((nx, part, cols), f32),
            pltpu.VMEM((nz, part, cols), LOW),
            pltpu.VMEM((nx, part, cols), LOW),
            pltpu.VMEM((nz, part, cols), LOW),
            pltpu.VMEM((nx, part, cols), LOW),
            dma((blocks, 2)), dma((nz, 2, 2)), dma((nz, 2)), dma((nz, 2)), dma((blocks, 2)), dma((heads, nx, 2)),
            dma((heads, nx, 2)), dma((nz, nx)), dma((blocks,)), dma((6,)),
            dma((tiles,)), dma((tiles,)), dma((blocks,)), dma((blocks,)), dma((blocks,)), dma((nz, nx)),
            dma((nz,)), dma((nz,)),
            dma((wide // 2,)), dma((wide // 2,)), dma((wide,)),
            dma((nz, nx)), dma((nz, nx)), dma((nx, nz)), dma((nz, nx)),
            dma((nz,)), dma((nx,)), dma((nz,)), dma((nx,)),
        ],
        compiler_params=pltpu.CompilerParams(
            vmem_limit_bytes=62 * 1024 * 1024, collective_id=0, has_side_effects=True
        ),
        cost_estimate=pl.CostEstimate(
            flops=10 * blocks * blocks * rows * sub * HEAD, bytes_accessed=1 << 22, transcendentals=0
        ),
        name="attention",
    )(q, g, k, v, gate, x)


def local(queries, keys, values, forget_logits, layer_input, out_grad):
    rows = queries.shape[0]
    heads = queries.shape[1] // HEAD
    blocks = lax.axis_size("sp")
    wide = lax.axis_size("tp")
    gates = jnp.cumsum(jax.nn.log_sigmoid(forget_logits), axis=0).T * LOG2E
    totals = jnp.broadcast_to(gates[:, rows - 1 :, None], (heads, 8 - rows // HEAD, HEAD))
    gates = jnp.concatenate([gates.reshape(heads, rows // HEAD, HEAD), totals], axis=1)
    return attention(blocks, wide, queries, out_grad, keys, values, gates, layer_input)


def solution(mesh):
    spec = P("sp", "tp")
    return jax.shard_map(
        local, mesh=mesh, in_specs=(spec,) * 6, out_specs=(spec,) * 4, check_vma=False
    )
```

```python
import jax
import jax.numpy as jnp
from jax import lax
from jax.experimental import pallas as pl
from jax.experimental.pallas import tpu as pltpu
from jax.sharding import PartitionSpec as P

HEAD = 128
LOG2E = 1.4426950408889634
SCALE = HEAD ** (-0.5)
LOW = jnp.bfloat16
NX = 4


def nt(a, b):
    return lax.dot_general(a, b, (((1,), (1,)), ((), ())), preferred_element_type=jnp.float32)


def nn(a, b):
    return lax.dot_general(a, b, (((1,), (0,)), ((), ())), preferred_element_type=jnp.float32)


def kernel_body(
    heads, wide,
    q_in, g_in, k_in, v_in, gate_in, x_in,
    dq_out, dk_out, dv_out, w_out,
    kv, qg, gates, kt, bias, wbuf, dpbuf, mrow, dk, dv, stat, stat_got,
    dq_stage, part_stage, mid, red, fin, dq_got, kv_got,
    x_all, low, wa_stage, wb_stage, wa_red, wb_red, wa_own, wb_own, wa_fin, wb_fin, wa_got, wb_got,
    kv_recv, xs_send, col_send, x2_send, qg_recv, q_send, qf_send, gate_send, gate_recv, local_sem,
    stat_send, stat_recv, dq_send, dq_recv, part_send, mid_recv, red_recv, fin_send, fin_recv,
    x_send, xf_send, x_recv, wa_send, wb_send, wa_recv, wb_recv, wa_fsend, wb_fsend, wa_frecv, wb_frecv,
):
    blocks, _, hk, _ = kv.shape
    nx = NX
    nz = blocks // nx
    halves = nz // heads
    sub = qg.shape[2]
    tiles = blocks // 2
    span = w_out.shape[0]
    part_rows = span // 2
    x_width = x_in.shape[1]
    column = lax.axis_index("tp")
    me = lax.axis_index("sp")
    z = me // nx
    x = lax.rem(me, nx)
    head = z // halves
    half = lax.rem(z, halves)

    def at(zt, xt):
        return zt * nx + xt

    def near(r, c):
        return lax.rem(z + r, nz), lax.rem(x + c, nx)

    def remote(src, dst, send, recv, target):
        return pltpu.make_async_remote_copy(
            src_ref=src, dst_ref=dst, send_sem=send, recv_sem=recv, device_id={"sp": target}
        )

    def arrived(ref, recv):
        remote(ref, ref, dq_send.at[0], recv, me).wait_recv()

    barrier = pltpu.get_barrier_semaphore()
    for r in range(1, blocks):
        pl.semaphore_signal(barrier, inc=1, device_id={"sp": lax.rem(me + r, blocks)})
    for r in range(1, wide):
        pl.semaphore_signal(barrier, inc=1, device_id={"tp": lax.rem(column + r, wide)})
    pl.semaphore_wait(barrier, blocks + wide - 2)

    def lanes(h):
        return pl.ds(pl.multiple_of(h * HEAD, HEAD), HEAD)

    sent = []

    def go(copy):
        copy.start()
        sent.append(copy)

    kv_in = (k_in, v_in)
    qg_in = (q_in, g_in)

    def kv_source(i, zt):
        begin = pl.multiple_of(lax.rem(zt, halves) * hk, hk)
        return kv_in[i].at[pl.ds(begin, hk), lanes(zt // halves)]

    def q_source(i, zt, xt):
        begin = pl.multiple_of(xt * sub, sub)
        return qg_in[i].at[pl.ds(begin, sub), lanes(zt // halves)]

    for r in range(nz):
        for c in range(nx):
            if (r, c) == (0, 0):
                continue
            zt, xt = near(r, c)
            go(remote(gate_in.at[zt // halves], gates.at[me], gate_send.at[r, c], gate_recv.at[me], at(zt, xt)))

    for d, c in ((0, 1), (1, nx - 1)):
        for i in range(2):
            go(remote(kv_source(i, z), kv.at[me, i], xs_send.at[0, d, i], kv_recv.at[me, i], at(z, near(0, c)[1])))
    for r in (1, nz - 1, 2):
        zt = near(r, 0)[0]
        for i in range(2):
            go(remote(kv_source(i, zt), kv.at[me, i], col_send.at[r, i], kv_recv.at[me, i], at(zt, x)))

    across = nz - 1 - z
    partner = z + 1 - 2 * half

    def q_plane(r):
        return z if r == 0 else across

    for i in range(2):
        go(remote(q_source(i, z, x), qg.at[me, i], qf_send.at[0, 0, i], qg_recv.at[me, i], at(partner, x)))
    for r in range(heads):
        for c in range(nx):
            if (r, c) == (0, 0):
                continue
            zt, xt = q_plane(r), near(0, c)[1]
            for i in range(2):
                go(remote(q_source(i, zt, xt), qg.at[me, i], q_send.at[r, c, i], qg_recv.at[me, i], at(zt, xt)))

    def x_copy(src, source, target, send):
        return pltpu.make_async_remote_copy(
            src_ref=src, dst_ref=x_all.at[source], send_sem=send, recv_sem=x_recv.at[source], device_id={"tp": target}
        )

    core = lax.rem(column, 2)
    twin = column + 1 - 2 * core
    for r in range(1, wide // 2):
        go(x_copy(x_in, column, lax.rem(column + 2 * r, wide), x_send.at[r]))
    go(x_copy(x_in, column, twin, x_send.at[0]))

    own = [pltpu.make_async_copy(kv_source(i, z), kv.at[me, i], local_sem.at[i]) for i in range(2)]
    own += [pltpu.make_async_copy(q_source(i, z, x), qg.at[me, i], local_sem.at[2 + i]) for i in range(2)]
    own += [pltpu.make_async_copy(gate_in.at[head], gates.at[me], local_sem.at[4])]
    own += [pltpu.make_async_copy(x_in, x_all.at[column], local_sem.at[5])]
    for copy in own:
        copy.start()
    for copy in own:
        copy.wait()

    @pl.loop(0, tiles)
    def _(j):
        dk[j] = jnp.zeros((2 * hk, HEAD), jnp.float32)
        dv[j] = jnp.zeros((2 * hk, HEAD), jnp.float32)

    done = set()

    def kv_wait(r, c, i):
        if (r, c, i) in done:
            return
        done.add((r, c, i))
        j = at(*near(r, c))
        arrived(kv.at[j, i], kv_recv.at[j, i])

    def column_on(r):
        j = at(near(r, 0)[0], x)
        for i in range(2):
            kv_wait(r, 0, i)
            for d, c in ((0, 1), (1, nx - 1)):
                go(remote(kv.at[j, i], kv.at[j, i], xs_send.at[r, d, i], kv_recv.at[j, i], at(z, near(0, c)[1])))

    def second_on(r):
        for i, c in ((0, nx - 1), (1, 1)):
            kv_wait(r, c, i)
            j = at(*near(r, c))
            go(remote(kv.at[j, i], kv.at[j, i], x2_send.at[r, i], kv_recv.at[j, i], at(z, near(0, nx - c)[1])))

    def q_wait(j):
        for i in range(2):
            arrived(qg.at[j, i], qg_recv.at[j, i])

    def q_on(r, c):
        j = at(q_plane(r), near(0, c)[1])
        q_wait(j)
        for i in range(2):
            go(remote(qg.at[j, i], qg.at[j, i], qf_send.at[r, c, i], qg_recv.at[j, i], at(partner, x)))

    column_on(1)
    column_on(nz - 1)
    second_on(0)
    for c in range(1, nx):
        q_on(0, c)
    column_on(2)
    second_on(1)
    second_on(nz - 1)
    for c in range(nx):
        q_on(1, c)
    second_on(2)
    for r in range(nz):
        for c in range(nx):
            if (r, c) != (0, 0):
                j = at(*near(r, c))
                arrived(gates.at[j], gate_recv.at[j])

    def prepare(j, base):
        per = hk // HEAD
        table = gates[j]
        mine = table[0:per]
        for n in range(1, halves):
            mine = jnp.where(half == n, table[n * per : (n + 1) * per], mine)
        for n in range(per):
            row = mine[n : n + 1] + base
            bias[j, n * HEAD : (n + 1) * HEAD] = jnp.broadcast_to(row, (HEAD, HEAD)).T
        return base + table[halves * per : halves * per + 1]

    lax.fori_loop(0, blocks, prepare, jnp.zeros((1, HEAD), jnp.float32))
    for plane in (partner, nz - 1 - partner):
        for c in range(nx):
            q_wait(at(plane, near(0, c)[1]))
    for r in range(nz):
        for c in range(nx):
            if (r, c) != (0, 0):
                for i in range(2):
                    kv_wait(r, c, i)

    @pl.loop(0, tiles)
    def _(j):
        for n in range(2):
            kt[j, :, n * hk : (n + 1) * hk] = kv[2 * j + n, 0].T

    width = 2 * sub
    keys_wide = 2 * hk

    def forward(t):
        slot = lax.rem(t, 2)
        q = qg[pl.ds(2 * t, 2), 0].reshape(width, HEAD)
        g = qg[pl.ds(2 * t, 2), 1].reshape(width, HEAD)

        def block(j, state, mask):
            m, total, terms = state
            k = kv[pl.ds(2 * j, 2), 0].reshape(keys_wide, HEAD)
            v = kv[pl.ds(2 * j, 2), 1].reshape(keys_wide, HEAD)
            column_bias = bias[pl.ds(2 * j, 2)].reshape(keys_wide, HEAD)
            s = nt(k, q) * (SCALE * LOG2E) - jnp.concatenate([column_bias] * (width // HEAD), axis=1)
            if mask is not None:
                s = jnp.where(mask, s, -1e30)
            top = jnp.maximum(m, jnp.max(s, axis=0, keepdims=True))
            w = jnp.exp2(s - top)
            old = jnp.exp2(m - top)
            dp = nt(v, g)
            wbuf[slot, j] = w
            dpbuf[slot, j] = dp
            mrow[slot, j] = jnp.broadcast_to(top, (8, width))
            total = total * old + jnp.sum(w, axis=0, keepdims=True)
            terms = terms * old + jnp.sum(w * dp, axis=0, keepdims=True)
            return top, total, terms

        zero = jnp.zeros((1, width), jnp.float32)
        state = lax.fori_loop(
            0, t, lambda j, state: block(j, state, None), (jnp.full((1, width), -1e30, jnp.float32), zero, zero)
        )
        rows = halves * hk
        key_row = lax.broadcasted_iota(jnp.int32, (keys_wide, width), 0)
        query_row = lax.broadcasted_iota(jnp.int32, (keys_wide, width), 1)
        key_pos = jnp.where(key_row >= hk, key_row - hk + rows, key_row) + half * hk
        query_pos = jnp.where(query_row >= sub, query_row - sub + rows, query_row) + x * sub
        m, total, terms = block(t, state, key_pos <= query_pos)
        stat[t] = jnp.concatenate([m, total, terms, jnp.zeros((5, width), jnp.float32)], axis=0)

    def backward(t):
        slot = lax.rem(t, 2)
        q = qg[pl.ds(2 * t, 2), 0].reshape(width, HEAD)
        g = qg[pl.ds(2 * t, 2), 1].reshape(width, HEAD)
        arrived(stat_got.at[t], stat_recv.at[t])
        mine = stat[t]
        other = stat_got[t]
        top = jnp.maximum(mine[0:1], other[0:1])
        scale_mine = jnp.exp2(mine[0:1] - top)
        scale_other = jnp.exp2(other[0:1] - top)
        inverse = 1.0 / (mine[1:2] * scale_mine + other[1:2] * scale_other)
        terms = (mine[2:3] * scale_mine + other[2:3] * scale_other) * inverse

        def block(j, acc):
            factor = jnp.exp2(mrow[slot, j][0:1] - top) * inverse
            prob = wbuf[slot, j] * factor
            ds = (prob * (dpbuf[slot, j] - terms)).astype(LOW)
            dv[j] += nn(prob.astype(LOW), g)
            dk[j] += nn(ds, q)
            return acc + nn(kt[j], ds)

        acc = block(t, jnp.zeros((HEAD, width), jnp.float32))
        for n in range(2):
            part_stage[2 * t + n, 0] = (dk[t, n * hk : (n + 1) * hk] * SCALE).astype(LOW)
            part_stage[2 * t + n, 1] = dv[t, n * hk : (n + 1) * hk].astype(LOW)
        acc = lax.fori_loop(0, t, block, acc)
        dq_t = (acc * SCALE).T.astype(LOW)
        for n in range(2):
            dq_stage[2 * t + n] = dq_t[n * sub : (n + 1) * sub]

    def stat_copy(t):
        return remote(stat.at[t], stat_got.at[t], stat_send.at[t], stat_recv.at[t], at(partner, x))

    def dq_copy(n):
        return remote(dq_stage.at[n], dq_got.at[z, x], dq_send.at[n], dq_recv.at[me], n)

    def away(n):
        return lax.rem(lax.rem(n, nx) + nx - x, nx)

    def opposite_copy(n, i):
        xt = lax.rem(x + (1 if i == 0 else nx - 1), nx)
        return remote(part_stage.at[n, i], mid.at[n // nx, i], part_send.at[n, i], mid_recv.at[n // nx, i], at(z, xt))

    def near_copy(n, side, i):
        return remote(
            part_stage.at[n, i], red.at[n // nx, side, i], part_send.at[n, i], red_recv.at[n // nx, side, i],
            at(z, lax.rem(n, nx)),
        )

    def first_sends(tile):
        for u in range(2):
            n = 2 * tile + u

            @pl.when(away(n) == 2)
            def _():
                opposite_copy(n, 0).start()
                opposite_copy(n, 1).start()

            @pl.when(away(n) == 1)
            def _():
                near_copy(n, 0, 1).start()

            @pl.when(away(n) == nx - 1)
            def _():
                near_copy(n, 1, 0).start()

    def add_on_way(tile):
        for u in range(2):
            n = 2 * tile + u
            zn = n // nx
            for i, d in ((0, 1), (1, nx - 1)):

                @pl.when(away(n) == d)
                def _():
                    arrived(mid.at[zn, i], mid_recv.at[zn, i])
                    value = dk[tile, u * hk : (u + 1) * hk] * SCALE if i == 0 else dv[tile, u * hk : (u + 1) * hk]
                    part_stage[n, i] = (value + mid[zn, i].astype(jnp.float32)).astype(LOW)

    def second_sends(tile):
        for u in range(2):
            n = 2 * tile + u

            @pl.when(away(n) == 1)
            def _():
                near_copy(n, 0, 0).start()

            @pl.when(away(n) == nx - 1)
            def _():
                near_copy(n, 1, 1).start()

    def reduce(tile):
        for u in range(2):
            n = 2 * tile + u

            @pl.when(away(n) == 0)
            def _():
                zn = n // nx
                for i in range(2):
                    for side in range(2):
                        arrived(red.at[zn, side, i], red_recv.at[zn, side, i])
                    value = dk[tile, u * hk : (u + 1) * hk] * SCALE if i == 0 else dv[tile, u * hk : (u + 1) * hk]
                    for side in range(2):
                        value = value + red[zn, side, i].astype(jnp.float32)
                    fin[zn, i] = value.astype(LOW)

    def fin_sends(tile):
        for u in range(2):
            n = 2 * tile + u

            @pl.when((away(n) == 0) & (n == me))
            def _():
                kv_got[z] = fin[n // nx]

            @pl.when((away(n) == 0) & (n != me))
            def _():
                fin_copy(n).start()

    def dq_sends(tile):
        for u in range(2):
            n = 2 * tile + u

            @pl.when(n == me)
            def _():
                dq_got[z, x] = dq_stage[n]

            @pl.when(n != me)
            def _():
                dq_copy(n).start()

    def fin_copy(n):
        return remote(fin.at[n // nx], kv_got.at[z], fin_send.at[n // nx], fin_recv.at[z], n)

    def x_on(r):
        return x_copy(
            x_all.at[lax.rem(column + 2 * r, wide)], lax.rem(column + 2 * r, wide), twin, xf_send.at[r]
        )

    def step(s, carry):
        t = tiles - 1 - s

        def stage(offset, work):
            pl.when((t + offset >= 0) & (t + offset < tiles))(lambda: work(t + offset))

        stage(0, forward)
        stage(2, dq_sends)
        stage(3, second_sends)
        stage(5, fin_sends)
        stage(0, lambda tile: stat_copy(tile).start())
        stage(1, backward)
        stage(1, first_sends)
        stage(2, add_on_way)
        stage(4, reduce)

        @pl.when(s == 2)
        def _():
            for r in range(1, wide // 2):
                source = lax.rem(column + 2 * r, wide)
                pltpu.make_async_remote_copy(
                    src_ref=x_all.at[source], dst_ref=x_all.at[source], send_sem=xf_send.at[r],
                    recv_sem=x_recv.at[source], device_id={"tp": twin},
                ).wait_recv()
                x_on(r).start()

        return carry

    lax.fori_loop(0, tiles + 2, step, 0)
    second_sends(0)
    fin_sends(2)

    for r in range(nz):
        for c in range(nx):
            if (r, c) != (0, 0):
                zs, xs = near(r, c)
                arrived(dq_got.at[zs, xs], dq_recv.at[at(zs, xs)])
    for h in range(heads):
        for n in range(nx):
            value = dq_got[h * halves, n].astype(jnp.float32)
            for m in range(1, halves):
                value = value + dq_got[h * halves + m, n].astype(jnp.float32)
            dq_out[n * sub : (n + 1) * sub, h * HEAD : (h + 1) * HEAD] = value
            low[n * sub : (n + 1) * sub, h * HEAD : (h + 1) * HEAD] = value.astype(LOW)
    reduce(1)
    for r in range(wide // 2):
        source = lax.rem(twin + 2 * r, wide)
        pltpu.make_async_remote_copy(
            src_ref=x_all.at[source], dst_ref=x_all.at[source], send_sem=x_send.at[0],
            recv_sem=x_recv.at[source], device_id={"tp": twin},
        ).wait_recv()

    def term(c):
        begin = c * span
        xs = x_all[begin // x_width, :, pl.ds(pl.multiple_of(lax.rem(begin, x_width), span), span)]
        return lax.dot_general(xs, low[...], (((0,), (0,)), ((), ())), preferred_element_type=jnp.float32)

    waiting = []

    def flush():
        for copy in waiting:
            go(copy)
        waiting.clear()

    order = [(r, c) for r in range(1, nz) for c in range(1, nx)]
    order += [(0, c) for c in range(1, nx)] + [(r, 0) for r in range(1, nz)] + [(0, 0)]
    for r, c in order:
        zt, xt = near(r, c)
        value = term(at(zt, xt))
        fresh = []
        if c:
            wa_stage[r, c] = value[:part_rows].astype(LOW)
            fresh.append(
                remote(wa_stage.at[r, c], wa_red.at[x, zt], wa_send.at[r, c], wa_recv.at[x, zt], at(z, xt))
            )
        else:
            wa_own[r] = value[:part_rows]
        if r:
            wb_stage[r, c] = value[part_rows:].astype(LOW)
            fresh.append(
                remote(wb_stage.at[r, c], wb_red.at[z, xt], wb_send.at[r, c], wb_recv.at[z, xt], at(zt, x))
            )
        else:
            wb_own[c] = value[part_rows:]
        flush()
        waiting.extend(fresh)
    flush()
    fin_sends(1)
    reduce(0)

    for n in list(range(1, nz)) + [0]:
        zt = near(n, 0)[0]
        value = wa_own[n]
        for c in range(1, nx):
            xs = near(0, c)[1]
            arrived(wa_red.at[xs, zt], wa_recv.at[xs, zt])
            value = value + wa_red[xs, zt].astype(jnp.float32)
        fresh = []
        if n:
            wa_fin[n] = value.astype(LOW)
            fresh.append(remote(wa_fin.at[n], wa_got.at[z], wa_fsend.at[n], wa_frecv.at[z], at(zt, x)))
        else:
            w_out[:part_rows] = value
        xt = near(0, n)[1]
        value = wb_own[n]
        for r in range(1, nz):
            zs = near(r, 0)[0]
            arrived(wb_red.at[zs, xt], wb_recv.at[zs, xt])
            value = value + wb_red[zs, xt].astype(jnp.float32)
        if n:
            wb_fin[n] = value.astype(LOW)
            fresh.append(remote(wb_fin.at[n], wb_got.at[x], wb_fsend.at[n], wb_frecv.at[x], at(z, xt)))
        else:
            w_out[part_rows:] = value
        flush()
        waiting.extend(fresh)
    flush()

    fin_sends(0)
    for r in range(1, nz):
        zs = near(r, 0)[0]
        arrived(kv_got.at[zs], fin_recv.at[zs])
    for h in range(heads):
        for m in range(halves):
            dk_out[m * hk : (m + 1) * hk, h * HEAD : (h + 1) * HEAD] = kv_got[h * halves + m, 0].astype(jnp.float32)
            dv_out[m * hk : (m + 1) * hk, h * HEAD : (h + 1) * HEAD] = kv_got[h * halves + m, 1].astype(jnp.float32)
    for n in range(1, nz):
        zs = near(n, 0)[0]
        arrived(wa_got.at[zs], wa_frecv.at[zs])
        w_out[:part_rows] += wa_got[zs].astype(jnp.float32)
        xs = near(0, n)[1]
        arrived(wb_got.at[xs], wb_frecv.at[xs])
        w_out[part_rows:] += wb_got[xs].astype(jnp.float32)

    for copy in sent:
        copy.wait_send()
    for r in range(1, wide // 2):
        x_on(r).wait_send()

    @pl.loop(0, tiles)
    def _(t):
        stat_copy(t).wait_send()

    @pl.loop(0, blocks)
    def _(n):
        @pl.when(n != me)
        def _():
            dq_copy(n).wait_send()

        @pl.when(away(n) == 2)
        def _():
            for i in range(2):
                opposite_copy(n, i).wait_send()

        for d, side in ((1, 0), (nx - 1, 1)):

            @pl.when(away(n) == d)
            def _():
                for i in range(2):
                    near_copy(n, side, i).wait_send()

        @pl.when((away(n) == 0) & (n != me))
        def _():
            fin_copy(n).wait_send()


def attention(blocks, wide, q, g, k, v, gate, x):
    rows, cols = k.shape
    heads = cols // HEAD
    nx = NX
    nz = blocks // nx
    halves = nz // heads
    hk = rows // halves
    sub = rows // nx
    tiles = blocks // 2
    vmem = pl.BlockSpec(memory_space=pltpu.VMEM)
    f32 = jnp.float32
    dma = pltpu.SemaphoreType.DMA
    span = x.shape[1] * wide // blocks
    part = span // 2
    grad = jax.ShapeDtypeStruct((rows, cols), f32)
    return pl.pallas_call(
        lambda *refs: kernel_body(heads, wide, *refs),
        out_shape=(grad, grad, grad, jax.ShapeDtypeStruct((span, cols), f32)),
        in_specs=[vmem] * 6,
        out_specs=(vmem,) * 4,
        scratch_shapes=[
            pltpu.VMEM((blocks, 2, hk, HEAD), LOW),
            pltpu.VMEM((blocks, 2, sub, HEAD), LOW),
            pltpu.VMEM((blocks, 8, HEAD), f32),
            pltpu.VMEM((tiles, HEAD, 2 * hk), LOW),
            pltpu.VMEM((blocks, hk, HEAD), f32),
            pltpu.VMEM((2, tiles, 2 * hk, 2 * sub), f32),
            pltpu.VMEM((2, tiles, 2 * hk, 2 * sub), f32),
            pltpu.VMEM((2, tiles, 8, 2 * sub), f32),
            pltpu.VMEM((tiles, 2 * hk, HEAD), f32),
            pltpu.VMEM((tiles, 2 * hk, HEAD), f32),
            pltpu.VMEM((tiles, 8, 2 * sub), f32),
            pltpu.VMEM((tiles, 8, 2 * sub), f32),
            pltpu.VMEM((blocks, sub, HEAD), LOW),
            pltpu.VMEM((blocks, 2, hk, HEAD), LOW),
            pltpu.VMEM((nz, 2, hk, HEAD), LOW),
            pltpu.VMEM((nz, 2, 2, hk, HEAD), LOW),
            pltpu.VMEM((nz, 2, hk, HEAD), LOW),
            pltpu.VMEM((nz, nx, sub, HEAD), LOW),
            pltpu.VMEM((nz, 2, hk, HEAD), LOW),
            pltpu.VMEM((wide, rows, x.shape[1]), LOW),
            pltpu.VMEM((rows, cols), LOW),
            pltpu.VMEM((nz, nx, part, cols), LOW),
            pltpu.VMEM((nz, nx, part, cols), LOW),
            pltpu.VMEM((nx, nz, part, cols), LOW),
            pltpu.VMEM((nz, nx, part, cols), LOW),
            pltpu.VMEM((nz, part, cols), f32),
            pltpu.VMEM((nx, part, cols), f32),
            pltpu.VMEM((nz, part, cols), LOW),
            pltpu.VMEM((nx, part, cols), LOW),
            pltpu.VMEM((nz, part, cols), LOW),
            pltpu.VMEM((nx, part, cols), LOW),
            dma((blocks, 2)), dma((nz, 2, 2)), dma((nz, 2)), dma((nz, 2)), dma((blocks, 2)), dma((heads, nx, 2)),
            dma((heads, nx, 2)), dma((nz, nx)), dma((blocks,)), dma((6,)),
            dma((tiles,)), dma((tiles,)), dma((blocks,)), dma((blocks,)), dma((blocks, 2)), dma((nz, 2)), dma((nz, 2, 2)),
            dma((nz,)), dma((nz,)),
            dma((wide // 2,)), dma((wide // 2,)), dma((wide,)),
            dma((nz, nx)), dma((nz, nx)), dma((nx, nz)), dma((nz, nx)),
            dma((nz,)), dma((nx,)), dma((nz,)), dma((nx,)),
        ],
        compiler_params=pltpu.CompilerParams(
            vmem_limit_bytes=62 * 1024 * 1024, collective_id=0, has_side_effects=True
        ),
        cost_estimate=pl.CostEstimate(
            flops=10 * blocks * blocks * rows * sub * HEAD, bytes_accessed=1 << 22, transcendentals=0
        ),
        name="attention",
    )(q, g, k, v, gate, x)


def local(queries, keys, values, forget_logits, layer_input, out_grad):
    rows = queries.shape[0]
    heads = queries.shape[1] // HEAD
    blocks = lax.axis_size("sp")
    wide = lax.axis_size("tp")
    gates = jnp.cumsum(jax.nn.log_sigmoid(forget_logits), axis=0).T * LOG2E
    totals = jnp.broadcast_to(gates[:, rows - 1 :, None], (heads, 8 - rows // HEAD, HEAD))
    gates = jnp.concatenate([gates.reshape(heads, rows // HEAD, HEAD), totals], axis=1)
    return attention(blocks, wide, queries, out_grad, keys, values, gates, layer_input)


def solution(mesh):
    spec = P("sp", "tp")
    return jax.shard_map(
        local, mesh=mesh, in_specs=(spec,) * 6, out_specs=(spec,) * 4, check_vma=False
    )
```

```python
import jax
import jax.numpy as jnp
from jax import lax
from jax.experimental import pallas as pl
from jax.experimental.pallas import tpu as pltpu
from jax.sharding import PartitionSpec as P

HEAD = 128
LOG2E = 1.4426950408889634
SCALE = HEAD ** (-0.5)
LOW = jnp.bfloat16
NX = 4


def nt(a, b):
    return lax.dot_general(a, b, (((1,), (1,)), ((), ())), preferred_element_type=jnp.float32)


def nn(a, b):
    return lax.dot_general(a, b, (((1,), (0,)), ((), ())), preferred_element_type=jnp.float32)


def kernel_body(
    heads, wide,
    q_hbm, g_hbm, k_hbm, v_hbm, logits_hbm, x_hbm,
    low_out, kv_out, w_out,
    q_in, g_in, k_in, v_in, logits, gate_in, w_sum, kv, qg, gates, kt, bias, wbuf, dpbuf, mrow, dk, dv, stat, stat_got,
    dq_stage, part_stage, mid, red, fin, dq_got, kv_got,
    x_all, low, wa_stage, wb_stage, wa_red, wb_red, wa_own, wb_own, wa_fin, wb_fin, wa_got, wb_got,
    in_sem, out_sem, kv_recv, xs_send, col_send, x2_send, qg_recv, q_send, qf_send, gate_send, gate_recv, local_sem,
    stat_send, stat_recv, dq_send, dq_recv, part_send, mid_recv, red_recv, fin_send, fin_recv,
    x_send, xf_send, x_recv, wa_send, wb_send, wa_recv, wb_recv, wa_fsend, wb_fsend, wa_frecv, wb_frecv,
):
    blocks, _, hk, _ = kv.shape
    nx = NX
    nz = blocks // nx
    halves = nz // heads
    sub = qg.shape[2]
    tiles = blocks // 2
    span = w_out.shape[0]
    part_rows = span // 2
    x_width = x_hbm.shape[1]
    column = lax.axis_index("tp")
    me = lax.axis_index("sp")
    z = me // nx
    x = lax.rem(me, nx)
    head = z // halves
    half = lax.rem(z, halves)

    def at(zt, xt):
        return zt * nx + xt

    def near(r, c):
        return lax.rem(z + r, nz), lax.rem(x + c, nx)

    def remote(src, dst, send, recv, target):
        return pltpu.make_async_remote_copy(
            src_ref=src, dst_ref=dst, send_sem=send, recv_sem=recv, device_id={"sp": target}
        )

    def arrived(ref, recv):
        remote(ref, ref, dq_send.at[0], recv, me).wait_recv()

    barrier = pltpu.get_barrier_semaphore()
    for r in range(1, blocks):
        pl.semaphore_signal(barrier, inc=1, device_id={"sp": lax.rem(me + r, blocks)})
    for r in range(1, wide):
        pl.semaphore_signal(barrier, inc=1, device_id={"tp": lax.rem(column + r, wide)})

    def lanes(h):
        return pl.ds(pl.multiple_of(h * HEAD, HEAD), HEAD)

    sent = []

    def go(copy):
        copy.start()
        sent.append(copy)

    kv_in = (k_in, v_in)
    qg_in = (q_in, g_in)

    def kv_source(i, zt):
        begin = pl.multiple_of(lax.rem(zt, halves) * hk, hk)
        return kv_in[i].at[pl.ds(begin, hk), lanes(zt // halves)]

    def q_source(i, zt, xt):
        begin = pl.multiple_of(xt * sub, sub)
        return qg_in[i].at[pl.ds(begin, sub), lanes(zt // halves)]

    loads = [
        pltpu.make_async_copy(src, dst, in_sem.at[n])
        for n, (src, dst) in enumerate(
            ((logits_hbm, logits), (k_hbm, k_in), (v_hbm, v_in), (q_hbm, q_in), (g_hbm, g_in), (x_hbm, x_all.at[column]))
        )
    ]
    for copy in loads:
        copy.start()

    @pl.loop(0, tiles)
    def _(j):
        dk[j] = jnp.zeros((2 * hk, HEAD), jnp.float32)
        dv[j] = jnp.zeros((2 * hk, HEAD), jnp.float32)

    loads[0].wait()
    chunks = logits.shape[1] // HEAD
    raw = jnp.concatenate(
        [logits[h : h + 1, u * HEAD : (u + 1) * HEAD] for h in range(heads) for u in range(chunks)], axis=0
    )
    logs = (jnp.minimum(raw, 0.0) - jnp.log1p(jnp.exp(-jnp.abs(raw)))) * LOG2E
    upto = lax.broadcasted_iota(jnp.int32, (HEAD, HEAD), 0) <= lax.broadcasted_iota(jnp.int32, (HEAD, HEAD), 1)
    sums = jnp.dot(
        logs, upto.astype(jnp.float32), precision=lax.Precision.HIGHEST, preferred_element_type=jnp.float32
    )
    for h in range(heads):
        base = jnp.zeros((1, HEAD), jnp.float32)
        for u in range(chunks):
            line = sums[h * chunks + u : h * chunks + u + 1]
            gate_in[h, u : u + 1] = line + base
            base = base + jnp.broadcast_to(line[:, HEAD - 1 :], (1, HEAD))
        gate_in[h, chunks:] = jnp.broadcast_to(base, (gate_in.shape[1] - chunks, HEAD))

    for copy in loads[1:]:
        copy.wait()
    own = [pltpu.make_async_copy(kv_source(i, z), kv.at[me, i], local_sem.at[i]) for i in range(2)]
    own += [pltpu.make_async_copy(q_source(i, z, x), qg.at[me, i], local_sem.at[2 + i]) for i in range(2)]
    own += [pltpu.make_async_copy(gate_in.at[head], gates.at[me], local_sem.at[4])]
    for copy in own:
        copy.start()
    for copy in own:
        copy.wait()
    pl.semaphore_wait(barrier, blocks + wide - 2)

    for r in range(nz):
        for c in range(nx):
            if (r, c) == (0, 0):
                continue
            zt, xt = near(r, c)
            go(remote(gate_in.at[zt // halves], gates.at[me], gate_send.at[r, c], gate_recv.at[me], at(zt, xt)))

    for d, c in ((0, 1), (1, nx - 1)):
        for i in range(2):
            go(remote(kv_source(i, z), kv.at[me, i], xs_send.at[0, d, i], kv_recv.at[me, i], at(z, near(0, c)[1])))
    for r in (1, nz - 1, 2):
        zt = near(r, 0)[0]
        for i in range(2):
            go(remote(kv_source(i, zt), kv.at[me, i], col_send.at[r, i], kv_recv.at[me, i], at(zt, x)))

    across = nz - 1 - z
    partner = z + 1 - 2 * half

    def q_plane(r):
        return z if r == 0 else across

    for i in range(2):
        go(remote(q_source(i, z, x), qg.at[me, i], qf_send.at[0, 0, i], qg_recv.at[me, i], at(partner, x)))
    for r in range(heads):
        for c in range(nx):
            if (r, c) == (0, 0):
                continue
            zt, xt = q_plane(r), near(0, c)[1]
            for i in range(2):
                go(remote(q_source(i, zt, xt), qg.at[me, i], q_send.at[r, c, i], qg_recv.at[me, i], at(zt, xt)))

    def x_copy(src, source, target, send):
        return pltpu.make_async_remote_copy(
            src_ref=src, dst_ref=x_all.at[source], send_sem=send, recv_sem=x_recv.at[source], device_id={"tp": target}
        )

    core = lax.rem(column, 2)
    twin = column + 1 - 2 * core
    for r in range(1, wide // 2):
        go(x_copy(x_all.at[column], column, lax.rem(column + 2 * r, wide), x_send.at[r]))
    go(x_copy(x_all.at[column], column, twin, x_send.at[0]))

    done = set()

    def kv_wait(r, c, i):
        if (r, c, i) in done:
            return
        done.add((r, c, i))
        j = at(*near(r, c))
        arrived(kv.at[j, i], kv_recv.at[j, i])

    def column_on(r):
        j = at(near(r, 0)[0], x)
        for i in range(2):
            kv_wait(r, 0, i)
            for d, c in ((0, 1), (1, nx - 1)):
                go(remote(kv.at[j, i], kv.at[j, i], xs_send.at[r, d, i], kv_recv.at[j, i], at(z, near(0, c)[1])))

    def second_on(r):
        for i, c in ((0, nx - 1), (1, 1)):
            kv_wait(r, c, i)
            j = at(*near(r, c))
            go(remote(kv.at[j, i], kv.at[j, i], x2_send.at[r, i], kv_recv.at[j, i], at(z, near(0, nx - c)[1])))

    def q_wait(j):
        for i in range(2):
            arrived(qg.at[j, i], qg_recv.at[j, i])

    def q_on(r, c):
        j = at(q_plane(r), near(0, c)[1])
        q_wait(j)
        for i in range(2):
            go(remote(qg.at[j, i], qg.at[j, i], qf_send.at[r, c, i], qg_recv.at[j, i], at(partner, x)))

    column_on(1)
    column_on(nz - 1)
    second_on(0)
    for c in range(1, nx):
        q_on(0, c)
    column_on(2)
    second_on(1)
    second_on(nz - 1)
    for c in range(nx):
        q_on(1, c)
    second_on(2)
    for r in range(nz):
        for c in range(nx):
            if (r, c) != (0, 0):
                j = at(*near(r, c))
                arrived(gates.at[j], gate_recv.at[j])

    def prepare(j, base):
        per = hk // HEAD
        table = gates[j]
        mine = table[0:per]
        for n in range(1, halves):
            mine = jnp.where(half == n, table[n * per : (n + 1) * per], mine)
        for n in range(per):
            row = mine[n : n + 1] + base
            bias[j, n * HEAD : (n + 1) * HEAD] = jnp.broadcast_to(row, (HEAD, HEAD)).T
        return base + table[halves * per : halves * per + 1]

    lax.fori_loop(0, blocks, prepare, jnp.zeros((1, HEAD), jnp.float32))
    for plane in (partner, nz - 1 - partner):
        for c in range(nx):
            q_wait(at(plane, near(0, c)[1]))
    for r in range(nz):
        for c in range(nx):
            if (r, c) != (0, 0):
                for i in range(2):
                    kv_wait(r, c, i)

    @pl.loop(0, tiles)
    def _(j):
        for n in range(2):
            kt[j, :, n * hk : (n + 1) * hk] = kv[2 * j + n, 0].T

    width = 2 * sub
    keys_wide = 2 * hk

    def forward(t):
        slot = lax.rem(t, 2)
        q = qg[pl.ds(2 * t, 2), 0].reshape(width, HEAD)
        g = qg[pl.ds(2 * t, 2), 1].reshape(width, HEAD)

        def block(j, state, mask):
            m, total, terms = state
            k = kv[pl.ds(2 * j, 2), 0].reshape(keys_wide, HEAD)
            v = kv[pl.ds(2 * j, 2), 1].reshape(keys_wide, HEAD)
            column_bias = bias[pl.ds(2 * j, 2)].reshape(keys_wide, HEAD)
            s = nt(k, q) * (SCALE * LOG2E) - jnp.concatenate([column_bias] * (width // HEAD), axis=1)
            if mask is not None:
                s = jnp.where(mask, s, -1e30)
            top = jnp.maximum(m, jnp.max(s, axis=0, keepdims=True))
            w = jnp.exp2(s - top)
            old = jnp.exp2(m - top)
            dp = nt(v, g)
            wbuf[slot, j] = w
            dpbuf[slot, j] = dp
            mrow[slot, j] = jnp.broadcast_to(top, (8, width))
            total = total * old + jnp.sum(w, axis=0, keepdims=True)
            terms = terms * old + jnp.sum(w * dp, axis=0, keepdims=True)
            return top, total, terms

        zero = jnp.zeros((1, width), jnp.float32)
        state = lax.fori_loop(
            0, t, lambda j, state: block(j, state, None), (jnp.full((1, width), -1e30, jnp.float32), zero, zero)
        )
        rows = halves * hk
        key_row = lax.broadcasted_iota(jnp.int32, (keys_wide, width), 0)
        query_row = lax.broadcasted_iota(jnp.int32, (keys_wide, width), 1)
        key_pos = jnp.where(key_row >= hk, key_row - hk + rows, key_row) + half * hk
        query_pos = jnp.where(query_row >= sub, query_row - sub + rows, query_row) + x * sub
        m, total, terms = block(t, state, key_pos <= query_pos)
        stat[t] = jnp.concatenate([m, total, terms, jnp.zeros((5, width), jnp.float32)], axis=0)

    def backward(t):
        slot = lax.rem(t, 2)
        q = qg[pl.ds(2 * t, 2), 0].reshape(width, HEAD)
        g = qg[pl.ds(2 * t, 2), 1].reshape(width, HEAD)
        arrived(stat_got.at[t], stat_recv.at[t])
        mine = stat[t]
        other = stat_got[t]
        top = jnp.maximum(mine[0:1], other[0:1])
        scale_mine = jnp.exp2(mine[0:1] - top)
        scale_other = jnp.exp2(other[0:1] - top)
        inverse = 1.0 / (mine[1:2] * scale_mine + other[1:2] * scale_other)
        terms = (mine[2:3] * scale_mine + other[2:3] * scale_other) * inverse

        def block(j, acc):
            factor = jnp.exp2(mrow[slot, j][0:1] - top) * inverse
            prob = wbuf[slot, j] * factor
            ds = (prob * (dpbuf[slot, j] - terms)).astype(LOW)
            dv[j] += nn(prob.astype(LOW), g)
            dk[j] += nn(ds, q)
            return acc + nn(kt[j], ds)

        acc = block(t, jnp.zeros((HEAD, width), jnp.float32))
        for n in range(2):
            part_stage[2 * t + n, 0] = (dk[t, n * hk : (n + 1) * hk] * SCALE).astype(LOW)
            part_stage[2 * t + n, 1] = dv[t, n * hk : (n + 1) * hk].astype(LOW)
        acc = lax.fori_loop(0, t, block, acc)
        dq_t = (acc * SCALE).T.astype(LOW)
        for n in range(2):
            dq_stage[2 * t + n] = dq_t[n * sub : (n + 1) * sub]

    def stat_copy(t):
        return remote(stat.at[t], stat_got.at[t], stat_send.at[t], stat_recv.at[t], at(partner, x))

    def dq_copy(n):
        return remote(dq_stage.at[n], dq_got.at[z, x], dq_send.at[n], dq_recv.at[me], n)

    def away(n):
        return lax.rem(lax.rem(n, nx) + nx - x, nx)

    def opposite_copy(n, i):
        xt = lax.rem(x + (1 if i == 0 else nx - 1), nx)
        return remote(part_stage.at[n, i], mid.at[n // nx, i], part_send.at[n, i], mid_recv.at[n // nx, i], at(z, xt))

    def near_copy(n, side, i):
        return remote(
            part_stage.at[n, i], red.at[n // nx, side, i], part_send.at[n, i], red_recv.at[n // nx, side, i],
            at(z, lax.rem(n, nx)),
        )

    def first_sends(tile):
        for u in range(2):
            n = 2 * tile + u

            @pl.when(away(n) == 2)
            def _():
                opposite_copy(n, 0).start()
                opposite_copy(n, 1).start()

            @pl.when(away(n) == 1)
            def _():
                near_copy(n, 0, 1).start()

            @pl.when(away(n) == nx - 1)
            def _():
                near_copy(n, 1, 0).start()

    def add_on_way(tile):
        for u in range(2):
            n = 2 * tile + u
            zn = n // nx
            for i, d in ((0, 1), (1, nx - 1)):

                @pl.when(away(n) == d)
                def _():
                    arrived(mid.at[zn, i], mid_recv.at[zn, i])
                    value = dk[tile, u * hk : (u + 1) * hk] * SCALE if i == 0 else dv[tile, u * hk : (u + 1) * hk]
                    part_stage[n, i] = (value + mid[zn, i].astype(jnp.float32)).astype(LOW)

    def second_sends(tile):
        for u in range(2):
            n = 2 * tile + u

            @pl.when(away(n) == 1)
            def _():
                near_copy(n, 0, 0).start()

            @pl.when(away(n) == nx - 1)
            def _():
                near_copy(n, 1, 1).start()

    def reduce(tile):
        for u in range(2):
            n = 2 * tile + u

            @pl.when(away(n) == 0)
            def _():
                zn = n // nx
                for i in range(2):
                    for side in range(2):
                        arrived(red.at[zn, side, i], red_recv.at[zn, side, i])
                    value = dk[tile, u * hk : (u + 1) * hk] * SCALE if i == 0 else dv[tile, u * hk : (u + 1) * hk]
                    for side in range(2):
                        value = value + red[zn, side, i].astype(jnp.float32)
                    fin[zn, i] = value.astype(LOW)

    def fin_sends(tile):
        for u in range(2):
            n = 2 * tile + u

            @pl.when((away(n) == 0) & (n == me))
            def _():
                kv_got[z] = fin[n // nx]

            @pl.when((away(n) == 0) & (n != me))
            def _():
                fin_copy(n).start()

    def dq_sends(tile):
        for u in range(2):
            n = 2 * tile + u

            @pl.when(n == me)
            def _():
                dq_got[z, x] = dq_stage[n]

            @pl.when(n != me)
            def _():
                dq_copy(n).start()

    def fin_copy(n):
        return remote(fin.at[n // nx], kv_got.at[z], fin_send.at[n // nx], fin_recv.at[z], n)

    def x_on(r):
        return x_copy(
            x_all.at[lax.rem(column + 2 * r, wide)], lax.rem(column + 2 * r, wide), twin, xf_send.at[r]
        )

    def step(s, carry):
        t = tiles - 1 - s

        def stage(offset, work):
            pl.when((t + offset >= 0) & (t + offset < tiles))(lambda: work(t + offset))

        stage(0, forward)
        stage(2, dq_sends)
        stage(3, second_sends)
        stage(5, fin_sends)
        stage(0, lambda tile: stat_copy(tile).start())
        stage(1, backward)
        stage(1, first_sends)
        stage(2, add_on_way)
        stage(4, reduce)

        @pl.when(s == 2)
        def _():
            for r in range(1, wide // 2):
                source = lax.rem(column + 2 * r, wide)
                pltpu.make_async_remote_copy(
                    src_ref=x_all.at[source], dst_ref=x_all.at[source], send_sem=xf_send.at[r],
                    recv_sem=x_recv.at[source], device_id={"tp": twin},
                ).wait_recv()
                x_on(r).start()

        return carry

    lax.fori_loop(0, tiles + 2, step, 0)
    second_sends(0)
    fin_sends(2)

    for r in range(nz):
        for c in range(nx):
            if (r, c) != (0, 0):
                zs, xs = near(r, c)
                arrived(dq_got.at[zs, xs], dq_recv.at[at(zs, xs)])
    for h in range(heads):
        for n in range(nx):
            value = dq_got[h * halves, n].astype(jnp.float32)
            for m in range(1, halves):
                value = value + dq_got[h * halves + m, n].astype(jnp.float32)
            low[n * sub : (n + 1) * sub, h * HEAD : (h + 1) * HEAD] = value.astype(LOW)
    low_copy = pltpu.make_async_copy(low, low_out, out_sem.at[0])
    reduce(1)
    for r in range(wide // 2):
        source = lax.rem(twin + 2 * r, wide)
        pltpu.make_async_remote_copy(
            src_ref=x_all.at[source], dst_ref=x_all.at[source], send_sem=x_send.at[0],
            recv_sem=x_recv.at[source], device_id={"tp": twin},
        ).wait_recv()

    def term(c):
        begin = c * span
        xs = x_all[begin // x_width, :, pl.ds(pl.multiple_of(lax.rem(begin, x_width), span), span)]
        return lax.dot_general(xs, low[...], (((0,), (0,)), ((), ())), preferred_element_type=jnp.float32)

    waiting = []

    def flush():
        for copy in waiting:
            go(copy)
        waiting.clear()

    order = [(r, c) for r in range(1, nz) for c in range(1, nx)]
    order += [(0, c) for c in range(1, nx)] + [(r, 0) for r in range(1, nz)] + [(0, 0)]
    for r, c in order:
        zt, xt = near(r, c)
        value = term(at(zt, xt))
        fresh = []
        if c:
            wa_stage[r, c] = value[:part_rows].astype(LOW)
            fresh.append(
                remote(wa_stage.at[r, c], wa_red.at[x, zt], wa_send.at[r, c], wa_recv.at[x, zt], at(z, xt))
            )
        else:
            wa_own[r] = value[:part_rows]
        if r:
            wb_stage[r, c] = value[part_rows:].astype(LOW)
            fresh.append(
                remote(wb_stage.at[r, c], wb_red.at[z, xt], wb_send.at[r, c], wb_recv.at[z, xt], at(zt, x))
            )
        else:
            wb_own[c] = value[part_rows:]
        flush()
        waiting.extend(fresh)
    flush()
    low_copy.start()
    fin_sends(1)
    reduce(0)

    for n in list(range(1, nz)) + [0]:
        zt = near(n, 0)[0]
        value = wa_own[n]
        for c in range(1, nx):
            xs = near(0, c)[1]
            arrived(wa_red.at[xs, zt], wa_recv.at[xs, zt])
            value = value + wa_red[xs, zt].astype(jnp.float32)
        fresh = []
        if n:
            wa_fin[n] = value.astype(LOW)
            fresh.append(remote(wa_fin.at[n], wa_got.at[z], wa_fsend.at[n], wa_frecv.at[z], at(zt, x)))
        else:
            w_sum[:part_rows] = value
        xt = near(0, n)[1]
        value = wb_own[n]
        for r in range(1, nz):
            zs = near(r, 0)[0]
            arrived(wb_red.at[zs, xt], wb_recv.at[zs, xt])
            value = value + wb_red[zs, xt].astype(jnp.float32)
        if n:
            wb_fin[n] = value.astype(LOW)
            fresh.append(remote(wb_fin.at[n], wb_got.at[x], wb_fsend.at[n], wb_frecv.at[x], at(z, xt)))
        else:
            w_sum[part_rows:] = value
        flush()
        waiting.extend(fresh)
    flush()

    fin_sends(0)
    for r in range(1, nz):
        zs = near(r, 0)[0]
        arrived(kv_got.at[zs], fin_recv.at[zs])
    kv_copy = pltpu.make_async_copy(kv_got, kv_out, out_sem.at[1])
    kv_copy.start()
    for n in range(1, nz):
        zs = near(n, 0)[0]
        arrived(wa_got.at[zs], wa_frecv.at[zs])
        w_sum[:part_rows] += wa_got[zs].astype(jnp.float32)
        xs = near(0, n)[1]
        arrived(wb_got.at[xs], wb_frecv.at[xs])
        w_sum[part_rows:] += wb_got[xs].astype(jnp.float32)

    w_copy = pltpu.make_async_copy(w_sum, w_out, out_sem.at[2])
    w_copy.start()
    low_copy.wait()
    kv_copy.wait()
    for copy in sent:
        copy.wait_send()
    for r in range(1, wide // 2):
        x_on(r).wait_send()

    @pl.loop(0, tiles)
    def _(t):
        stat_copy(t).wait_send()

    @pl.loop(0, blocks)
    def _(n):
        @pl.when(n != me)
        def _():
            dq_copy(n).wait_send()

        @pl.when(away(n) == 2)
        def _():
            for i in range(2):
                opposite_copy(n, i).wait_send()

        for d, side in ((1, 0), (nx - 1, 1)):

            @pl.when(away(n) == d)
            def _():
                for i in range(2):
                    near_copy(n, side, i).wait_send()

        @pl.when((away(n) == 0) & (n != me))
        def _():
            fin_copy(n).wait_send()

    w_copy.wait()


def attention(blocks, wide, q, g, k, v, logits, x):
    rows, cols = k.shape
    heads = cols // HEAD
    nx = NX
    nz = blocks // nx
    halves = nz // heads
    hk = rows // halves
    sub = rows // nx
    tiles = blocks // 2
    anywhere = pl.BlockSpec(memory_space=pl.ANY)
    f32 = jnp.float32
    dma = pltpu.SemaphoreType.DMA
    span = x.shape[1] * wide // blocks
    part = span // 2
    return pl.pallas_call(
        lambda *refs: kernel_body(heads, wide, *refs),
        out_shape=(
            jax.ShapeDtypeStruct((rows, cols), LOW),
            jax.ShapeDtypeStruct((nz, 2, hk, HEAD), LOW),
            jax.ShapeDtypeStruct((span, cols), f32),
        ),
        in_specs=[anywhere] * 6,
        out_specs=(anywhere,) * 3,
        scratch_shapes=[
            pltpu.VMEM((rows, cols), LOW),
            pltpu.VMEM((rows, cols), LOW),
            pltpu.VMEM((rows, cols), LOW),
            pltpu.VMEM((rows, cols), LOW),
            pltpu.VMEM((heads, rows), f32),
            pltpu.VMEM((heads, 8, HEAD), f32),
            pltpu.VMEM((span, cols), f32),
            pltpu.VMEM((blocks, 2, hk, HEAD), LOW),
            pltpu.VMEM((blocks, 2, sub, HEAD), LOW),
            pltpu.VMEM((blocks, 8, HEAD), f32),
            pltpu.VMEM((tiles, HEAD, 2 * hk), LOW),
            pltpu.VMEM((blocks, hk, HEAD), f32),
            pltpu.VMEM((2, tiles, 2 * hk, 2 * sub), f32),
            pltpu.VMEM((2, tiles, 2 * hk, 2 * sub), f32),
            pltpu.VMEM((2, tiles, 8, 2 * sub), f32),
            pltpu.VMEM((tiles, 2 * hk, HEAD), f32),
            pltpu.VMEM((tiles, 2 * hk, HEAD), f32),
            pltpu.VMEM((tiles, 8, 2 * sub), f32),
            pltpu.VMEM((tiles, 8, 2 * sub), f32),
            pltpu.VMEM((blocks, sub, HEAD), LOW),
            pltpu.VMEM((blocks, 2, hk, HEAD), LOW),
            pltpu.VMEM((nz, 2, hk, HEAD), LOW),
            pltpu.VMEM((nz, 2, 2, hk, HEAD), LOW),
            pltpu.VMEM((nz, 2, hk, HEAD), LOW),
            pltpu.VMEM((nz, nx, sub, HEAD), LOW),
            pltpu.VMEM((nz, 2, hk, HEAD), LOW),
            pltpu.VMEM((wide, rows, x.shape[1]), LOW),
            pltpu.VMEM((rows, cols), LOW),
            pltpu.VMEM((nz, nx, part, cols), LOW),
            pltpu.VMEM((nz, nx, part, cols), LOW),
            pltpu.VMEM((nx, nz, part, cols), LOW),
            pltpu.VMEM((nz, nx, part, cols), LOW),
            pltpu.VMEM((nz, part, cols), f32),
            pltpu.VMEM((nx, part, cols), f32),
            pltpu.VMEM((nz, part, cols), LOW),
            pltpu.VMEM((nx, part, cols), LOW),
            pltpu.VMEM((nz, part, cols), LOW),
            pltpu.VMEM((nx, part, cols), LOW),
            dma((6,)), dma((3,)),
            dma((blocks, 2)), dma((nz, 2, 2)), dma((nz, 2)), dma((nz, 2)), dma((blocks, 2)), dma((heads, nx, 2)),
            dma((heads, nx, 2)), dma((nz, nx)), dma((blocks,)), dma((6,)),
            dma((tiles,)), dma((tiles,)), dma((blocks,)), dma((blocks,)), dma((blocks, 2)), dma((nz, 2)), dma((nz, 2, 2)),
            dma((nz,)), dma((nz,)),
            dma((wide // 2,)), dma((wide // 2,)), dma((wide,)),
            dma((nz, nx)), dma((nz, nx)), dma((nx, nz)), dma((nz, nx)),
            dma((nz,)), dma((nx,)), dma((nz,)), dma((nx,)),
        ],
        compiler_params=pltpu.CompilerParams(
            vmem_limit_bytes=62 * 1024 * 1024, collective_id=0, has_side_effects=True
        ),
        cost_estimate=pl.CostEstimate(
            flops=10 * blocks * blocks * rows * sub * HEAD, bytes_accessed=1 << 22, transcendentals=0
        ),
        name="attention",
    )(q, g, k, v, logits, x)


def finish_body(
    heads, low_hbm, kv_hbm, w_hbm, dq_out, dk_out, dv_out, w_out, low, kv, w, dq, dk, dv, in_sem, out_sem
):
    halves = kv.shape[0] // heads
    hk = kv.shape[2]
    loads = [
        pltpu.make_async_copy(src, dst, in_sem.at[n])
        for n, (src, dst) in enumerate(((low_hbm, low), (kv_hbm, kv), (w_hbm, w)))
    ]
    for copy in loads:
        copy.start()
    stores = [
        pltpu.make_async_copy(src, dst, out_sem.at[n])
        for n, (src, dst) in enumerate(((dq, dq_out), (dk, dk_out), (dv, dv_out), (w, w_out)))
    ]
    loads[0].wait()
    dq[...] = low[...].astype(jnp.float32)
    stores[0].start()
    loads[1].wait()
    for i, grad in enumerate((dk, dv)):
        for h in range(heads):
            for m in range(halves):
                grad[m * hk : (m + 1) * hk, h * HEAD : (h + 1) * HEAD] = kv[h * halves + m, i].astype(jnp.float32)
        stores[1 + i].start()
    loads[2].wait()
    stores[3].start()
    for copy in stores:
        copy.wait()


def finish(heads, low, kv, w):
    anywhere = pl.BlockSpec(memory_space=pl.ANY)
    f32 = jnp.float32
    grad = jax.ShapeDtypeStruct(low.shape, f32)
    return pl.pallas_call(
        lambda *refs: finish_body(heads, *refs),
        out_shape=(grad, grad, grad, jax.ShapeDtypeStruct(w.shape, f32)),
        in_specs=[anywhere] * 3,
        out_specs=(anywhere,) * 4,
        scratch_shapes=[
            pltpu.VMEM(low.shape, LOW), pltpu.VMEM(kv.shape, LOW), pltpu.VMEM(w.shape, f32),
            pltpu.VMEM(low.shape, f32), pltpu.VMEM(low.shape, f32), pltpu.VMEM(low.shape, f32),
            pltpu.SemaphoreType.DMA((3,)), pltpu.SemaphoreType.DMA((4,)),
        ],
        compiler_params=pltpu.CompilerParams(vmem_limit_bytes=62 * 1024 * 1024),
        name="finish",
    )(low, kv, w)


def local(queries, keys, values, forget_logits, layer_input, out_grad):
    heads = queries.shape[1] // HEAD
    blocks = lax.axis_size("sp")
    wide = lax.axis_size("tp")
    pieces = attention(blocks, wide, queries, out_grad, keys, values, forget_logits.T, layer_input)
    return finish(heads, *pieces)


def solution(mesh):
    spec = P("sp", "tp")
    return jax.shard_map(
        local, mesh=mesh, in_specs=(spec,) * 6, out_specs=(spec,) * 4, check_vma=False
    )
```

```python
import jax
import jax.numpy as jnp
from jax import lax
from jax.experimental import pallas as pl
from jax.experimental.pallas import tpu as pltpu
from jax.sharding import PartitionSpec as P

HEAD = 128
LOG2E = 1.4426950408889634
SCALE = HEAD ** (-0.5)
LOW = jnp.bfloat16
NX = 4


def nt(a, b):
    return lax.dot_general(a, b, (((1,), (1,)), ((), ())), preferred_element_type=jnp.float32)


def nn(a, b):
    return lax.dot_general(a, b, (((1,), (0,)), ((), ())), preferred_element_type=jnp.float32)


def kernel_body(
    heads, wide,
    q_hbm, g_hbm, k_hbm, v_hbm, logits_hbm, x_hbm,
    low_out, kv_out, w_out,
    q_in, g_in, k_in, v_in, logits, gate_in, w_sum, kv, qg, gates, kt, bias, wbuf, mrow, dk, dv, stat, stat_got,
    dq_stage, part_stage, mid, red, fin, dq_got, kv_got,
    x_all, low, wa_stage, wb_stage, wa_red, wb_red, wa_own, wb_own, wa_fin, wb_fin, wa_got, wb_got,
    in_sem, out_sem, kv_recv, xs_send, col_send, x2_send, qg_recv, q_send, qf_send, gate_send, gate_recv, local_sem,
    stat_send, stat_recv, dq_send, dq_recv, part_send, mid_recv, red_recv, fin_send, fin_recv,
    x_send, xf_send, x_recv, wa_send, wb_send, wa_recv, wb_recv, wa_fsend, wb_fsend, wa_frecv, wb_frecv,
):
    blocks, _, hk, _ = kv.shape
    nx = NX
    nz = blocks // nx
    halves = nz // heads
    sub = qg.shape[2]
    tiles = blocks // 2
    span = w_out.shape[0]
    part_rows = span // 2
    x_width = x_hbm.shape[1]
    column = lax.axis_index("tp")
    me = lax.axis_index("sp")
    z = me // nx
    x = lax.rem(me, nx)
    head = z // halves
    half = lax.rem(z, halves)

    def at(zt, xt):
        return zt * nx + xt

    def near(r, c):
        return lax.rem(z + r, nz), lax.rem(x + c, nx)

    def remote(src, dst, send, recv, target):
        return pltpu.make_async_remote_copy(
            src_ref=src, dst_ref=dst, send_sem=send, recv_sem=recv, device_id={"sp": target}
        )

    def arrived(ref, recv):
        remote(ref, ref, dq_send.at[0], recv, me).wait_recv()

    barrier = pltpu.get_barrier_semaphore()
    for r in range(1, blocks):
        pl.semaphore_signal(barrier, inc=1, device_id={"sp": lax.rem(me + r, blocks)})
    for r in range(1, wide):
        pl.semaphore_signal(barrier, inc=1, device_id={"tp": lax.rem(column + r, wide)})

    def lanes(h):
        return pl.ds(pl.multiple_of(h * HEAD, HEAD), HEAD)

    sent = []

    def go(copy):
        copy.start()
        sent.append(copy)

    kv_in = (k_in, v_in)
    qg_in = (q_in, g_in)

    def kv_source(i, zt):
        begin = pl.multiple_of(lax.rem(zt, halves) * hk, hk)
        return kv_in[i].at[pl.ds(begin, hk), lanes(zt // halves)]

    def q_source(i, zt, xt):
        begin = pl.multiple_of(xt * sub, sub)
        return qg_in[i].at[pl.ds(begin, sub), lanes(zt // halves)]

    loads = [
        pltpu.make_async_copy(src, dst, in_sem.at[n])
        for n, (src, dst) in enumerate(
            ((logits_hbm, logits), (k_hbm, k_in), (v_hbm, v_in), (q_hbm, q_in), (g_hbm, g_in), (x_hbm, x_all.at[column]))
        )
    ]
    for copy in loads:
        copy.start()

    width = 2 * sub
    keys_wide = 2 * hk
    line = lax.broadcasted_iota(jnp.int32, (8, width), 0)

    @pl.loop(0, tiles)
    def _(j):
        dk[j] = jnp.zeros((keys_wide, HEAD), jnp.float32)
        dv[j] = jnp.zeros((keys_wide, HEAD), jnp.float32)
        stat[j] = jnp.where(line == 0, -1e30, 0.0)

    loads[0].wait()
    chunks = logits.shape[1] // HEAD
    raw = jnp.concatenate(
        [logits[h : h + 1, u * HEAD : (u + 1) * HEAD] for h in range(heads) for u in range(chunks)], axis=0
    )
    logs = (jnp.minimum(raw, 0.0) - jnp.log1p(jnp.exp(-jnp.abs(raw)))) * LOG2E
    upto = lax.broadcasted_iota(jnp.int32, (HEAD, HEAD), 0) <= lax.broadcasted_iota(jnp.int32, (HEAD, HEAD), 1)
    sums = jnp.dot(
        logs, upto.astype(jnp.float32), precision=lax.Precision.HIGHEST, preferred_element_type=jnp.float32
    )
    for h in range(heads):
        base = jnp.zeros((1, HEAD), jnp.float32)
        for u in range(chunks):
            line = sums[h * chunks + u : h * chunks + u + 1]
            gate_in[h, u : u + 1] = line + base
            base = base + jnp.broadcast_to(line[:, HEAD - 1 :], (1, HEAD))
        gate_in[h, chunks:] = jnp.broadcast_to(base, (gate_in.shape[1] - chunks, HEAD))

    for copy in loads[1:]:
        copy.wait()
    own = [pltpu.make_async_copy(kv_source(i, z), kv.at[me, i], local_sem.at[i]) for i in range(2)]
    own += [pltpu.make_async_copy(q_source(i, z, x), qg.at[me, i], local_sem.at[2 + i]) for i in range(2)]
    own += [pltpu.make_async_copy(gate_in.at[head], gates.at[me], local_sem.at[4])]
    for copy in own:
        copy.start()
    for copy in own:
        copy.wait()
    pl.semaphore_wait(barrier, blocks + wide - 2)

    for r in range(nz):
        for c in range(nx):
            if (r, c) == (0, 0):
                continue
            zt, xt = near(r, c)
            go(remote(gate_in.at[zt // halves], gates.at[me], gate_send.at[r, c], gate_recv.at[me], at(zt, xt)))

    for r in (1, nz - 1, 2):
        zt = near(r, 0)[0]
        for i in range(2):
            go(remote(kv_source(i, zt), kv.at[me, i], col_send.at[r, i], kv_recv.at[me, i], at(zt, x)))

    across = nz - 1 - z
    partner = z + 1 - 2 * half

    def q_plane(r):
        return z if r == 0 else across

    for i in range(2):
        go(remote(q_source(i, z, x), qg.at[me, i], qf_send.at[0, 0, i], qg_recv.at[me, i], at(partner, x)))
    for r in range(heads):
        for c in range(nx):
            if (r, c) == (0, 0):
                continue
            zt, xt = q_plane(r), near(0, c)[1]
            for i in range(2):
                go(remote(q_source(i, zt, xt), qg.at[me, i], q_send.at[r, c, i], qg_recv.at[me, i], at(zt, xt)))

    def x_copy(src, source, target, send):
        return pltpu.make_async_remote_copy(
            src_ref=src, dst_ref=x_all.at[source], send_sem=send, recv_sem=x_recv.at[source], device_id={"tp": target}
        )

    core = lax.rem(column, 2)
    twin = column + 1 - 2 * core
    for r in range(1, wide // 2):
        go(x_copy(x_all.at[column], column, lax.rem(column + 2 * r, wide), x_send.at[r]))
    go(x_copy(x_all.at[column], column, twin, x_send.at[0]))

    def kv_arrived(j, i):
        arrived(kv.at[j, i], kv_recv.at[j, i])

    def round_copy(p, c, i):
        j = at(p, x)
        return remote(kv.at[j, i], kv.at[j, i], xs_send.at[p, c // 2, i], kv_recv.at[j, i], at(z, near(0, c)[1]))

    def onward_copy(p, i):
        c = nx - 1 if i == 0 else 1
        j = at(p, near(0, c)[1])
        return remote(kv.at[j, i], kv.at[j, i], x2_send.at[p, i], kv_recv.at[j, i], at(z, near(0, nx - c)[1]))

    def column_on(p):
        @pl.when(z != p)
        def _():
            for i in range(2):
                kv_arrived(at(p, x), i)

        for i in range(2):
            for c in (1, nx - 1):
                round_copy(p, c, i).start()

    def second_on(p):
        for i, c in ((0, nx - 1), (1, 1)):
            kv_arrived(at(p, near(0, c)[1]), i)
            onward_copy(p, i).start()

    def q_wait(j):
        for i in range(2):
            arrived(qg.at[j, i], qg_recv.at[j, i])

    def q_on(r, c):
        j = at(q_plane(r), near(0, c)[1])
        q_wait(j)
        for i in range(2):
            go(remote(qg.at[j, i], qg.at[j, i], qf_send.at[r, c, i], qg_recv.at[j, i], at(partner, x)))

    column_on(0)
    column_on(1)
    for c in range(1, nx):
        q_on(0, c)
    second_on(0)
    column_on(2)
    column_on(3)
    for c in range(nx):
        q_on(1, c)
    second_on(1)
    for r in range(nz):
        for c in range(nx):
            if (r, c) != (0, 0):
                j = at(*near(r, c))
                arrived(gates.at[j], gate_recv.at[j])

    def prepare(j, base):
        per = hk // HEAD
        table = gates[j]
        mine = table[0:per]
        for n in range(1, halves):
            mine = jnp.where(half == n, table[n * per : (n + 1) * per], mine)
        for n in range(per):
            row = mine[n : n + 1] + base
            bias[j, n * HEAD : (n + 1) * HEAD] = jnp.broadcast_to(row, (HEAD, HEAD)).T
        return base + table[halves * per : halves * per + 1]

    lax.fori_loop(0, blocks, prepare, jnp.zeros((1, HEAD), jnp.float32))
    for plane in (partner, nz - 1 - partner):
        for c in range(nx):
            q_wait(at(plane, near(0, c)[1]))

    rows = halves * hk
    key_row = lax.broadcasted_iota(jnp.int32, (keys_wide, width), 0)
    query_row = lax.broadcasted_iota(jnp.int32, (keys_wide, width), 1)
    key_pos = jnp.where(key_row >= hk, key_row - hk + rows, key_row) + half * hk
    query_pos = jnp.where(query_row >= sub, query_row - sub + rows, query_row) + x * sub

    def pair(i, j):
        return kv[pl.ds(2 * j, 2), i].reshape(keys_wide, HEAD)

    def queries(i, t):
        return qg[pl.ds(2 * t, 2), i].reshape(width, HEAD)

    def place(t, j):
        return t * (t + 1) // 2 + j

    def scores(t, j, masked):
        state = stat[t]
        m, total, terms = state[0:1], state[1:2], state[2:3]
        column_bias = bias[pl.ds(2 * j, 2)].reshape(keys_wide, HEAD)
        s = nt(pair(0, j), queries(0, t)) * (SCALE * LOG2E) - jnp.concatenate([column_bias] * (width // HEAD), axis=1)
        if masked:
            s = jnp.where(key_pos <= query_pos, s, -1e30)
        top = jnp.maximum(m, jnp.max(s, axis=0, keepdims=True))
        w = jnp.exp2(s - top)
        old = jnp.exp2(m - top)
        dp = nt(pair(1, j), queries(1, t))
        wbuf[place(t, j)] = w
        mrow[place(t, j)] = jnp.broadcast_to(top, (8, width))
        total = total * old + jnp.sum(w, axis=0, keepdims=True)
        terms = terms * old + jnp.sum(w * dp, axis=0, keepdims=True)
        stat[t] = jnp.concatenate([top, total, terms, jnp.zeros((5, width), jnp.float32)], axis=0)

    def forward(j, carry):
        for u in range(2):
            b = 2 * j + u
            d = lax.rem(lax.rem(b, nx) + nx - x, nx)

            @pl.when((d == 1) | (d == 2))
            def _():
                kv_arrived(b, 0)

            @pl.when((d == nx - 1) | (d == 2))
            def _():
                kv_arrived(b, 1)

        for n in range(2):
            kt[j, :, n * hk : (n + 1) * hk] = kv[2 * j + n, 0].T
        scores(j, j, True)

        @pl.loop(j + 1, tiles)
        def _(t):
            scores(t, j, False)

        @pl.when(j < tiles - 1)
        def _():
            stat_copy(j).start()

        @pl.when(j < 2)
        def _():
            second_on(j + 2)

        return carry

    def backward(t):
        q, g = queries(0, t), queries(1, t)
        arrived(stat_got.at[t], stat_recv.at[t])
        mine = stat[t]
        other = stat_got[t]
        top = jnp.maximum(mine[0:1], other[0:1])
        scale_mine = jnp.exp2(mine[0:1] - top)
        scale_other = jnp.exp2(other[0:1] - top)
        inverse = 1.0 / (mine[1:2] * scale_mine + other[1:2] * scale_other)
        terms = (mine[2:3] * scale_mine + other[2:3] * scale_other) * inverse

        def block(j, acc):
            factor = jnp.exp2(mrow[place(t, j)][0:1] - top) * inverse
            prob = wbuf[place(t, j)] * factor
            ds = (prob * (nt(pair(1, j), g) - terms)).astype(LOW)
            dv[j] += nn(prob.astype(LOW), g)
            dk[j] += nn(ds, q)
            return acc + nn(kt[j], ds)

        acc = block(t, jnp.zeros((HEAD, width), jnp.float32))
        for n in range(2):
            part_stage[2 * t + n, 0] = (dk[t, n * hk : (n + 1) * hk] * SCALE).astype(LOW)
            part_stage[2 * t + n, 1] = dv[t, n * hk : (n + 1) * hk].astype(LOW)
        acc = lax.fori_loop(0, t, block, acc)
        dq_t = (acc * SCALE).T.astype(LOW)
        for n in range(2):
            dq_stage[2 * t + n] = dq_t[n * sub : (n + 1) * sub]

    def stat_copy(t):
        return remote(stat.at[t], stat_got.at[t], stat_send.at[t], stat_recv.at[t], at(partner, x))

    def dq_copy(n):
        return remote(dq_stage.at[n], dq_got.at[z, x], dq_send.at[n], dq_recv.at[me], n)

    def away(n):
        return lax.rem(lax.rem(n, nx) + nx - x, nx)

    def opposite_copy(n, i):
        xt = lax.rem(x + (1 if i == 0 else nx - 1), nx)
        return remote(part_stage.at[n, i], mid.at[n // nx, i], part_send.at[n, i], mid_recv.at[n // nx, i], at(z, xt))

    def near_copy(n, side, i):
        return remote(
            part_stage.at[n, i], red.at[n // nx, side, i], part_send.at[n, i], red_recv.at[n // nx, side, i],
            at(z, lax.rem(n, nx)),
        )

    def first_sends(tile):
        for u in range(2):
            n = 2 * tile + u

            @pl.when(away(n) == 2)
            def _():
                opposite_copy(n, 0).start()
                opposite_copy(n, 1).start()

            @pl.when(away(n) == 1)
            def _():
                near_copy(n, 0, 1).start()

            @pl.when(away(n) == nx - 1)
            def _():
                near_copy(n, 1, 0).start()

    def add_on_way(tile):
        for u in range(2):
            n = 2 * tile + u
            zn = n // nx
            for i, d in ((0, 1), (1, nx - 1)):

                @pl.when(away(n) == d)
                def _():
                    arrived(mid.at[zn, i], mid_recv.at[zn, i])
                    value = dk[tile, u * hk : (u + 1) * hk] * SCALE if i == 0 else dv[tile, u * hk : (u + 1) * hk]
                    part_stage[n, i] = (value + mid[zn, i].astype(jnp.float32)).astype(LOW)

    def second_sends(tile):
        for u in range(2):
            n = 2 * tile + u

            @pl.when(away(n) == 1)
            def _():
                near_copy(n, 0, 0).start()

            @pl.when(away(n) == nx - 1)
            def _():
                near_copy(n, 1, 1).start()

    def reduce(tile):
        for u in range(2):
            n = 2 * tile + u

            @pl.when(away(n) == 0)
            def _():
                zn = n // nx
                for i in range(2):
                    for side in range(2):
                        arrived(red.at[zn, side, i], red_recv.at[zn, side, i])
                    value = dk[tile, u * hk : (u + 1) * hk] * SCALE if i == 0 else dv[tile, u * hk : (u + 1) * hk]
                    for side in range(2):
                        value = value + red[zn, side, i].astype(jnp.float32)
                    fin[zn, i] = value.astype(LOW)

    def fin_sends(tile):
        for u in range(2):
            n = 2 * tile + u

            @pl.when((away(n) == 0) & (n == me))
            def _():
                kv_got[z] = fin[n // nx]

            @pl.when((away(n) == 0) & (n != me))
            def _():
                fin_copy(n).start()

    def dq_sends(tile):
        for u in range(2):
            n = 2 * tile + u

            @pl.when(n == me)
            def _():
                dq_got[z, x] = dq_stage[n]

            @pl.when(n != me)
            def _():
                dq_copy(n).start()

    def fin_copy(n):
        return remote(fin.at[n // nx], kv_got.at[z], fin_send.at[n // nx], fin_recv.at[z], n)

    def x_on(r):
        return x_copy(
            x_all.at[lax.rem(column + 2 * r, wide)], lax.rem(column + 2 * r, wide), twin, xf_send.at[r]
        )

    lax.fori_loop(0, tiles, forward, 0)

    for r in range(1, wide // 2):
        source = lax.rem(column + 2 * r, wide)
        pltpu.make_async_remote_copy(
            src_ref=x_all.at[source], dst_ref=x_all.at[source], send_sem=xf_send.at[r],
            recv_sem=x_recv.at[source], device_id={"tp": twin},
        ).wait_recv()
        x_on(r).start()
    stat_copy(tiles - 1).start()

    def step(s, carry):
        t = tiles - 1 - s

        def stage(offset, work):
            pl.when((t + offset >= 0) & (t + offset < tiles))(lambda: work(t + offset))

        stage(1, dq_sends)
        stage(3, second_sends)
        stage(5, fin_sends)
        stage(0, backward)
        stage(0, first_sends)
        stage(2, add_on_way)
        stage(4, reduce)
        return carry

    lax.fori_loop(0, tiles + 1, step, 0)
    second_sends(1)
    fin_sends(3)
    add_on_way(0)

    for r in range(nz):
        for c in range(nx):
            if (r, c) != (0, 0):
                zs, xs = near(r, c)
                arrived(dq_got.at[zs, xs], dq_recv.at[at(zs, xs)])
    for h in range(heads):
        for n in range(nx):
            value = dq_got[h * halves, n].astype(jnp.float32)
            for m in range(1, halves):
                value = value + dq_got[h * halves + m, n].astype(jnp.float32)
            low[n * sub : (n + 1) * sub, h * HEAD : (h + 1) * HEAD] = value.astype(LOW)
    low_copy = pltpu.make_async_copy(low, low_out, out_sem.at[0])
    second_sends(0)
    reduce(2)
    for r in range(wide // 2):
        source = lax.rem(twin + 2 * r, wide)
        pltpu.make_async_remote_copy(
            src_ref=x_all.at[source], dst_ref=x_all.at[source], send_sem=x_send.at[0],
            recv_sem=x_recv.at[source], device_id={"tp": twin},
        ).wait_recv()

    def term(c):
        begin = c * span
        xs = x_all[begin // x_width, :, pl.ds(pl.multiple_of(lax.rem(begin, x_width), span), span)]
        return lax.dot_general(xs, low[...], (((0,), (0,)), ((), ())), preferred_element_type=jnp.float32)

    waiting = []

    def flush():
        for copy in waiting:
            go(copy)
        waiting.clear()

    order = [(r, c) for r in range(1, nz) for c in range(1, nx)]
    order += [(0, c) for c in range(1, nx)] + [(r, 0) for r in range(1, nz)] + [(0, 0)]
    for r, c in order:
        zt, xt = near(r, c)
        value = term(at(zt, xt))
        fresh = []
        if c:
            wa_stage[r, c] = value[:part_rows].astype(LOW)
            fresh.append(
                remote(wa_stage.at[r, c], wa_red.at[x, zt], wa_send.at[r, c], wa_recv.at[x, zt], at(z, xt))
            )
        else:
            wa_own[r] = value[:part_rows]
        if r:
            wb_stage[r, c] = value[part_rows:].astype(LOW)
            fresh.append(
                remote(wb_stage.at[r, c], wb_red.at[z, xt], wb_send.at[r, c], wb_recv.at[z, xt], at(zt, x))
            )
        else:
            wb_own[c] = value[part_rows:]
        flush()
        waiting.extend(fresh)
    flush()
    low_copy.start()
    fin_sends(2)
    reduce(1)

    for n in list(range(1, nz)) + [0]:
        zt = near(n, 0)[0]
        value = wa_own[n]
        for c in range(1, nx):
            xs = near(0, c)[1]
            arrived(wa_red.at[xs, zt], wa_recv.at[xs, zt])
            value = value + wa_red[xs, zt].astype(jnp.float32)
        fresh = []
        if n:
            wa_fin[n] = value.astype(LOW)
            fresh.append(remote(wa_fin.at[n], wa_got.at[z], wa_fsend.at[n], wa_frecv.at[z], at(zt, x)))
        else:
            w_sum[:part_rows] = value
        xt = near(0, n)[1]
        value = wb_own[n]
        for r in range(1, nz):
            zs = near(r, 0)[0]
            arrived(wb_red.at[zs, xt], wb_recv.at[zs, xt])
            value = value + wb_red[zs, xt].astype(jnp.float32)
        if n:
            wb_fin[n] = value.astype(LOW)
            fresh.append(remote(wb_fin.at[n], wb_got.at[x], wb_fsend.at[n], wb_frecv.at[x], at(z, xt)))
        else:
            w_sum[part_rows:] = value
        flush()
        waiting.extend(fresh)
    flush()

    fin_sends(1)
    reduce(0)
    fin_sends(0)
    for r in range(1, nz):
        zs = near(r, 0)[0]
        arrived(kv_got.at[zs], fin_recv.at[zs])
    kv_copy = pltpu.make_async_copy(kv_got, kv_out, out_sem.at[1])
    kv_copy.start()
    for n in range(1, nz):
        zs = near(n, 0)[0]
        arrived(wa_got.at[zs], wa_frecv.at[zs])
        w_sum[:part_rows] += wa_got[zs].astype(jnp.float32)
        xs = near(0, n)[1]
        arrived(wb_got.at[xs], wb_frecv.at[xs])
        w_sum[part_rows:] += wb_got[xs].astype(jnp.float32)

    w_copy = pltpu.make_async_copy(w_sum, w_out, out_sem.at[2])
    w_copy.start()
    low_copy.wait()
    kv_copy.wait()
    for copy in sent:
        copy.wait_send()
    for r in range(1, wide // 2):
        x_on(r).wait_send()

    @pl.loop(0, nz)
    def _(p):
        for i in range(2):
            for c in (1, nx - 1):
                round_copy(p, c, i).wait_send()
            onward_copy(p, i).wait_send()

    @pl.loop(0, tiles)
    def _(t):
        stat_copy(t).wait_send()

    @pl.loop(0, blocks)
    def _(n):
        @pl.when(n != me)
        def _():
            dq_copy(n).wait_send()

        @pl.when(away(n) == 2)
        def _():
            for i in range(2):
                opposite_copy(n, i).wait_send()

        for d, side in ((1, 0), (nx - 1, 1)):

            @pl.when(away(n) == d)
            def _():
                for i in range(2):
                    near_copy(n, side, i).wait_send()

        @pl.when((away(n) == 0) & (n != me))
        def _():
            fin_copy(n).wait_send()

    w_copy.wait()


def attention(blocks, wide, q, g, k, v, logits, x):
    rows, cols = k.shape
    heads = cols // HEAD
    nx = NX
    nz = blocks // nx
    halves = nz // heads
    hk = rows // halves
    sub = rows // nx
    tiles = blocks // 2
    anywhere = pl.BlockSpec(memory_space=pl.ANY)
    f32 = jnp.float32
    dma = pltpu.SemaphoreType.DMA
    span = x.shape[1] * wide // blocks
    part = span // 2
    return pl.pallas_call(
        lambda *refs: kernel_body(heads, wide, *refs),
        out_shape=(
            jax.ShapeDtypeStruct((rows, cols), LOW),
            jax.ShapeDtypeStruct((nz, 2, hk, HEAD), LOW),
            jax.ShapeDtypeStruct((span, cols), f32),
        ),
        in_specs=[anywhere] * 6,
        out_specs=(anywhere,) * 3,
        scratch_shapes=[
            pltpu.VMEM((rows, cols), LOW),
            pltpu.VMEM((rows, cols), LOW),
            pltpu.VMEM((rows, cols), LOW),
            pltpu.VMEM((rows, cols), LOW),
            pltpu.VMEM((heads, rows), f32),
            pltpu.VMEM((heads, 8, HEAD), f32),
            pltpu.VMEM((span, cols), f32),
            pltpu.VMEM((blocks, 2, hk, HEAD), LOW),
            pltpu.VMEM((blocks, 2, sub, HEAD), LOW),
            pltpu.VMEM((blocks, 8, HEAD), f32),
            pltpu.VMEM((tiles, HEAD, 2 * hk), LOW),
            pltpu.VMEM((blocks, hk, HEAD), f32),
            pltpu.VMEM((tiles * (tiles + 1) // 2, 2 * hk, 2 * sub), f32),
            pltpu.VMEM((tiles * (tiles + 1) // 2, 8, 2 * sub), f32),
            pltpu.VMEM((tiles, 2 * hk, HEAD), f32),
            pltpu.VMEM((tiles, 2 * hk, HEAD), f32),
            pltpu.VMEM((tiles, 8, 2 * sub), f32),
            pltpu.VMEM((tiles, 8, 2 * sub), f32),
            pltpu.VMEM((blocks, sub, HEAD), LOW),
            pltpu.VMEM((blocks, 2, hk, HEAD), LOW),
            pltpu.VMEM((nz, 2, hk, HEAD), LOW),
            pltpu.VMEM((nz, 2, 2, hk, HEAD), LOW),
            pltpu.VMEM((nz, 2, hk, HEAD), LOW),
            pltpu.VMEM((nz, nx, sub, HEAD), LOW),
            pltpu.VMEM((nz, 2, hk, HEAD), LOW),
            pltpu.VMEM((wide, rows, x.shape[1]), LOW),
            pltpu.VMEM((rows, cols), LOW),
            pltpu.VMEM((nz, nx, part, cols), LOW),
            pltpu.VMEM((nz, nx, part, cols), LOW),
            pltpu.VMEM((nx, nz, part, cols), LOW),
            pltpu.VMEM((nz, nx, part, cols), LOW),
            pltpu.VMEM((nz, part, cols), f32),
            pltpu.VMEM((nx, part, cols), f32),
            pltpu.VMEM((nz, part, cols), LOW),
            pltpu.VMEM((nx, part, cols), LOW),
            pltpu.VMEM((nz, part, cols), LOW),
            pltpu.VMEM((nx, part, cols), LOW),
            dma((6,)), dma((3,)),
            dma((blocks, 2)), dma((nz, 2, 2)), dma((nz, 2)), dma((nz, 2)), dma((blocks, 2)), dma((heads, nx, 2)),
            dma((heads, nx, 2)), dma((nz, nx)), dma((blocks,)), dma((6,)),
            dma((tiles,)), dma((tiles,)), dma((blocks,)), dma((blocks,)), dma((blocks, 2)), dma((nz, 2)), dma((nz, 2, 2)),
            dma((nz,)), dma((nz,)),
            dma((wide // 2,)), dma((wide // 2,)), dma((wide,)),
            dma((nz, nx)), dma((nz, nx)), dma((nx, nz)), dma((nz, nx)),
            dma((nz,)), dma((nx,)), dma((nz,)), dma((nx,)),
        ],
        compiler_params=pltpu.CompilerParams(
            vmem_limit_bytes=62 * 1024 * 1024, collective_id=0, has_side_effects=True
        ),
        cost_estimate=pl.CostEstimate(
            flops=10 * blocks * blocks * rows * sub * HEAD, bytes_accessed=1 << 22, transcendentals=0
        ),
        name="attention",
    )(q, g, k, v, logits, x)


def finish_body(
    heads, low_hbm, kv_hbm, w_hbm, dq_out, dk_out, dv_out, w_out, low, kv, w, dq, dk, dv, in_sem, out_sem
):
    halves = kv.shape[0] // heads
    hk = kv.shape[2]
    loads = [
        pltpu.make_async_copy(src, dst, in_sem.at[n])
        for n, (src, dst) in enumerate(((low_hbm, low), (kv_hbm, kv), (w_hbm, w)))
    ]
    for copy in loads:
        copy.start()
    stores = [
        pltpu.make_async_copy(src, dst, out_sem.at[n])
        for n, (src, dst) in enumerate(((dq, dq_out), (dk, dk_out), (dv, dv_out), (w, w_out)))
    ]
    loads[0].wait()
    dq[...] = low[...].astype(jnp.float32)
    stores[0].start()
    loads[1].wait()
    for i, grad in enumerate((dk, dv)):
        for h in range(heads):
            for m in range(halves):
                grad[m * hk : (m + 1) * hk, h * HEAD : (h + 1) * HEAD] = kv[h * halves + m, i].astype(jnp.float32)
        stores[1 + i].start()
    loads[2].wait()
    stores[3].start()
    for copy in stores:
        copy.wait()


def finish(heads, low, kv, w):
    anywhere = pl.BlockSpec(memory_space=pl.ANY)
    f32 = jnp.float32
    grad = jax.ShapeDtypeStruct(low.shape, f32)
    return pl.pallas_call(
        lambda *refs: finish_body(heads, *refs),
        out_shape=(grad, grad, grad, jax.ShapeDtypeStruct(w.shape, f32)),
        in_specs=[anywhere] * 3,
        out_specs=(anywhere,) * 4,
        scratch_shapes=[
            pltpu.VMEM(low.shape, LOW), pltpu.VMEM(kv.shape, LOW), pltpu.VMEM(w.shape, f32),
            pltpu.VMEM(low.shape, f32), pltpu.VMEM(low.shape, f32), pltpu.VMEM(low.shape, f32),
            pltpu.SemaphoreType.DMA((3,)), pltpu.SemaphoreType.DMA((4,)),
        ],
        compiler_params=pltpu.CompilerParams(vmem_limit_bytes=62 * 1024 * 1024),
        name="finish",
    )(low, kv, w)


def local(queries, keys, values, forget_logits, layer_input, out_grad):
    heads = queries.shape[1] // HEAD
    blocks = lax.axis_size("sp")
    wide = lax.axis_size("tp")
    pieces = attention(blocks, wide, queries, out_grad, keys, values, forget_logits.T, layer_input)
    return finish(heads, *pieces)


def solution(mesh):
    spec = P("sp", "tp")
    return jax.shard_map(
        local, mesh=mesh, in_specs=(spec,) * 6, out_specs=(spec,) * 4, check_vma=False
    )
```

```python
import jax
import jax.numpy as jnp
from jax import lax
from jax.experimental import pallas as pl
from jax.experimental.pallas import tpu as pltpu
from jax.sharding import PartitionSpec as P

HEAD = 128
LOG2E = 1.4426950408889634
SCALE = HEAD ** (-0.5)
LOW = jnp.bfloat16
NX = 4


def nt(a, b):
    return lax.dot_general(a, b, (((1,), (1,)), ((), ())), preferred_element_type=jnp.float32)


def nn(a, b):
    return lax.dot_general(a, b, (((1,), (0,)), ((), ())), preferred_element_type=jnp.float32)


def kernel_body(
    heads, wide,
    q_hbm, g_hbm, k_hbm, v_hbm, logits_hbm, x_hbm,
    low_out, kv_out, w_out,
    q_in, g_in, k_in, v_in, logits, gate_in, w_sum, kv, qg, gates, kt, bias, wbuf, mrow, grads, stat, stat_got,
    dq_stage, part_stage, mid, red, fin, dq_got, kv_got,
    x_all, low, wa_stage, wb_stage, wa_red, wb_red, wa_own, wb_own, wa_fin, wb_fin, wa_got, wb_got,
    in_sem, out_sem, kv_recv, xs_send, col_send, x2_send, qg_recv, q_send, qf_send, gate_send, gate_recv, local_sem,
    stat_send, stat_recv, dq_send, dq_recv, part_send, mid_recv, red_recv, fin_send, fin_recv,
    x_send, xf_send, x_recv, wa_send, wb_send, wa_recv, wb_recv, wa_fsend, wb_fsend, wa_frecv, wb_frecv,
):
    blocks, _, hk, _ = kv.shape
    nx = NX
    nz = blocks // nx
    halves = nz // heads
    sub = qg.shape[2]
    tiles = blocks // 2
    span = w_out.shape[0]
    part_rows = span // 2
    x_width = x_hbm.shape[1]
    column = lax.axis_index("tp")
    me = lax.axis_index("sp")
    z = me // nx
    x = lax.rem(me, nx)
    head = z // halves
    half = lax.rem(z, halves)

    def at(zt, xt):
        return zt * nx + xt

    def near(r, c):
        return lax.rem(z + r, nz), lax.rem(x + c, nx)

    def remote(src, dst, send, recv, target):
        return pltpu.make_async_remote_copy(
            src_ref=src, dst_ref=dst, send_sem=send, recv_sem=recv, device_id={"sp": target}
        )

    def arrived(ref, recv):
        remote(ref, ref, dq_send.at[0], recv, me).wait_recv()

    barrier = pltpu.get_barrier_semaphore()
    for r in range(1, blocks):
        pl.semaphore_signal(barrier, inc=1, device_id={"sp": lax.rem(me + r, blocks)})
    for r in range(1, wide):
        pl.semaphore_signal(barrier, inc=1, device_id={"tp": lax.rem(column + r, wide)})

    def lanes(h):
        return pl.ds(pl.multiple_of(h * HEAD, HEAD), HEAD)

    sent = []

    def go(copy):
        copy.start()
        sent.append(copy)

    kv_in = (k_in, v_in)
    qg_in = (q_in, g_in)

    def kv_source(i, zt):
        begin = pl.multiple_of(lax.rem(zt, halves) * hk, hk)
        return kv_in[i].at[pl.ds(begin, hk), lanes(zt // halves)]

    def q_source(i, zt, xt):
        begin = pl.multiple_of(xt * sub, sub)
        return qg_in[i].at[pl.ds(begin, sub), lanes(zt // halves)]

    loads = [
        pltpu.make_async_copy(src, dst, in_sem.at[n])
        for n, (src, dst) in enumerate(
            ((logits_hbm, logits), (k_hbm, k_in), (v_hbm, v_in), (q_hbm, q_in), (g_hbm, g_in), (x_hbm, x_all.at[column]))
        )
    ]
    for copy in loads:
        copy.start()

    width = 2 * sub
    keys_wide = 2 * hk
    line = lax.broadcasted_iota(jnp.int32, (8, width), 0)

    @pl.loop(0, tiles)
    def _(j):
        grads[0, j] = jnp.zeros((keys_wide, HEAD), jnp.float32)
        grads[1, j] = jnp.zeros((keys_wide, HEAD), jnp.float32)
        stat[j] = jnp.where(line == 0, -1e30, 0.0)

    loads[0].wait()
    chunks = logits.shape[1] // HEAD
    raw = jnp.concatenate(
        [logits[h : h + 1, u * HEAD : (u + 1) * HEAD] for h in range(heads) for u in range(chunks)], axis=0
    )
    logs = (jnp.minimum(raw, 0.0) - jnp.log1p(jnp.exp(-jnp.abs(raw)))) * LOG2E
    upto = lax.broadcasted_iota(jnp.int32, (HEAD, HEAD), 0) <= lax.broadcasted_iota(jnp.int32, (HEAD, HEAD), 1)
    sums = jnp.dot(
        logs, upto.astype(jnp.float32), precision=lax.Precision.HIGHEST, preferred_element_type=jnp.float32
    )
    for h in range(heads):
        base = jnp.zeros((1, HEAD), jnp.float32)
        for u in range(chunks):
            line = sums[h * chunks + u : h * chunks + u + 1]
            gate_in[h, u : u + 1] = line + base
            base = base + jnp.broadcast_to(line[:, HEAD - 1 :], (1, HEAD))
        gate_in[h, chunks:] = jnp.broadcast_to(base, (gate_in.shape[1] - chunks, HEAD))

    for copy in loads[1:]:
        copy.wait()
    own = [pltpu.make_async_copy(kv_source(i, z), kv.at[me, i], local_sem.at[i]) for i in range(2)]
    own += [pltpu.make_async_copy(q_source(i, z, x), qg.at[me, i], local_sem.at[2 + i]) for i in range(2)]
    own += [pltpu.make_async_copy(gate_in.at[head], gates.at[me], local_sem.at[4])]
    for copy in own:
        copy.start()
    for copy in own:
        copy.wait()
    pl.semaphore_wait(barrier, blocks + wide - 2)

    for r in range(nz):
        for c in range(nx):
            if (r, c) == (0, 0):
                continue
            zt, xt = near(r, c)
            go(remote(gate_in.at[zt // halves], gates.at[me], gate_send.at[r, c], gate_recv.at[me], at(zt, xt)))

    def kv_arrived(j, i):
        arrived(kv.at[j, i], kv_recv.at[j, i])

    def round_copy(p, c, i):
        j = at(p, x)
        return remote(kv.at[j, i], kv.at[j, i], xs_send.at[p, c // 2, i], kv_recv.at[j, i], at(z, near(0, c)[1]))

    for i in range(2):
        for c in (1, nx - 1):
            round_copy(z, c, i).start()

    for r in (1, nz - 1, 2):
        zt = near(r, 0)[0]
        for i in range(2):
            go(remote(kv_source(i, zt), kv.at[me, i], col_send.at[r, i], kv_recv.at[me, i], at(zt, x)))

    across = nz - 1 - z
    partner = z + 1 - 2 * half

    def q_plane(r):
        return z if r == 0 else across

    for i in range(2):
        go(remote(q_source(i, z, x), qg.at[me, i], qf_send.at[0, 0, i], qg_recv.at[me, i], at(partner, x)))
    for r in range(heads):
        for c in range(nx):
            if (r, c) == (0, 0):
                continue
            zt, xt = q_plane(r), near(0, c)[1]
            for i in range(2):
                go(remote(q_source(i, zt, xt), qg.at[me, i], q_send.at[r, c, i], qg_recv.at[me, i], at(zt, xt)))

    def x_copy(src, source, target, send):
        return pltpu.make_async_remote_copy(
            src_ref=src, dst_ref=x_all.at[source], send_sem=send, recv_sem=x_recv.at[source], device_id={"tp": target}
        )

    core = lax.rem(column, 2)
    twin = column + 1 - 2 * core
    for r in range(1, wide // 2):
        go(x_copy(x_all.at[column], column, lax.rem(column + 2 * r, wide), x_send.at[r]))
    go(x_copy(x_all.at[column], column, twin, x_send.at[0]))

    def onward_copy(p, i):
        c = nx - 1 if i == 0 else 1
        j = at(p, near(0, c)[1])
        return remote(kv.at[j, i], kv.at[j, i], x2_send.at[p, i], kv_recv.at[j, i], at(z, near(0, nx - c)[1]))

    def column_on(r):
        p = near(r, 0)[0]
        for i in range(2):
            kv_arrived(at(p, x), i)
            for c in (1, nx - 1):
                round_copy(p, c, i).start()

    def second_on(p):
        for i, c in ((0, nx - 1), (1, 1)):
            kv_arrived(at(p, near(0, c)[1]), i)
            onward_copy(p, i).start()

    def q_wait(j):
        for i in range(2):
            arrived(qg.at[j, i], qg_recv.at[j, i])

    def q_on(r, c):
        j = at(q_plane(r), near(0, c)[1])
        q_wait(j)
        for i in range(2):
            go(remote(qg.at[j, i], qg.at[j, i], qf_send.at[r, c, i], qg_recv.at[j, i], at(partner, x)))

    column_on(1)
    column_on(nz - 1)
    for c in range(1, nx):
        if c == 2:
            column_on(2)
        q_on(0, c)
    second_on(0)
    second_on(1)
    for c in range(nx):
        q_on(1, c)
    for r in range(nz):
        for c in range(nx):
            if (r, c) != (0, 0):
                j = at(*near(r, c))
                arrived(gates.at[j], gate_recv.at[j])

    def prepare(j, base):
        per = hk // HEAD
        table = gates[j]
        mine = table[0:per]
        for n in range(1, halves):
            mine = jnp.where(half == n, table[n * per : (n + 1) * per], mine)
        for n in range(per):
            row = mine[n : n + 1] + base
            bias[j, n * HEAD : (n + 1) * HEAD] = jnp.broadcast_to(row, (HEAD, HEAD)).T
        return base + table[halves * per : halves * per + 1]

    lax.fori_loop(0, blocks, prepare, jnp.zeros((1, HEAD), jnp.float32))
    second_on(2)
    second_on(3)

    rows = halves * hk
    key_row = lax.broadcasted_iota(jnp.int32, (keys_wide, width), 0)
    query_row = lax.broadcasted_iota(jnp.int32, (keys_wide, width), 1)
    key_pos = jnp.where(key_row >= hk, key_row - hk + rows, key_row) + half * hk
    query_pos = jnp.where(query_row >= sub, query_row - sub + rows, query_row) + x * sub

    def pair(i, j):
        return kv[pl.ds(2 * j, 2), i].reshape(keys_wide, HEAD)

    def queries(i, t):
        return qg[pl.ds(2 * t, 2), i].reshape(width, HEAD)

    def place(t, j):
        return t * (t + 1) // 2 + j

    def scores(t, j):
        state = stat[t]
        m, total, terms = state[0:1], state[1:2], state[2:3]
        column_bias = bias[pl.ds(2 * j, 2)].reshape(keys_wide, HEAD)
        s = nt(pair(0, j), queries(0, t)) * (SCALE * LOG2E) - jnp.concatenate([column_bias] * (width // HEAD), axis=1)
        s = jnp.where(key_pos <= query_pos + (t - j) * (2 * rows), s, -1e30)
        top = jnp.maximum(m, jnp.max(s, axis=0, keepdims=True))
        w = jnp.exp2(s - top)
        old = jnp.exp2(m - top)
        dp = nt(pair(1, j), queries(1, t))
        wbuf[place(t, j)] = w
        mrow[place(t, j)] = jnp.broadcast_to(top, (8, width))
        total = total * old + jnp.sum(w, axis=0, keepdims=True)
        terms = terms * old + jnp.sum(w * dp, axis=0, keepdims=True)
        stat[t] = jnp.concatenate([top, total, terms, jnp.zeros((5, width), jnp.float32)], axis=0)

    def pair_wait(j):
        for u in range(2):
            b = 2 * j + u
            d = lax.rem(lax.rem(b, nx) + nx - x, nx)

            @pl.when((d == 1) | (d == 2))
            def _():
                kv_arrived(b, 0)

            @pl.when((d == nx - 1) | (d == 2))
            def _():
                kv_arrived(b, 1)

        for n in range(2):
            kt[j, :, n * hk : (n + 1) * hk] = kv[2 * j + n, 0].T

    outer = (z == 0) | (z == nz - 1)
    quarter = tiles // 4

    def group(direct, j):
        ends = outer if direct else jnp.logical_not(outer)

        @pl.loop(0, 2 * quarter)
        def _(m):
            t = jnp.where(ends, jnp.where(m >= quarter, m + 2 * quarter, m), m + quarter)

            @pl.when(t >= j)
            def _():
                scores(t, j)

    def backward(t):
        q, g = queries(0, t), queries(1, t)
        arrived(stat_got.at[t], stat_recv.at[t])
        mine = stat[t]
        other = stat_got[t]
        top = jnp.maximum(mine[0:1], other[0:1])
        scale_mine = jnp.exp2(mine[0:1] - top)
        scale_other = jnp.exp2(other[0:1] - top)
        inverse = 1.0 / (mine[1:2] * scale_mine + other[1:2] * scale_other)
        terms = (mine[2:3] * scale_mine + other[2:3] * scale_other) * inverse

        def block(j, acc):
            factor = jnp.exp2(mrow[place(t, j)][0:1] - top) * inverse
            prob = wbuf[place(t, j)] * factor
            ds = (prob * (nt(pair(1, j), g) - terms)).astype(LOW)
            grads[1, j] += nn(prob.astype(LOW), g)
            grads[0, j] += nn(ds, q)
            return acc + nn(kt[j], ds)

        acc = block(t, jnp.zeros((HEAD, width), jnp.float32))
        for n, (u, i) in enumerate(((0, 0), (1, 0), (1, 1), (0, 1))):
            value = grads[i, t, u * hk : (u + 1) * hk]
            part_stage[t, n] = (value * SCALE if i == 0 else value).astype(LOW)
        acc = lax.fori_loop(0, t, block, acc)
        dq_t = (acc * SCALE).T.astype(LOW)
        for n in range(2):
            dq_stage[2 * t + n] = dq_t[n * sub : (n + 1) * sub]

    def stat_copy(t):
        return remote(stat.at[t], stat_got.at[t], stat_send.at[t], stat_recv.at[t], at(partner, x))

    def dq_copy(n):
        return remote(dq_stage.at[n], dq_got.at[z, x], dq_send.at[n], dq_recv.at[me], n)

    hr = hk // 2

    def role(tile):
        return lax.rem(x + nx - 2 * lax.rem(tile, nx // 2), nx)

    def array(tile, c):
        return lax.rem(role(tile) + c, nx)

    def share(tile, n, way):
        u = jnp.where((n == 1) | (n == 2), 1, 0)
        i = n // 2
        value = grads[i, tile, pl.ds(pl.multiple_of(u * hk + way * hr, hr), hr)]
        return value * jnp.where(i == 0, SCALE, 1.0)

    def half_of(tile, n, way):
        return part_stage.at[tile, n, pl.ds(way * hr, hr)]

    def opposite_copy(tile, way):
        n = array(tile, 2)
        return remote(
            half_of(tile, n, way), mid.at[tile, way], part_send.at[tile, n, way], mid_recv.at[tile, way],
            at(z, near(0, nx - 1 if way else 1)[1]),
        )

    def near_copy(tile, side, way):
        c = nx - 1 if side else 1
        n = array(tile, c)
        return remote(
            half_of(tile, n, way), red.at[tile, side, way], part_send.at[tile, n, way], red_recv.at[tile, side, way],
            at(z, near(0, c)[1]),
        )

    def first_sends(tile):
        for way in range(2):
            opposite_copy(tile, way).start()
        near_copy(tile, 0, 1).start()
        near_copy(tile, 1, 0).start()

    def add_on_way(tile):
        for way, c in ((0, 1), (1, nx - 1)):
            n = array(tile, c)
            arrived(mid.at[tile, way], mid_recv.at[tile, way])
            part_stage[tile, n, way * hr : (way + 1) * hr] = (
                share(tile, n, way) + mid[tile, way].astype(jnp.float32)
            ).astype(LOW)

    def second_sends(tile):
        near_copy(tile, 0, 0).start()
        near_copy(tile, 1, 1).start()

    def reduce(tile):
        n = array(tile, 0)
        for way in range(2):
            value = share(tile, n, way)
            for side in range(2):
                arrived(red.at[tile, side, way], red_recv.at[tile, side, way])
                value = value + red[tile, side, way].astype(jnp.float32)
            fin[tile, way * hr : (way + 1) * hr] = value.astype(LOW)

    def fin_owner(tile):
        n = array(tile, 0)
        return 2 * tile + jnp.where((n == 1) | (n == 2), 1, 0), n // 2

    def fin_copy(tile):
        owner, i = fin_owner(tile)
        return remote(fin.at[tile], kv_got.at[z, i], fin_send.at[tile], fin_recv.at[z, i], owner)

    def fin_sends(tile):
        owner, i = fin_owner(tile)

        @pl.when(owner == me)
        def _():
            kv_got[z, i] = fin[tile]

        @pl.when(owner != me)
        def _():
            fin_copy(tile).start()

    def dq_sends(tile):
        for u in range(2):
            n = 2 * tile + u

            @pl.when(n == me)
            def _():
                dq_got[z, x] = dq_stage[n]

            @pl.when(n != me)
            def _():
                dq_copy(n).start()

    def x_on(r):
        return x_copy(
            x_all.at[lax.rem(column + 2 * r, wide)], lax.rem(column + 2 * r, wide), twin, xf_send.at[r]
        )

    @pl.loop(0, tiles // 2)
    def _(j):
        pair_wait(j)
        group(True, j)

    for plane in (partner, nz - 1 - partner):
        for c in range(nx):
            q_wait(at(plane, near(0, c)[1]))

    @pl.loop(0, tiles // 2)
    def _(j):
        group(False, j)

    @pl.loop(tiles // 2, tiles)
    def _(j):
        pair_wait(j)

        @pl.loop(j, tiles)
        def _(t):
            scores(t, j)

        stat_copy(j - tiles // 2).start()

        @pl.when(j < tiles - 1)
        def _():
            stat_copy(j).start()

    for r in range(1, wide // 2):
        source = lax.rem(column + 2 * r, wide)
        pltpu.make_async_remote_copy(
            src_ref=x_all.at[source], dst_ref=x_all.at[source], send_sem=xf_send.at[r],
            recv_sem=x_recv.at[source], device_id={"tp": twin},
        ).wait_recv()
        x_on(r).start()
    stat_copy(tiles - 1).start()

    def step(s, carry):
        t = tiles - 1 - s

        def stage(offset, work):
            pl.when((t + offset >= 0) & (t + offset < tiles))(lambda: work(t + offset))

        stage(1, dq_sends)
        stage(3, second_sends)
        stage(5, fin_sends)
        stage(0, backward)
        stage(0, first_sends)
        stage(2, add_on_way)
        stage(4, reduce)
        return carry

    lax.fori_loop(0, tiles + 1, step, 0)
    second_sends(1)
    fin_sends(3)
    add_on_way(0)

    for r in range(nz):
        for c in range(nx):
            if (r, c) != (0, 0):
                zs, xs = near(r, c)
                arrived(dq_got.at[zs, xs], dq_recv.at[at(zs, xs)])
    for h in range(heads):
        for n in range(nx):
            value = dq_got[h * halves, n].astype(jnp.float32)
            for m in range(1, halves):
                value = value + dq_got[h * halves + m, n].astype(jnp.float32)
            low[n * sub : (n + 1) * sub, h * HEAD : (h + 1) * HEAD] = value.astype(LOW)
    low_copy = pltpu.make_async_copy(low, low_out, out_sem.at[0])
    second_sends(0)
    reduce(2)
    for r in range(wide // 2):
        source = lax.rem(twin + 2 * r, wide)
        pltpu.make_async_remote_copy(
            src_ref=x_all.at[source], dst_ref=x_all.at[source], send_sem=x_send.at[0],
            recv_sem=x_recv.at[source], device_id={"tp": twin},
        ).wait_recv()

    def term(c):
        begin = c * span
        xs = x_all[begin // x_width, :, pl.ds(pl.multiple_of(lax.rem(begin, x_width), span), span)]
        return lax.dot_general(xs, low[...], (((0,), (0,)), ((), ())), preferred_element_type=jnp.float32)

    waiting = []

    def flush():
        for copy in waiting:
            go(copy)
        waiting.clear()

    order = [(r, c) for r in range(1, nz) for c in range(1, nx)]
    order += [(0, c) for c in range(1, nx)] + [(r, 0) for r in range(1, nz)] + [(0, 0)]
    for r, c in order:
        zt, xt = near(r, c)
        value = term(at(zt, xt))
        fresh = []
        if c:
            wa_stage[r, c] = value[:part_rows].astype(LOW)
            fresh.append(
                remote(wa_stage.at[r, c], wa_red.at[x, zt], wa_send.at[r, c], wa_recv.at[x, zt], at(z, xt))
            )
        else:
            wa_own[r] = value[:part_rows]
        if r:
            wb_stage[r, c] = value[part_rows:].astype(LOW)
            fresh.append(
                remote(wb_stage.at[r, c], wb_red.at[z, xt], wb_send.at[r, c], wb_recv.at[z, xt], at(zt, x))
            )
        else:
            wb_own[c] = value[part_rows:]
        flush()
        waiting.extend(fresh)
    flush()
    low_copy.start()
    fin_sends(2)
    reduce(1)

    for n in list(range(1, nz)) + [0]:
        zt = near(n, 0)[0]
        value = wa_own[n]
        for c in range(1, nx):
            xs = near(0, c)[1]
            arrived(wa_red.at[xs, zt], wa_recv.at[xs, zt])
            value = value + wa_red[xs, zt].astype(jnp.float32)
        fresh = []
        if n:
            wa_fin[n] = value.astype(LOW)
            fresh.append(remote(wa_fin.at[n], wa_got.at[z], wa_fsend.at[n], wa_frecv.at[z], at(zt, x)))
        else:
            w_sum[:part_rows] = value
        xt = near(0, n)[1]
        value = wb_own[n]
        for r in range(1, nz):
            zs = near(r, 0)[0]
            arrived(wb_red.at[zs, xt], wb_recv.at[zs, xt])
            value = value + wb_red[zs, xt].astype(jnp.float32)
        if n:
            wb_fin[n] = value.astype(LOW)
            fresh.append(remote(wb_fin.at[n], wb_got.at[x], wb_fsend.at[n], wb_frecv.at[x], at(z, xt)))
        else:
            w_sum[part_rows:] = value
        flush()
        waiting.extend(fresh)
    flush()

    fin_sends(1)
    reduce(0)
    fin_sends(0)
    my_tile = me // 2
    for r in range(nz):
        zs = near(r, 0)[0]
        for i in range(2):
            if r == 0:
                owner, mine = fin_owner(my_tile)

                @pl.when(jnp.logical_not((owner == me) & (mine == i)))
                def _():
                    arrived(kv_got.at[zs, i], fin_recv.at[zs, i])
            else:
                arrived(kv_got.at[zs, i], fin_recv.at[zs, i])
    kv_copy = pltpu.make_async_copy(kv_got, kv_out, out_sem.at[1])
    kv_copy.start()
    for n in range(1, nz):
        zs = near(n, 0)[0]
        arrived(wa_got.at[zs], wa_frecv.at[zs])
        w_sum[:part_rows] += wa_got[zs].astype(jnp.float32)
        xs = near(0, n)[1]
        arrived(wb_got.at[xs], wb_frecv.at[xs])
        w_sum[part_rows:] += wb_got[xs].astype(jnp.float32)

    w_copy = pltpu.make_async_copy(w_sum, w_out, out_sem.at[2])
    w_copy.start()
    low_copy.wait()
    kv_copy.wait()
    for copy in sent:
        copy.wait_send()
    for r in range(1, wide // 2):
        x_on(r).wait_send()

    @pl.loop(0, nz)
    def _(p):
        for i in range(2):
            for c in (1, nx - 1):
                round_copy(p, c, i).wait_send()
            onward_copy(p, i).wait_send()

    @pl.loop(0, tiles)
    def _(t):
        stat_copy(t).wait_send()

    @pl.loop(0, blocks)
    def _(n):
        @pl.when(n != me)
        def _():
            dq_copy(n).wait_send()

    @pl.loop(0, tiles)
    def _(tile):
        for way in range(2):
            opposite_copy(tile, way).wait_send()
            for side in range(2):
                near_copy(tile, side, way).wait_send()

        @pl.when(fin_owner(tile)[0] != me)
        def _():
            fin_copy(tile).wait_send()

    w_copy.wait()


def attention(blocks, wide, q, g, k, v, logits, x):
    rows, cols = k.shape
    heads = cols // HEAD
    nx = NX
    nz = blocks // nx
    halves = nz // heads
    hk = rows // halves
    sub = rows // nx
    tiles = blocks // 2
    anywhere = pl.BlockSpec(memory_space=pl.ANY)
    f32 = jnp.float32
    dma = pltpu.SemaphoreType.DMA
    span = x.shape[1] * wide // blocks
    part = span // 2
    return pl.pallas_call(
        lambda *refs: kernel_body(heads, wide, *refs),
        out_shape=(
            jax.ShapeDtypeStruct((rows, cols), LOW),
            jax.ShapeDtypeStruct((nz, 2, hk, HEAD), LOW),
            jax.ShapeDtypeStruct((span, cols), f32),
        ),
        in_specs=[anywhere] * 6,
        out_specs=(anywhere,) * 3,
        scratch_shapes=[
            pltpu.VMEM((rows, cols), LOW),
            pltpu.VMEM((rows, cols), LOW),
            pltpu.VMEM((rows, cols), LOW),
            pltpu.VMEM((rows, cols), LOW),
            pltpu.VMEM((heads, rows), f32),
            pltpu.VMEM((heads, 8, HEAD), f32),
            pltpu.VMEM((span, cols), f32),
            pltpu.VMEM((blocks, 2, hk, HEAD), LOW),
            pltpu.VMEM((blocks, 2, sub, HEAD), LOW),
            pltpu.VMEM((blocks, 8, HEAD), f32),
            pltpu.VMEM((tiles, HEAD, 2 * hk), LOW),
            pltpu.VMEM((blocks, hk, HEAD), f32),
            pltpu.VMEM((tiles * (tiles + 1) // 2, 2 * hk, 2 * sub), f32),
            pltpu.VMEM((tiles * (tiles + 1) // 2, 8, 2 * sub), f32),
            pltpu.VMEM((2, tiles, 2 * hk, HEAD), f32),
            pltpu.VMEM((tiles, 8, 2 * sub), f32),
            pltpu.VMEM((tiles, 8, 2 * sub), f32),
            pltpu.VMEM((blocks, sub, HEAD), LOW),
            pltpu.VMEM((tiles, nx, hk, HEAD), LOW),
            pltpu.VMEM((tiles, 2, hk // 2, HEAD), LOW),
            pltpu.VMEM((tiles, 2, 2, hk // 2, HEAD), LOW),
            pltpu.VMEM((tiles, hk, HEAD), LOW),
            pltpu.VMEM((nz, nx, sub, HEAD), LOW),
            pltpu.VMEM((nz, 2, hk, HEAD), LOW),
            pltpu.VMEM((wide, rows, x.shape[1]), LOW),
            pltpu.VMEM((rows, cols), LOW),
            pltpu.VMEM((nz, nx, part, cols), LOW),
            pltpu.VMEM((nz, nx, part, cols), LOW),
            pltpu.VMEM((nx, nz, part, cols), LOW),
            pltpu.VMEM((nz, nx, part, cols), LOW),
            pltpu.VMEM((nz, part, cols), f32),
            pltpu.VMEM((nx, part, cols), f32),
            pltpu.VMEM((nz, part, cols), LOW),
            pltpu.VMEM((nx, part, cols), LOW),
            pltpu.VMEM((nz, part, cols), LOW),
            pltpu.VMEM((nx, part, cols), LOW),
            dma((6,)), dma((3,)),
            dma((blocks, 2)), dma((nz, 2, 2)), dma((nz, 2)), dma((nz, 2)), dma((blocks, 2)), dma((heads, nx, 2)),
            dma((heads, nx, 2)), dma((nz, nx)), dma((blocks,)), dma((6,)),
            dma((tiles,)), dma((tiles,)), dma((blocks,)), dma((blocks,)), dma((tiles, nx, 2)), dma((tiles, 2)),
            dma((tiles, 2, 2)), dma((tiles,)), dma((nz, 2)),
            dma((wide // 2,)), dma((wide // 2,)), dma((wide,)),
            dma((nz, nx)), dma((nz, nx)), dma((nx, nz)), dma((nz, nx)),
            dma((nz,)), dma((nx,)), dma((nz,)), dma((nx,)),
        ],
        compiler_params=pltpu.CompilerParams(
            vmem_limit_bytes=62 * 1024 * 1024, collective_id=0, has_side_effects=True
        ),
        cost_estimate=pl.CostEstimate(
            flops=10 * blocks * blocks * rows * sub * HEAD, bytes_accessed=1 << 22, transcendentals=0
        ),
        name="attention",
    )(q, g, k, v, logits, x)


def finish_body(
    heads, low_hbm, kv_hbm, w_hbm, dq_out, dk_out, dv_out, w_out, low, kv, w, dq, dk, dv, in_sem, out_sem
):
    halves = kv.shape[0] // heads
    hk = kv.shape[2]
    loads = [
        pltpu.make_async_copy(src, dst, in_sem.at[n])
        for n, (src, dst) in enumerate(((low_hbm, low), (kv_hbm, kv), (w_hbm, w)))
    ]
    for copy in loads:
        copy.start()
    stores = [
        pltpu.make_async_copy(src, dst, out_sem.at[n])
        for n, (src, dst) in enumerate(((dq, dq_out), (dk, dk_out), (dv, dv_out), (w, w_out)))
    ]
    loads[0].wait()
    dq[...] = low[...].astype(jnp.float32)
    stores[0].start()
    loads[1].wait()
    for i, grad in enumerate((dk, dv)):
        for h in range(heads):
            for m in range(halves):
                grad[m * hk : (m + 1) * hk, h * HEAD : (h + 1) * HEAD] = kv[h * halves + m, i].astype(jnp.float32)
        stores[1 + i].start()
    loads[2].wait()
    stores[3].start()
    for copy in stores:
        copy.wait()


def finish(heads, low, kv, w):
    anywhere = pl.BlockSpec(memory_space=pl.ANY)
    f32 = jnp.float32
    grad = jax.ShapeDtypeStruct(low.shape, f32)
    return pl.pallas_call(
        lambda *refs: finish_body(heads, *refs),
        out_shape=(grad, grad, grad, jax.ShapeDtypeStruct(w.shape, f32)),
        in_specs=[anywhere] * 3,
        out_specs=(anywhere,) * 4,
        scratch_shapes=[
            pltpu.VMEM(low.shape, LOW), pltpu.VMEM(kv.shape, LOW), pltpu.VMEM(w.shape, f32),
            pltpu.VMEM(low.shape, f32), pltpu.VMEM(low.shape, f32), pltpu.VMEM(low.shape, f32),
            pltpu.SemaphoreType.DMA((3,)), pltpu.SemaphoreType.DMA((4,)),
        ],
        compiler_params=pltpu.CompilerParams(vmem_limit_bytes=62 * 1024 * 1024),
        name="finish",
    )(low, kv, w)


def local(queries, keys, values, forget_logits, layer_input, out_grad):
    heads = queries.shape[1] // HEAD
    blocks = lax.axis_size("sp")
    wide = lax.axis_size("tp")
    pieces = attention(blocks, wide, queries, out_grad, keys, values, forget_logits.T, layer_input)
    return finish(heads, *pieces)


def solution(mesh):
    spec = P("sp", "tp")
    return jax.shard_map(
        local, mesh=mesh, in_specs=(spec,) * 6, out_specs=(spec,) * 4, check_vma=False
    )
```

```python
import jax
import jax.numpy as jnp
from jax import lax
from jax.experimental import pallas as pl
from jax.experimental.pallas import tpu as pltpu
from jax.sharding import PartitionSpec as P

HEAD = 128
LOG2E = 1.4426950408889634
SCALE = HEAD ** (-0.5)
LOW = jnp.bfloat16
NX = 4


def nt(a, b):
    return lax.dot_general(a, b, (((1,), (1,)), ((), ())), preferred_element_type=jnp.float32)


def nn(a, b):
    return lax.dot_general(a, b, (((1,), (0,)), ((), ())), preferred_element_type=jnp.float32)


def kernel_body(
    heads, wide,
    q_hbm, g_hbm, k_hbm, v_hbm, logits_hbm, x_hbm,
    low_out, kv_out, w_out,
    q_in, g_in, k_in, v_in, logits, gate_in, w_sum, kv, qg, gates, kt, bias, wbuf, mrow, grads, stat, stat_got,
    dq_stage, part_stage, mid, red, fin, dq_got, kv_got,
    x_all, low, wa_stage, wb_stage, wa_red, wb_red, wa_own, wb_own, wa_fin, wb_fin, wa_got, wb_got,
    in_sem, out_sem, kv_recv, xs_send, col_send, x2_send, qg_recv, q_send, qf_send, gate_send, gate_recv, local_sem,
    stat_send, stat_recv, dq_send, dq_recv, part_send, mid_recv, red_recv, fin_send, fin_recv,
    x_send, xf_send, x_recv, wa_send, wb_send, wa_recv, wb_recv, wa_fsend, wb_fsend, wa_frecv, wb_frecv,
):
    blocks, _, hk, _ = kv.shape
    nx = NX
    nz = blocks // nx
    halves = nz // heads
    sub = qg.shape[2]
    tiles = blocks // 2
    span = w_out.shape[0]
    part_rows = span // 2
    x_width = x_hbm.shape[1]
    column = lax.axis_index("tp")
    me = lax.axis_index("sp")
    z = me // nx
    x = lax.rem(me, nx)
    head = z // halves
    half = lax.rem(z, halves)

    def at(zt, xt):
        return zt * nx + xt

    def near(r, c):
        return lax.rem(z + r, nz), lax.rem(x + c, nx)

    def remote(src, dst, send, recv, target):
        return pltpu.make_async_remote_copy(
            src_ref=src, dst_ref=dst, send_sem=send, recv_sem=recv, device_id={"sp": target}
        )

    def arrived(ref, recv):
        remote(ref, ref, dq_send.at[0], recv, me).wait_recv()

    barrier = pltpu.get_barrier_semaphore()
    for r in range(1, blocks):
        pl.semaphore_signal(barrier, inc=1, device_id={"sp": lax.rem(me + r, blocks)})
    for r in range(1, wide):
        pl.semaphore_signal(barrier, inc=1, device_id={"tp": lax.rem(column + r, wide)})

    def lanes(h):
        return pl.ds(pl.multiple_of(h * HEAD, HEAD), HEAD)

    sent = []

    def go(copy):
        copy.start()
        sent.append(copy)

    kv_in = (k_in, v_in)
    qg_in = (q_in, g_in)

    def kv_source(i, zt):
        begin = pl.multiple_of(lax.rem(zt, halves) * hk, hk)
        return kv_in[i].at[pl.ds(begin, hk), lanes(zt // halves)]

    def q_source(i, zt, xt):
        begin = pl.multiple_of(xt * sub, sub)
        return qg_in[i].at[pl.ds(begin, sub), lanes(zt // halves)]

    loads = [
        pltpu.make_async_copy(src, dst, in_sem.at[n])
        for n, (src, dst) in enumerate(
            ((logits_hbm, logits), (k_hbm, k_in), (v_hbm, v_in), (q_hbm, q_in), (g_hbm, g_in), (x_hbm, x_all.at[column]))
        )
    ]
    for copy in loads:
        copy.start()

    width = 2 * sub
    keys_wide = 2 * hk
    line = lax.broadcasted_iota(jnp.int32, (8, width), 0)

    @pl.loop(0, tiles)
    def _(j):
        grads[0, j] = jnp.zeros((keys_wide, HEAD), jnp.float32)
        grads[1, j] = jnp.zeros((keys_wide, HEAD), jnp.float32)
        stat[j] = jnp.where(line == 0, -1e30, 0.0)

    loads[0].wait()
    chunks = logits.shape[1] // HEAD
    raw = jnp.concatenate(
        [logits[h : h + 1, u * HEAD : (u + 1) * HEAD] for h in range(heads) for u in range(chunks)], axis=0
    )
    logs = (jnp.minimum(raw, 0.0) - jnp.log1p(jnp.exp(-jnp.abs(raw)))) * LOG2E
    upto = lax.broadcasted_iota(jnp.int32, (HEAD, HEAD), 0) <= lax.broadcasted_iota(jnp.int32, (HEAD, HEAD), 1)
    sums = jnp.dot(
        logs, upto.astype(jnp.float32), precision=lax.Precision.HIGHEST, preferred_element_type=jnp.float32
    )
    for h in range(heads):
        base = jnp.zeros((1, HEAD), jnp.float32)
        for u in range(chunks):
            line = sums[h * chunks + u : h * chunks + u + 1]
            gate_in[h, u : u + 1] = line + base
            base = base + jnp.broadcast_to(line[:, HEAD - 1 :], (1, HEAD))
        gate_in[h, chunks:] = jnp.broadcast_to(base, (gate_in.shape[1] - chunks, HEAD))

    for copy in loads[1:]:
        copy.wait()
    own = [pltpu.make_async_copy(kv_source(i, z), kv.at[me, i], local_sem.at[i]) for i in range(2)]
    own += [pltpu.make_async_copy(q_source(i, z, x), qg.at[me, i], local_sem.at[2 + i]) for i in range(2)]
    own += [pltpu.make_async_copy(gate_in.at[head], gates.at[me], local_sem.at[4])]
    for copy in own:
        copy.start()
    for copy in own:
        copy.wait()
    pl.semaphore_wait(barrier, blocks + wide - 2)

    for r in range(nz):
        for c in range(nx):
            if (r, c) == (0, 0):
                continue
            zt, xt = near(r, c)
            go(remote(gate_in.at[zt // halves], gates.at[me], gate_send.at[r, c], gate_recv.at[me], at(zt, xt)))

    def kv_arrived(j, i):
        arrived(kv.at[j, i], kv_recv.at[j, i])

    def round_copy(p, c, i):
        j = at(p, x)
        return remote(kv.at[j, i], kv.at[j, i], xs_send.at[p, c // 2, i], kv_recv.at[j, i], at(z, near(0, c)[1]))

    for i in range(2):
        for c in (1, nx - 1):
            round_copy(z, c, i).start()

    for r in (1, nz - 1, 2):
        zt = near(r, 0)[0]
        for i in range(2):
            go(remote(kv_source(i, zt), kv.at[me, i], col_send.at[r, i], kv_recv.at[me, i], at(zt, x)))

    across = nz - 1 - z
    partner = z + 1 - 2 * half

    def q_plane(r):
        return z if r == 0 else across

    for i in range(2):
        go(remote(q_source(i, z, x), qg.at[me, i], qf_send.at[0, 0, i], qg_recv.at[me, i], at(partner, x)))
    for r in range(heads):
        for c in range(nx):
            if (r, c) == (0, 0):
                continue
            zt, xt = q_plane(r), near(0, c)[1]
            for i in range(2):
                go(remote(q_source(i, zt, xt), qg.at[me, i], q_send.at[r, c, i], qg_recv.at[me, i], at(zt, xt)))

    def x_copy(src, source, target, send):
        return pltpu.make_async_remote_copy(
            src_ref=src, dst_ref=x_all.at[source], send_sem=send, recv_sem=x_recv.at[source], device_id={"tp": target}
        )

    core = lax.rem(column, 2)
    twin = column + 1 - 2 * core
    for r in range(1, wide // 2):
        go(x_copy(x_all.at[column], column, lax.rem(column + 2 * r, wide), x_send.at[r]))
    go(x_copy(x_all.at[column], column, twin, x_send.at[0]))

    def onward_copy(p, i):
        c = nx - 1 if i == 0 else 1
        j = at(p, near(0, c)[1])
        return remote(kv.at[j, i], kv.at[j, i], x2_send.at[p, i], kv_recv.at[j, i], at(z, near(0, nx - c)[1]))

    def column_on(r):
        p = near(r, 0)[0]
        for i in range(2):
            kv_arrived(at(p, x), i)
            for c in (1, nx - 1):
                round_copy(p, c, i).start()

    def second_on(p):
        for i, c in ((0, nx - 1), (1, 1)):
            kv_arrived(at(p, near(0, c)[1]), i)
            onward_copy(p, i).start()

    def q_wait(j):
        for i in range(2):
            arrived(qg.at[j, i], qg_recv.at[j, i])

    def q_on(r, c):
        j = at(q_plane(r), near(0, c)[1])
        q_wait(j)
        for i in range(2):
            go(remote(qg.at[j, i], qg.at[j, i], qf_send.at[r, c, i], qg_recv.at[j, i], at(partner, x)))

    column_on(1)
    column_on(nz - 1)
    for c in range(1, nx):
        if c == 2:
            column_on(2)
        q_on(0, c)
    second_on(0)
    second_on(1)
    for c in range(nx):
        q_on(1, c)
    for r in range(nz):
        for c in range(nx):
            if (r, c) != (0, 0):
                j = at(*near(r, c))
                arrived(gates.at[j], gate_recv.at[j])

    def prepare(j, base):
        per = hk // HEAD
        table = gates[j]
        mine = table[0:per]
        for n in range(1, halves):
            mine = jnp.where(half == n, table[n * per : (n + 1) * per], mine)
        for n in range(per):
            row = mine[n : n + 1] + base
            bias[j, n * HEAD : (n + 1) * HEAD] = jnp.broadcast_to(row, (HEAD, HEAD)).T
        return base + table[halves * per : halves * per + 1]

    lax.fori_loop(0, blocks, prepare, jnp.zeros((1, HEAD), jnp.float32))
    rows = halves * hk
    key_row = lax.broadcasted_iota(jnp.int32, (keys_wide, width), 0)
    query_row = lax.broadcasted_iota(jnp.int32, (keys_wide, width), 1)
    key_pos = jnp.where(key_row >= hk, key_row - hk + rows, key_row) + half * hk
    query_pos = jnp.where(query_row >= sub, query_row - sub + rows, query_row) + x * sub

    def pair(i, j):
        return kv[pl.ds(2 * j, 2), i].reshape(keys_wide, HEAD)

    def queries(i, t):
        return qg[pl.ds(2 * t, 2), i].reshape(width, HEAD)

    def place(t, j):
        return t * (t + 1) // 2 + j

    def scores(t, j):
        state = stat[t]
        m, total, terms = state[0:1], state[1:2], state[2:3]
        column_bias = bias[pl.ds(2 * j, 2)].reshape(keys_wide, HEAD)
        s = nt(pair(0, j), queries(0, t)) * (SCALE * LOG2E) - jnp.concatenate([column_bias] * (width // HEAD), axis=1)
        s = jnp.where(key_pos <= query_pos + (t - j) * (2 * rows), s, -1e30)
        top = jnp.maximum(m, jnp.max(s, axis=0, keepdims=True))
        w = jnp.exp2(s - top)
        old = jnp.exp2(m - top)
        dp = nt(pair(1, j), queries(1, t))
        wbuf[place(t, j)] = w
        mrow[place(t, j)] = jnp.broadcast_to(top, (8, width))
        total = total * old + jnp.sum(w, axis=0, keepdims=True)
        terms = terms * old + jnp.sum(w * dp, axis=0, keepdims=True)
        stat[t] = jnp.concatenate([top, total, terms, jnp.zeros((5, width), jnp.float32)], axis=0)

    def pair_wait(j):
        for u in range(2):
            b = 2 * j + u
            d = lax.rem(lax.rem(b, nx) + nx - x, nx)

            @pl.when((d == 1) | (d == 2))
            def _():
                kv_arrived(b, 0)

            @pl.when((d == nx - 1) | (d == 2))
            def _():
                kv_arrived(b, 1)

        for n in range(2):
            kt[j, :, n * hk : (n + 1) * hk] = kv[2 * j + n, 0].T

    outer = (z == 0) | (z == nz - 1)
    quarter = tiles // 4

    def group(direct, j):
        ends = outer if direct else jnp.logical_not(outer)

        @pl.loop(0, 2 * quarter)
        def _(m):
            t = jnp.where(ends, jnp.where(m >= quarter, m + 2 * quarter, m), m + quarter)

            @pl.when(t >= j)
            def _():
                scores(t, j)

    def backward(t):
        q, g = queries(0, t), queries(1, t)
        arrived(stat_got.at[t], stat_recv.at[t])
        mine = stat[t]
        other = stat_got[t]
        top = jnp.maximum(mine[0:1], other[0:1])
        scale_mine = jnp.exp2(mine[0:1] - top)
        scale_other = jnp.exp2(other[0:1] - top)
        inverse = 1.0 / (mine[1:2] * scale_mine + other[1:2] * scale_other)
        terms = (mine[2:3] * scale_mine + other[2:3] * scale_other) * inverse

        def block(j, acc):
            factor = jnp.exp2(mrow[place(t, j)][0:1] - top) * inverse
            prob = wbuf[place(t, j)] * factor
            ds = (prob * (nt(pair(1, j), g) - terms)).astype(LOW)
            grads[1, j] += nn(prob.astype(LOW), g)
            grads[0, j] += nn(ds, q)
            return acc + nn(kt[j], ds)

        acc = block(t, jnp.zeros((HEAD, width), jnp.float32))
        for n, (u, i) in enumerate(((0, 0), (1, 0), (1, 1), (0, 1))):
            value = grads[i, t, u * hk : (u + 1) * hk]
            part_stage[t, n] = (value * SCALE if i == 0 else value).astype(LOW)
        acc = lax.fori_loop(0, t, block, acc)
        dq_t = (acc * SCALE).T.astype(LOW)
        for n in range(2):
            dq_stage[2 * t + n] = dq_t[n * sub : (n + 1) * sub]

    def stat_copy(t):
        return remote(stat.at[t], stat_got.at[t], stat_send.at[t], stat_recv.at[t], at(partner, x))

    def dq_copy(n):
        return remote(dq_stage.at[n], dq_got.at[z, x], dq_send.at[n], dq_recv.at[me], n)

    hr = hk // 2

    def role(tile):
        return lax.rem(x + nx - 2 * lax.rem(tile, nx // 2), nx)

    def array(tile, c):
        return lax.rem(role(tile) + c, nx)

    def share(tile, n, way):
        u = jnp.where((n == 1) | (n == 2), 1, 0)
        i = n // 2
        value = grads[i, tile, pl.ds(pl.multiple_of(u * hk + way * hr, hr), hr)]
        return value * jnp.where(i == 0, SCALE, 1.0)

    def half_of(tile, n, way):
        return part_stage.at[tile, n, pl.ds(way * hr, hr)]

    def opposite_copy(tile, way):
        n = array(tile, 2)
        return remote(
            half_of(tile, n, way), mid.at[tile, way], part_send.at[tile, n, way], mid_recv.at[tile, way],
            at(z, near(0, nx - 1 if way else 1)[1]),
        )

    def near_copy(tile, side, way):
        c = nx - 1 if side else 1
        n = array(tile, c)
        return remote(
            half_of(tile, n, way), red.at[tile, side, way], part_send.at[tile, n, way], red_recv.at[tile, side, way],
            at(z, near(0, c)[1]),
        )

    def first_sends(tile):
        for way in range(2):
            opposite_copy(tile, way).start()
        near_copy(tile, 0, 1).start()
        near_copy(tile, 1, 0).start()

    def add_on_way(tile):
        for way, c in ((0, 1), (1, nx - 1)):
            n = array(tile, c)
            arrived(mid.at[tile, way], mid_recv.at[tile, way])
            part_stage[tile, n, way * hr : (way + 1) * hr] = (
                share(tile, n, way) + mid[tile, way].astype(jnp.float32)
            ).astype(LOW)

    def second_sends(tile):
        near_copy(tile, 0, 0).start()
        near_copy(tile, 1, 1).start()

    def reduce(tile):
        n = array(tile, 0)
        for way in range(2):
            value = share(tile, n, way)
            for side in range(2):
                arrived(red.at[tile, side, way], red_recv.at[tile, side, way])
                value = value + red[tile, side, way].astype(jnp.float32)
            fin[tile, way * hr : (way + 1) * hr] = value.astype(LOW)

    def fin_owner(tile):
        n = array(tile, 0)
        return 2 * tile + jnp.where((n == 1) | (n == 2), 1, 0), n // 2

    def fin_copy(tile):
        owner, i = fin_owner(tile)
        return remote(fin.at[tile], kv_got.at[z, i], fin_send.at[tile], fin_recv.at[z, i], owner)

    def fin_sends(tile):
        owner, i = fin_owner(tile)

        @pl.when(owner == me)
        def _():
            kv_got[z, i] = fin[tile]

        @pl.when(owner != me)
        def _():
            fin_copy(tile).start()

    def dq_sends(tile):
        for u in range(2):
            n = 2 * tile + u

            @pl.when(n == me)
            def _():
                dq_got[z, x] = dq_stage[n]

            @pl.when(n != me)
            def _():
                dq_copy(n).start()

    def x_on(r):
        return x_copy(
            x_all.at[lax.rem(column + 2 * r, wide)], lax.rem(column + 2 * r, wide), twin, xf_send.at[r]
        )

    @pl.loop(0, tiles // 2)
    def _(j):
        pair_wait(j)
        group(True, j)

        @pl.when(lax.rem(j, 2) == 1)
        def _():
            second_on(2 + j // 2)

    for plane in (partner, nz - 1 - partner):
        for c in range(nx):
            q_wait(at(plane, near(0, c)[1]))

    @pl.loop(0, tiles // 2)
    def _(j):
        group(False, j)

    @pl.loop(tiles // 2, tiles)
    def _(j):
        pair_wait(j)

        @pl.loop(j, tiles)
        def _(t):
            scores(t, j)

        stat_copy(j - tiles // 2).start()

        @pl.when(j < tiles - 1)
        def _():
            stat_copy(j).start()

    for r in range(1, wide // 2):
        source = lax.rem(column + 2 * r, wide)
        pltpu.make_async_remote_copy(
            src_ref=x_all.at[source], dst_ref=x_all.at[source], send_sem=xf_send.at[r],
            recv_sem=x_recv.at[source], device_id={"tp": twin},
        ).wait_recv()
        x_on(r).start()
    stat_copy(tiles - 1).start()

    def step(s, carry):
        t = tiles - 1 - s

        def stage(offset, work):
            pl.when((t + offset >= 0) & (t + offset < tiles))(lambda: work(t + offset))

        stage(1, dq_sends)
        stage(4, second_sends)
        stage(0, backward)
        stage(0, first_sends)
        stage(3, add_on_way)
        return carry

    lax.fori_loop(0, tiles + 1, step, 0)
    second_sends(2)
    add_on_way(1)
    add_on_way(0)

    for r in range(nz):
        for c in range(nx):
            if (r, c) != (0, 0):
                zs, xs = near(r, c)
                arrived(dq_got.at[zs, xs], dq_recv.at[at(zs, xs)])
    for h in range(heads):
        for n in range(nx):
            value = dq_got[h * halves, n].astype(jnp.float32)
            for m in range(1, halves):
                value = value + dq_got[h * halves + m, n].astype(jnp.float32)
            low[n * sub : (n + 1) * sub, h * HEAD : (h + 1) * HEAD] = value.astype(LOW)
    low_copy = pltpu.make_async_copy(low, low_out, out_sem.at[0])
    second_sends(1)
    second_sends(0)
    for r in range(wide // 2):
        source = lax.rem(twin + 2 * r, wide)
        pltpu.make_async_remote_copy(
            src_ref=x_all.at[source], dst_ref=x_all.at[source], send_sem=x_send.at[0],
            recv_sem=x_recv.at[source], device_id={"tp": twin},
        ).wait_recv()

    def term(c):
        begin = c * span
        xs = x_all[begin // x_width, :, pl.ds(pl.multiple_of(lax.rem(begin, x_width), span), span)]
        return lax.dot_general(xs, low[...], (((0,), (0,)), ((), ())), preferred_element_type=jnp.float32)

    waiting = []

    def flush():
        for copy in waiting:
            go(copy)
        waiting.clear()

    order = [(r, c) for r in range(1, nz) for c in range(1, nx)]
    order += [(0, c) for c in range(1, nx)] + [(r, 0) for r in range(1, nz)] + [(0, 0)]
    for r, c in order:
        zt, xt = near(r, c)
        value = term(at(zt, xt))
        fresh = []
        if c:
            wa_stage[r, c] = value[:part_rows].astype(LOW)
            fresh.append(
                remote(wa_stage.at[r, c], wa_red.at[x, zt], wa_send.at[r, c], wa_recv.at[x, zt], at(z, xt))
            )
        else:
            wa_own[r] = value[:part_rows]
        if r:
            wb_stage[r, c] = value[part_rows:].astype(LOW)
            fresh.append(
                remote(wb_stage.at[r, c], wb_red.at[z, xt], wb_send.at[r, c], wb_recv.at[z, xt], at(zt, x))
            )
        else:
            wb_own[c] = value[part_rows:]
        flush()
        waiting.extend(fresh)
    flush()
    low_copy.start()

    @pl.loop(0, tiles)
    def _(n):
        reduce(tiles - 1 - n)

        @pl.when(n > 0)
        def _():
            fin_sends(tiles - n)


    for n in list(range(1, nz)) + [0]:
        if n == 2:
            fin_sends(0)
        zt = near(n, 0)[0]
        value = wa_own[n]
        for c in range(1, nx):
            xs = near(0, c)[1]
            arrived(wa_red.at[xs, zt], wa_recv.at[xs, zt])
            value = value + wa_red[xs, zt].astype(jnp.float32)
        fresh = []
        if n:
            wa_fin[n] = value.astype(LOW)
            fresh.append(remote(wa_fin.at[n], wa_got.at[z], wa_fsend.at[n], wa_frecv.at[z], at(zt, x)))
        else:
            w_sum[:part_rows] = value
        xt = near(0, n)[1]
        value = wb_own[n]
        for r in range(1, nz):
            zs = near(r, 0)[0]
            arrived(wb_red.at[zs, xt], wb_recv.at[zs, xt])
            value = value + wb_red[zs, xt].astype(jnp.float32)
        if n:
            wb_fin[n] = value.astype(LOW)
            fresh.append(remote(wb_fin.at[n], wb_got.at[x], wb_fsend.at[n], wb_frecv.at[x], at(z, xt)))
        else:
            w_sum[part_rows:] = value
        flush()
        waiting.extend(fresh)
    flush()

    my_tile = me // 2
    for r in range(nz):
        zs = near(r, 0)[0]
        for i in range(2):
            if r == 0:
                owner, mine = fin_owner(my_tile)

                @pl.when(jnp.logical_not((owner == me) & (mine == i)))
                def _():
                    arrived(kv_got.at[zs, i], fin_recv.at[zs, i])
            else:
                arrived(kv_got.at[zs, i], fin_recv.at[zs, i])
    kv_copy = pltpu.make_async_copy(kv_got, kv_out, out_sem.at[1])
    kv_copy.start()
    for n in range(1, nz):
        zs = near(n, 0)[0]
        arrived(wa_got.at[zs], wa_frecv.at[zs])
        w_sum[:part_rows] += wa_got[zs].astype(jnp.float32)
        xs = near(0, n)[1]
        arrived(wb_got.at[xs], wb_frecv.at[xs])
        w_sum[part_rows:] += wb_got[xs].astype(jnp.float32)

    w_copy = pltpu.make_async_copy(w_sum, w_out, out_sem.at[2])
    w_copy.start()
    low_copy.wait()
    kv_copy.wait()
    for copy in sent:
        copy.wait_send()
    for r in range(1, wide // 2):
        x_on(r).wait_send()

    @pl.loop(0, nz)
    def _(p):
        for i in range(2):
            for c in (1, nx - 1):
                round_copy(p, c, i).wait_send()
            onward_copy(p, i).wait_send()

    @pl.loop(0, tiles)
    def _(t):
        stat_copy(t).wait_send()

    @pl.loop(0, blocks)
    def _(n):
        @pl.when(n != me)
        def _():
            dq_copy(n).wait_send()

    @pl.loop(0, tiles)
    def _(tile):
        for way in range(2):
            opposite_copy(tile, way).wait_send()
            for side in range(2):
                near_copy(tile, side, way).wait_send()

        @pl.when(fin_owner(tile)[0] != me)
        def _():
            fin_copy(tile).wait_send()

    w_copy.wait()


def attention(blocks, wide, q, g, k, v, logits, x):
    rows, cols = k.shape
    heads = cols // HEAD
    nx = NX
    nz = blocks // nx
    halves = nz // heads
    hk = rows // halves
    sub = rows // nx
    tiles = blocks // 2
    anywhere = pl.BlockSpec(memory_space=pl.ANY)
    f32 = jnp.float32
    dma = pltpu.SemaphoreType.DMA
    span = x.shape[1] * wide // blocks
    part = span // 2
    return pl.pallas_call(
        lambda *refs: kernel_body(heads, wide, *refs),
        out_shape=(
            jax.ShapeDtypeStruct((rows, cols), LOW),
            jax.ShapeDtypeStruct((nz, 2, hk, HEAD), LOW),
            jax.ShapeDtypeStruct((span, cols), f32),
        ),
        in_specs=[anywhere] * 6,
        out_specs=(anywhere,) * 3,
        scratch_shapes=[
            pltpu.VMEM((rows, cols), LOW),
            pltpu.VMEM((rows, cols), LOW),
            pltpu.VMEM((rows, cols), LOW),
            pltpu.VMEM((rows, cols), LOW),
            pltpu.VMEM((heads, rows), f32),
            pltpu.VMEM((heads, 8, HEAD), f32),
            pltpu.VMEM((span, cols), f32),
            pltpu.VMEM((blocks, 2, hk, HEAD), LOW),
            pltpu.VMEM((blocks, 2, sub, HEAD), LOW),
            pltpu.VMEM((blocks, 8, HEAD), f32),
            pltpu.VMEM((tiles, HEAD, 2 * hk), LOW),
            pltpu.VMEM((blocks, hk, HEAD), f32),
            pltpu.VMEM((tiles * (tiles + 1) // 2, 2 * hk, 2 * sub), f32),
            pltpu.VMEM((tiles * (tiles + 1) // 2, 8, 2 * sub), f32),
            pltpu.VMEM((2, tiles, 2 * hk, HEAD), f32),
            pltpu.VMEM((tiles, 8, 2 * sub), f32),
            pltpu.VMEM((tiles, 8, 2 * sub), f32),
            pltpu.VMEM((blocks, sub, HEAD), LOW),
            pltpu.VMEM((tiles, nx, hk, HEAD), LOW),
            pltpu.VMEM((tiles, 2, hk // 2, HEAD), LOW),
            pltpu.VMEM((tiles, 2, 2, hk // 2, HEAD), LOW),
            pltpu.VMEM((tiles, hk, HEAD), LOW),
            pltpu.VMEM((nz, nx, sub, HEAD), LOW),
            pltpu.VMEM((nz, 2, hk, HEAD), LOW),
            pltpu.VMEM((wide, rows, x.shape[1]), LOW),
            pltpu.VMEM((rows, cols), LOW),
            pltpu.VMEM((nz, nx, part, cols), LOW),
            pltpu.VMEM((nz, nx, part, cols), LOW),
            pltpu.VMEM((nx, nz, part, cols), LOW),
            pltpu.VMEM((nz, nx, part, cols), LOW),
            pltpu.VMEM((nz, part, cols), f32),
            pltpu.VMEM((nx, part, cols), f32),
            pltpu.VMEM((nz, part, cols), LOW),
            pltpu.VMEM((nx, part, cols), LOW),
            pltpu.VMEM((nz, part, cols), LOW),
            pltpu.VMEM((nx, part, cols), LOW),
            dma((6,)), dma((3,)),
            dma((blocks, 2)), dma((nz, 2, 2)), dma((nz, 2)), dma((nz, 2)), dma((blocks, 2)), dma((heads, nx, 2)),
            dma((heads, nx, 2)), dma((nz, nx)), dma((blocks,)), dma((6,)),
            dma((tiles,)), dma((tiles,)), dma((blocks,)), dma((blocks,)), dma((tiles, nx, 2)), dma((tiles, 2)),
            dma((tiles, 2, 2)), dma((tiles,)), dma((nz, 2)),
            dma((wide // 2,)), dma((wide // 2,)), dma((wide,)),
            dma((nz, nx)), dma((nz, nx)), dma((nx, nz)), dma((nz, nx)),
            dma((nz,)), dma((nx,)), dma((nz,)), dma((nx,)),
        ],
        compiler_params=pltpu.CompilerParams(
            vmem_limit_bytes=62 * 1024 * 1024, collective_id=0, has_side_effects=True
        ),
        cost_estimate=pl.CostEstimate(
            flops=10 * blocks * blocks * rows * sub * HEAD, bytes_accessed=1 << 22, transcendentals=0
        ),
        name="attention",
    )(q, g, k, v, logits, x)


def finish_body(
    heads, low_hbm, kv_hbm, w_hbm, dq_out, dk_out, dv_out, w_out, low, kv, w, dq, dk, dv, in_sem, out_sem
):
    halves = kv.shape[0] // heads
    hk = kv.shape[2]
    loads = [
        pltpu.make_async_copy(src, dst, in_sem.at[n])
        for n, (src, dst) in enumerate(((low_hbm, low), (kv_hbm, kv), (w_hbm, w)))
    ]
    for copy in loads:
        copy.start()
    stores = [
        pltpu.make_async_copy(src, dst, out_sem.at[n])
        for n, (src, dst) in enumerate(((dq, dq_out), (dk, dk_out), (dv, dv_out), (w, w_out)))
    ]
    loads[0].wait()
    dq[...] = low[...].astype(jnp.float32)
    stores[0].start()
    loads[1].wait()
    for i, grad in enumerate((dk, dv)):
        for h in range(heads):
            for m in range(halves):
                grad[m * hk : (m + 1) * hk, h * HEAD : (h + 1) * HEAD] = kv[h * halves + m, i].astype(jnp.float32)
        stores[1 + i].start()
    loads[2].wait()
    stores[3].start()
    for copy in stores:
        copy.wait()


def finish(heads, low, kv, w):
    anywhere = pl.BlockSpec(memory_space=pl.ANY)
    f32 = jnp.float32
    grad = jax.ShapeDtypeStruct(low.shape, f32)
    return pl.pallas_call(
        lambda *refs: finish_body(heads, *refs),
        out_shape=(grad, grad, grad, jax.ShapeDtypeStruct(w.shape, f32)),
        in_specs=[anywhere] * 3,
        out_specs=(anywhere,) * 4,
        scratch_shapes=[
            pltpu.VMEM(low.shape, LOW), pltpu.VMEM(kv.shape, LOW), pltpu.VMEM(w.shape, f32),
            pltpu.VMEM(low.shape, f32), pltpu.VMEM(low.shape, f32), pltpu.VMEM(low.shape, f32),
            pltpu.SemaphoreType.DMA((3,)), pltpu.SemaphoreType.DMA((4,)),
        ],
        compiler_params=pltpu.CompilerParams(vmem_limit_bytes=62 * 1024 * 1024),
        name="finish",
    )(low, kv, w)


def local(queries, keys, values, forget_logits, layer_input, out_grad):
    heads = queries.shape[1] // HEAD
    blocks = lax.axis_size("sp")
    wide = lax.axis_size("tp")
    pieces = attention(blocks, wide, queries, out_grad, keys, values, forget_logits.T, layer_input)
    return finish(heads, *pieces)


def solution(mesh):
    spec = P("sp", "tp")
    return jax.shard_map(
        local, mesh=mesh, in_specs=(spec,) * 6, out_specs=(spec,) * 4, check_vma=False
    )
```

```python
import jax
import jax.numpy as jnp
from jax import lax
from jax.experimental import pallas as pl
from jax.experimental.pallas import tpu as pltpu
from jax.sharding import PartitionSpec as P

HEAD = 128
LOG2E = 1.4426950408889634
SCALE = HEAD ** (-0.5)
LOW = jnp.bfloat16
NX = 4


def nt(a, b):
    return lax.dot_general(a, b, (((1,), (1,)), ((), ())), preferred_element_type=jnp.float32)


def nn(a, b):
    return lax.dot_general(a, b, (((1,), (0,)), ((), ())), preferred_element_type=jnp.float32)


def kernel_body(
    heads, wide,
    q_hbm, g_hbm, k_hbm, v_hbm, logits_hbm, x_hbm,
    low_out, kv_out, w_out,
    q_in, g_in, k_in, v_in, logits, gate_in, w_sum, kv, qg, gates, kt, bias, wbuf, mrow, grads, acc, stat, stat_got,
    dq_stage, part_stage, mid, red, fin, dq_got, kv_got,
    x_all, low, wa_stage, wb_stage, wa_red, wb_red, wa_own, wb_own, wa_fin, wb_fin, wa_got, wb_got,
    in_sem, out_sem, kv_recv, xs_send, col_send, x2_send, qg_recv, q_send, qf_send, gate_send, gate_recv, local_sem,
    stat_send, stat_recv, dq_send, dq_recv, part_send, mid_recv, red_recv, fin_send, fin_recv,
    x_send, xf_send, x_recv, wa_send, wb_send, wa_recv, wb_recv, wa_fsend, wb_fsend, wa_frecv, wb_frecv,
):
    blocks, _, hk, _ = kv.shape
    nx = NX
    nz = blocks // nx
    halves = nz // heads
    sub = qg.shape[2]
    tiles = blocks // 2
    span = w_out.shape[0]
    part_rows = span // 2
    x_width = x_hbm.shape[1]
    column = lax.axis_index("tp")
    me = lax.axis_index("sp")
    z = me // nx
    x = lax.rem(me, nx)
    head = z // halves
    half = lax.rem(z, halves)

    def at(zt, xt):
        return zt * nx + xt

    def near(r, c):
        return lax.rem(z + r, nz), lax.rem(x + c, nx)

    def remote(src, dst, send, recv, target):
        return pltpu.make_async_remote_copy(
            src_ref=src, dst_ref=dst, send_sem=send, recv_sem=recv, device_id={"sp": target}
        )

    def arrived(ref, recv):
        remote(ref, ref, dq_send.at[0], recv, me).wait_recv()

    barrier = pltpu.get_barrier_semaphore()
    for r in range(1, blocks):
        pl.semaphore_signal(barrier, inc=1, device_id={"sp": lax.rem(me + r, blocks)})
    for r in range(1, wide):
        pl.semaphore_signal(barrier, inc=1, device_id={"tp": lax.rem(column + r, wide)})

    def lanes(h):
        return pl.ds(pl.multiple_of(h * HEAD, HEAD), HEAD)

    sent = []

    def go(copy):
        copy.start()
        sent.append(copy)

    kv_in = (k_in, v_in)
    qg_in = (q_in, g_in)

    def kv_source(i, zt):
        begin = pl.multiple_of(lax.rem(zt, halves) * hk, hk)
        return kv_in[i].at[pl.ds(begin, hk), lanes(zt // halves)]

    def q_source(i, zt, xt):
        begin = pl.multiple_of(xt * sub, sub)
        return qg_in[i].at[pl.ds(begin, sub), lanes(zt // halves)]

    loads = [
        pltpu.make_async_copy(src, dst, in_sem.at[n])
        for n, (src, dst) in enumerate(
            ((logits_hbm, logits), (k_hbm, k_in), (v_hbm, v_in), (q_hbm, q_in), (g_hbm, g_in), (x_hbm, x_all.at[column]))
        )
    ]
    for copy in loads:
        copy.start()

    width = 2 * sub
    keys_wide = 2 * hk
    line = lax.broadcasted_iota(jnp.int32, (8, width), 0)

    @pl.loop(0, tiles)
    def _(j):
        grads[0, j] = jnp.zeros((keys_wide, HEAD), jnp.float32)
        grads[1, j] = jnp.zeros((keys_wide, HEAD), jnp.float32)
        stat[j] = jnp.where(line == 0, -1e30, 0.0)

    loads[0].wait()
    chunks = logits.shape[1] // HEAD
    raw = jnp.concatenate(
        [logits[h : h + 1, u * HEAD : (u + 1) * HEAD] for h in range(heads) for u in range(chunks)], axis=0
    )
    logs = (jnp.minimum(raw, 0.0) - jnp.log1p(jnp.exp(-jnp.abs(raw)))) * LOG2E
    upto = lax.broadcasted_iota(jnp.int32, (HEAD, HEAD), 0) <= lax.broadcasted_iota(jnp.int32, (HEAD, HEAD), 1)
    sums = jnp.dot(
        logs, upto.astype(jnp.float32), precision=lax.Precision.HIGHEST, preferred_element_type=jnp.float32
    )
    for h in range(heads):
        base = jnp.zeros((1, HEAD), jnp.float32)
        for u in range(chunks):
            line = sums[h * chunks + u : h * chunks + u + 1]
            gate_in[h, u : u + 1] = line + base
            base = base + jnp.broadcast_to(line[:, HEAD - 1 :], (1, HEAD))
        gate_in[h, chunks:] = jnp.broadcast_to(base, (gate_in.shape[1] - chunks, HEAD))

    for copy in loads[1:]:
        copy.wait()
    own = [pltpu.make_async_copy(kv_source(i, z), kv.at[me, i], local_sem.at[i]) for i in range(2)]
    own += [pltpu.make_async_copy(q_source(i, z, x), qg.at[me, i], local_sem.at[2 + i]) for i in range(2)]
    own += [pltpu.make_async_copy(gate_in.at[head], gates.at[me], local_sem.at[4])]
    for copy in own:
        copy.start()
    for copy in own:
        copy.wait()
    pl.semaphore_wait(barrier, blocks + wide - 2)

    for r in range(nz):
        for c in range(nx):
            if (r, c) == (0, 0):
                continue
            zt, xt = near(r, c)
            go(remote(gate_in.at[zt // halves], gates.at[me], gate_send.at[r, c], gate_recv.at[me], at(zt, xt)))

    def kv_arrived(j, i):
        arrived(kv.at[j, i], kv_recv.at[j, i])

    def round_copy(p, c, i):
        j = at(p, x)
        return remote(kv.at[j, i], kv.at[j, i], xs_send.at[p, c // 2, i], kv_recv.at[j, i], at(z, near(0, c)[1]))

    for i in range(2):
        for c in (1, nx - 1):
            round_copy(z, c, i).start()

    for r in (1, nz - 1, 2):
        zt = near(r, 0)[0]
        for i in range(2):
            go(remote(kv_source(i, zt), kv.at[me, i], col_send.at[r, i], kv_recv.at[me, i], at(zt, x)))

    across = nz - 1 - z
    partner = z + 1 - 2 * half

    def q_plane(r):
        return z if r == 0 else across

    for i in range(2):
        go(remote(q_source(i, z, x), qg.at[me, i], qf_send.at[0, 0, i], qg_recv.at[me, i], at(partner, x)))
    for r in range(heads):
        for c in range(nx):
            if (r, c) == (0, 0):
                continue
            zt, xt = q_plane(r), near(0, c)[1]
            for i in range(2):
                go(remote(q_source(i, zt, xt), qg.at[me, i], q_send.at[r, c, i], qg_recv.at[me, i], at(zt, xt)))

    def x_copy(src, source, target, send):
        return pltpu.make_async_remote_copy(
            src_ref=src, dst_ref=x_all.at[source], send_sem=send, recv_sem=x_recv.at[source], device_id={"tp": target}
        )

    core = lax.rem(column, 2)
    twin = column + 1 - 2 * core
    for r in range(1, wide // 2):
        go(x_copy(x_all.at[column], column, lax.rem(column + 2 * r, wide), x_send.at[r]))
    go(x_copy(x_all.at[column], column, twin, x_send.at[0]))

    def onward_copy(p, i):
        c = nx - 1 if i == 0 else 1
        j = at(p, near(0, c)[1])
        return remote(kv.at[j, i], kv.at[j, i], x2_send.at[p, i], kv_recv.at[j, i], at(z, near(0, nx - c)[1]))

    def column_on(r):
        p = near(r, 0)[0]
        for i in range(2):
            kv_arrived(at(p, x), i)
            for c in (1, nx - 1):
                round_copy(p, c, i).start()

    def second_on(p):
        for i, c in ((0, nx - 1), (1, 1)):
            kv_arrived(at(p, near(0, c)[1]), i)
            onward_copy(p, i).start()

    def q_wait(j):
        for i in range(2):
            arrived(qg.at[j, i], qg_recv.at[j, i])

    def q_on(r, c):
        j = at(q_plane(r), near(0, c)[1])
        q_wait(j)
        for i in range(2):
            go(remote(qg.at[j, i], qg.at[j, i], qf_send.at[r, c, i], qg_recv.at[j, i], at(partner, x)))

    column_on(1)
    column_on(nz - 1)
    for c in range(1, nx):
        if c == 2:
            column_on(2)
        q_on(0, c)
    for r in range(nz):
        for c in range(nx):
            if (r, c) != (0, 0):
                j = at(*near(r, c))
                arrived(gates.at[j], gate_recv.at[j])

    def prepare(j, base):
        per = hk // HEAD
        table = gates[j]
        mine = table[0:per]
        for n in range(1, halves):
            mine = jnp.where(half == n, table[n * per : (n + 1) * per], mine)
        for n in range(per):
            row = mine[n : n + 1] + base
            bias[j, n * HEAD : (n + 1) * HEAD] = jnp.broadcast_to(row, (HEAD, HEAD)).T
        return base + table[halves * per : halves * per + 1]

    lax.fori_loop(0, blocks, prepare, jnp.zeros((1, HEAD), jnp.float32))
    second_on(0)
    second_on(1)
    for c in range(nx):
        q_on(1, c)
    rows = halves * hk
    key_row = lax.broadcasted_iota(jnp.int32, (keys_wide, width), 0)
    query_row = lax.broadcasted_iota(jnp.int32, (keys_wide, width), 1)
    key_pos = jnp.where(key_row >= hk, key_row - hk + rows, key_row) + half * hk
    query_pos = jnp.where(query_row >= sub, query_row - sub + rows, query_row) + x * sub

    def pair(i, j):
        return kv[pl.ds(2 * j, 2), i].reshape(keys_wide, HEAD)

    def queries(i, t):
        return qg[pl.ds(2 * t, 2), i].reshape(width, HEAD)

    def place(t, j):
        return t * (t + 1) // 2 + j

    def scores(j, *group):
        k, v = pair(0, j), pair(1, j)
        column_bias = bias[pl.ds(2 * j, 2)].reshape(keys_wide, HEAD)
        column_bias = jnp.concatenate([column_bias] * (width // HEAD), axis=1)
        states = [stat[t] for t, _ in group]
        results = []
        for (t, masked), state in zip(group, states):
            m, total, terms = state[0:1], state[1:2], state[2:3]
            s = nt(k, queries(0, t)) * (SCALE * LOG2E) - column_bias
            if masked:
                s = jnp.where(key_pos <= query_pos, s, -1e30)
            top = jnp.maximum(m, jnp.max(s, axis=0, keepdims=True))
            w = jnp.exp2(s - top)
            old = jnp.exp2(m - top)
            dp = nt(v, queries(1, t))
            total = total * old + jnp.sum(w, axis=0, keepdims=True)
            terms = terms * old + jnp.sum(w * dp, axis=0, keepdims=True)
            wbuf[place(t, j)] = w
            results.append((top, total, terms))
        for (t, _), (top, total, terms) in zip(group, results):
            mrow[place(t, j)] = jnp.broadcast_to(top, (8, width))
            stat[t] = jnp.concatenate([top, total, terms, jnp.zeros((5, width), jnp.float32)], axis=0)

    def pair_wait(j):
        for u in range(2):
            b = 2 * j + u
            d = lax.rem(lax.rem(b, nx) + nx - x, nx)

            @pl.when((d == 1) | (d == 2))
            def _():
                kv_arrived(b, 0)

            @pl.when((d == nx - 1) | (d == 2))
            def _():
                kv_arrived(b, 1)

        for n in range(2):
            kt[j, :, n * hk : (n + 1) * hk] = kv[2 * j + n, 0].T

    outer = (z == 0) | (z == nz - 1)
    quarter = tiles // 4

    def group(direct, j):
        ends = outer if direct else jnp.logical_not(outer)

        @pl.loop(0, quarter)
        def _(m):
            t = jnp.where(ends, m * 3 * quarter, quarter + m * 2)

            @pl.when(t > j)
            def _():
                scores(j, (t, False), (t + 1, False))

            @pl.when(t == j)
            def _():
                scores(j, (t, True), (t + 1, False))

            @pl.when(t + 1 == j)
            def _():
                scores(j, (t + 1, True))

    def backward(t):
        q, g = queries(0, t), queries(1, t)
        arrived(stat_got.at[t], stat_recv.at[t])
        mine = stat[t]
        other = stat_got[t]
        top = jnp.maximum(mine[0:1], other[0:1])
        scale_mine = jnp.exp2(mine[0:1] - top)
        scale_other = jnp.exp2(other[0:1] - top)
        inverse = 1.0 / (mine[1:2] * scale_mine + other[1:2] * scale_other)
        terms = (mine[2:3] * scale_mine + other[2:3] * scale_other) * inverse

        def blocks_of(*pairs):
            added = []
            for j in pairs:
                factor = jnp.exp2(mrow[place(t, j)][0:1] - top) * inverse
                prob = wbuf[place(t, j)] * factor
                ds = (prob * (nt(pair(1, j), g) - terms)).astype(LOW)
                added.append((j, nn(prob.astype(LOW), g), nn(ds, q), nn(kt[j], ds)))
            for j, dv, dk, _ in added:
                grads[1, j] += dv
                grads[0, j] += dk
            acc[...] += sum(term for _, _, _, term in added)

        acc[...] = jnp.zeros((HEAD, width), jnp.float32)
        blocks_of(t)
        for n, (u, i) in enumerate(((0, 0), (1, 0), (1, 1), (0, 1))):
            value = grads[i, t, u * hk : (u + 1) * hk]
            part_stage[t, n] = (value * SCALE if i == 0 else value).astype(LOW)

        @pl.loop(0, t // 2)
        def _(n):
            blocks_of(2 * n, 2 * n + 1)

        @pl.when(lax.rem(t, 2) == 1)
        def _():
            blocks_of(t - 1)

        dq_t = (acc[...] * SCALE).T.astype(LOW)
        for n in range(2):
            dq_stage[2 * t + n] = dq_t[n * sub : (n + 1) * sub]

    def stat_copy(t):
        return remote(stat.at[t], stat_got.at[t], stat_send.at[t], stat_recv.at[t], at(partner, x))

    def dq_copy(n):
        return remote(dq_stage.at[n], dq_got.at[z, x], dq_send.at[n], dq_recv.at[me], n)

    hr = hk // 2

    def role(tile):
        return lax.rem(x + nx - 2 * lax.rem(tile, nx // 2), nx)

    def array(tile, c):
        return lax.rem(role(tile) + c, nx)

    def share(tile, n, way):
        u = jnp.where((n == 1) | (n == 2), 1, 0)
        i = n // 2
        value = grads[i, tile, pl.ds(pl.multiple_of(u * hk + way * hr, hr), hr)]
        return value * jnp.where(i == 0, SCALE, 1.0)

    def half_of(tile, n, way):
        return part_stage.at[tile, n, pl.ds(way * hr, hr)]

    def opposite_copy(tile, way):
        n = array(tile, 2)
        return remote(
            half_of(tile, n, way), mid.at[tile, way], part_send.at[tile, n, way], mid_recv.at[tile, way],
            at(z, near(0, nx - 1 if way else 1)[1]),
        )

    def near_copy(tile, side, way):
        c = nx - 1 if side else 1
        n = array(tile, c)
        return remote(
            half_of(tile, n, way), red.at[tile, side, way], part_send.at[tile, n, way], red_recv.at[tile, side, way],
            at(z, near(0, c)[1]),
        )

    def first_sends(tile):
        for way in range(2):
            opposite_copy(tile, way).start()
        near_copy(tile, 0, 1).start()
        near_copy(tile, 1, 0).start()

    def add_on_way(tile):
        for way, c in ((0, 1), (1, nx - 1)):
            n = array(tile, c)
            arrived(mid.at[tile, way], mid_recv.at[tile, way])
            part_stage[tile, n, way * hr : (way + 1) * hr] = (
                share(tile, n, way) + mid[tile, way].astype(jnp.float32)
            ).astype(LOW)

    def second_sends(tile):
        near_copy(tile, 0, 0).start()
        near_copy(tile, 1, 1).start()

    def reduce(tile):
        n = array(tile, 0)
        for way in range(2):
            value = share(tile, n, way)
            for side in range(2):
                arrived(red.at[tile, side, way], red_recv.at[tile, side, way])
                value = value + red[tile, side, way].astype(jnp.float32)
            fin[tile, way * hr : (way + 1) * hr] = value.astype(LOW)

    def fin_owner(tile):
        n = array(tile, 0)
        return 2 * tile + jnp.where((n == 1) | (n == 2), 1, 0), n // 2

    def fin_copy(tile):
        owner, i = fin_owner(tile)
        return remote(fin.at[tile], kv_got.at[z, i], fin_send.at[tile], fin_recv.at[z, i], owner)

    def fin_sends(tile):
        owner, i = fin_owner(tile)

        @pl.when(owner == me)
        def _():
            kv_got[z, i] = fin[tile]

        @pl.when(owner != me)
        def _():
            fin_copy(tile).start()

    def dq_sends(tile):
        for u in range(2):
            n = 2 * tile + u

            @pl.when(n == me)
            def _():
                dq_got[z, x] = dq_stage[n]

            @pl.when(n != me)
            def _():
                dq_copy(n).start()

    def x_on(r):
        return x_copy(
            x_all.at[lax.rem(column + 2 * r, wide)], lax.rem(column + 2 * r, wide), twin, xf_send.at[r]
        )

    @pl.loop(0, tiles // 2)
    def _(j):
        pair_wait(j)
        group(True, j)

        @pl.when(lax.rem(j, 2) == 1)
        def _():
            second_on(2 + j // 2)

    for plane in (partner, nz - 1 - partner):
        for c in range(nx):
            q_wait(at(plane, near(0, c)[1]))

    @pl.loop(0, tiles // 2)
    def _(j):
        group(False, j)

    @pl.loop(tiles // 2, tiles)
    def _(j):
        pair_wait(j)

        odd = lax.rem(tiles - 1 - j, 2)

        @pl.when(odd == 1)
        def _():
            scores(j, (j, True), (j + 1, False))

        @pl.when(odd == 0)
        def _():
            scores(j, (j, True))

        @pl.loop(0, (tiles - 1 - j) // 2)
        def _(n):
            t = j + 1 + odd + 2 * n
            scores(j, (t, False), (t + 1, False))

        stat_copy(j - tiles // 2).start()

        @pl.when(j < tiles - 1)
        def _():
            stat_copy(j).start()

    for r in range(1, wide // 2):
        source = lax.rem(column + 2 * r, wide)
        pltpu.make_async_remote_copy(
            src_ref=x_all.at[source], dst_ref=x_all.at[source], send_sem=xf_send.at[r],
            recv_sem=x_recv.at[source], device_id={"tp": twin},
        ).wait_recv()
        x_on(r).start()
    stat_copy(tiles - 1).start()

    def step(s, carry):
        t = tiles - 1 - s

        def stage(offset, work):
            pl.when((t + offset >= 0) & (t + offset < tiles))(lambda: work(t + offset))

        stage(4, second_sends)
        stage(7, fin_sends)
        stage(0, backward)
        stage(0, first_sends)
        stage(0, dq_sends)
        stage(3, add_on_way)
        stage(6, reduce)
        return carry

    lax.fori_loop(0, tiles, step, 0)
    second_sends(3)
    add_on_way(2)
    add_on_way(1)
    second_sends(2)
    add_on_way(0)
    second_sends(1)
    fin_sends(6)
    second_sends(0)
    reduce(5)
    reduce(4)

    for r in range(nz):
        for c in range(nx):
            if (r, c) != (0, 0):
                zs, xs = near(r, c)
                arrived(dq_got.at[zs, xs], dq_recv.at[at(zs, xs)])
    for h in range(heads):
        for n in range(nx):
            value = dq_got[h * halves, n].astype(jnp.float32)
            for m in range(1, halves):
                value = value + dq_got[h * halves + m, n].astype(jnp.float32)
            low[n * sub : (n + 1) * sub, h * HEAD : (h + 1) * HEAD] = value.astype(LOW)
    low_copy = pltpu.make_async_copy(low, low_out, out_sem.at[0])
    fin_sends(5)
    fin_sends(4)
    for r in range(wide // 2):
        source = lax.rem(twin + 2 * r, wide)
        pltpu.make_async_remote_copy(
            src_ref=x_all.at[source], dst_ref=x_all.at[source], send_sem=x_send.at[0],
            recv_sem=x_recv.at[source], device_id={"tp": twin},
        ).wait_recv()

    def term(c):
        begin = c * span
        xs = x_all[begin // x_width, :, pl.ds(pl.multiple_of(lax.rem(begin, x_width), span), span)]
        return lax.dot_general(xs, low[...], (((0,), (0,)), ((), ())), preferred_element_type=jnp.float32)

    waiting = []

    def flush():
        for copy in waiting:
            go(copy)
        waiting.clear()

    order = [(r, c) for r in range(1, nz) for c in range(1, nx)]
    order += [(0, c) for c in range(1, nx)] + [(r, 0) for r in range(1, nz)] + [(0, 0)]
    for r, c in order:
        zt, xt = near(r, c)
        value = term(at(zt, xt))
        fresh = []
        if c:
            wa_stage[r, c] = value[:part_rows].astype(LOW)
            fresh.append(
                remote(wa_stage.at[r, c], wa_red.at[x, zt], wa_send.at[r, c], wa_recv.at[x, zt], at(z, xt))
            )
        else:
            wa_own[r] = value[:part_rows]
        if r:
            wb_stage[r, c] = value[part_rows:].astype(LOW)
            fresh.append(
                remote(wb_stage.at[r, c], wb_red.at[z, xt], wb_send.at[r, c], wb_recv.at[z, xt], at(zt, x))
            )
        else:
            wb_own[c] = value[part_rows:]
        flush()
        waiting.extend(fresh)
    flush()
    low_copy.start()

    @pl.loop(0, 4)
    def _(n):
        reduce(3 - n)

        @pl.when(n > 0)
        def _():
            fin_sends(4 - n)


    for n in list(range(1, nz)) + [0]:
        if n == 2:
            fin_sends(0)
        zt = near(n, 0)[0]
        value = wa_own[n]
        for c in range(1, nx):
            xs = near(0, c)[1]
            arrived(wa_red.at[xs, zt], wa_recv.at[xs, zt])
            value = value + wa_red[xs, zt].astype(jnp.float32)
        fresh = []
        if n:
            wa_fin[n] = value.astype(LOW)
            fresh.append(remote(wa_fin.at[n], wa_got.at[z], wa_fsend.at[n], wa_frecv.at[z], at(zt, x)))
        else:
            w_sum[:part_rows] = value
        xt = near(0, n)[1]
        value = wb_own[n]
        for r in range(1, nz):
            zs = near(r, 0)[0]
            arrived(wb_red.at[zs, xt], wb_recv.at[zs, xt])
            value = value + wb_red[zs, xt].astype(jnp.float32)
        if n:
            wb_fin[n] = value.astype(LOW)
            fresh.append(remote(wb_fin.at[n], wb_got.at[x], wb_fsend.at[n], wb_frecv.at[x], at(z, xt)))
        else:
            w_sum[part_rows:] = value
        flush()
        waiting.extend(fresh)
    flush()

    my_tile = me // 2
    for r in range(nz):
        zs = near(r, 0)[0]
        for i in range(2):
            if r == 0:
                owner, mine = fin_owner(my_tile)

                @pl.when(jnp.logical_not((owner == me) & (mine == i)))
                def _():
                    arrived(kv_got.at[zs, i], fin_recv.at[zs, i])
            else:
                arrived(kv_got.at[zs, i], fin_recv.at[zs, i])
    kv_copy = pltpu.make_async_copy(kv_got, kv_out, out_sem.at[1])
    kv_copy.start()
    for n in range(1, nz):
        zs = near(n, 0)[0]
        arrived(wa_got.at[zs], wa_frecv.at[zs])
        w_sum[:part_rows] += wa_got[zs].astype(jnp.float32)
        xs = near(0, n)[1]
        arrived(wb_got.at[xs], wb_frecv.at[xs])
        w_sum[part_rows:] += wb_got[xs].astype(jnp.float32)

    w_copy = pltpu.make_async_copy(w_sum, w_out, out_sem.at[2])
    w_copy.start()
    low_copy.wait()
    kv_copy.wait()
    for copy in sent:
        copy.wait_send()
    for r in range(1, wide // 2):
        x_on(r).wait_send()

    @pl.loop(0, nz)
    def _(p):
        for i in range(2):
            for c in (1, nx - 1):
                round_copy(p, c, i).wait_send()
            onward_copy(p, i).wait_send()

    @pl.loop(0, tiles)
    def _(t):
        stat_copy(t).wait_send()

    @pl.loop(0, blocks)
    def _(n):
        @pl.when(n != me)
        def _():
            dq_copy(n).wait_send()

    @pl.loop(0, tiles)
    def _(tile):
        for way in range(2):
            opposite_copy(tile, way).wait_send()
            for side in range(2):
                near_copy(tile, side, way).wait_send()

        @pl.when(fin_owner(tile)[0] != me)
        def _():
            fin_copy(tile).wait_send()

    w_copy.wait()


def attention(blocks, wide, q, g, k, v, logits, x):
    rows, cols = k.shape
    heads = cols // HEAD
    nx = NX
    nz = blocks // nx
    halves = nz // heads
    hk = rows // halves
    sub = rows // nx
    tiles = blocks // 2
    anywhere = pl.BlockSpec(memory_space=pl.ANY)
    f32 = jnp.float32
    dma = pltpu.SemaphoreType.DMA
    span = x.shape[1] * wide // blocks
    part = span // 2
    return pl.pallas_call(
        lambda *refs: kernel_body(heads, wide, *refs),
        out_shape=(
            jax.ShapeDtypeStruct((rows, cols), LOW),
            jax.ShapeDtypeStruct((nz, 2, hk, HEAD), LOW),
            jax.ShapeDtypeStruct((span, cols), f32),
        ),
        in_specs=[anywhere] * 6,
        out_specs=(anywhere,) * 3,
        scratch_shapes=[
            pltpu.VMEM((rows, cols), LOW),
            pltpu.VMEM((rows, cols), LOW),
            pltpu.VMEM((rows, cols), LOW),
            pltpu.VMEM((rows, cols), LOW),
            pltpu.VMEM((heads, rows), f32),
            pltpu.VMEM((heads, 8, HEAD), f32),
            pltpu.VMEM((span, cols), f32),
            pltpu.VMEM((blocks, 2, hk, HEAD), LOW),
            pltpu.VMEM((blocks, 2, sub, HEAD), LOW),
            pltpu.VMEM((blocks, 8, HEAD), f32),
            pltpu.VMEM((tiles, HEAD, 2 * hk), LOW),
            pltpu.VMEM((blocks, hk, HEAD), f32),
            pltpu.VMEM((tiles * (tiles + 1) // 2, 2 * hk, 2 * sub), f32),
            pltpu.VMEM((tiles * (tiles + 1) // 2, 8, 2 * sub), f32),
            pltpu.VMEM((2, tiles, 2 * hk, HEAD), f32),
            pltpu.VMEM((HEAD, 2 * sub), f32),
            pltpu.VMEM((tiles, 8, 2 * sub), f32),
            pltpu.VMEM((tiles, 8, 2 * sub), f32),
            pltpu.VMEM((blocks, sub, HEAD), LOW),
            pltpu.VMEM((tiles, nx, hk, HEAD), LOW),
            pltpu.VMEM((tiles, 2, hk // 2, HEAD), LOW),
            pltpu.VMEM((tiles, 2, 2, hk // 2, HEAD), LOW),
            pltpu.VMEM((tiles, hk, HEAD), LOW),
            pltpu.VMEM((nz, nx, sub, HEAD), LOW),
            pltpu.VMEM((nz, 2, hk, HEAD), LOW),
            pltpu.VMEM((wide, rows, x.shape[1]), LOW),
            pltpu.VMEM((rows, cols), LOW),
            pltpu.VMEM((nz, nx, part, cols), LOW),
            pltpu.VMEM((nz, nx, part, cols), LOW),
            pltpu.VMEM((nx, nz, part, cols), LOW),
            pltpu.VMEM((nz, nx, part, cols), LOW),
            pltpu.VMEM((nz, part, cols), f32),
            pltpu.VMEM((nx, part, cols), f32),
            pltpu.VMEM((nz, part, cols), LOW),
            pltpu.VMEM((nx, part, cols), LOW),
            pltpu.VMEM((nz, part, cols), LOW),
            pltpu.VMEM((nx, part, cols), LOW),
            dma((6,)), dma((3,)),
            dma((blocks, 2)), dma((nz, 2, 2)), dma((nz, 2)), dma((nz, 2)), dma((blocks, 2)), dma((heads, nx, 2)),
            dma((heads, nx, 2)), dma((nz, nx)), dma((blocks,)), dma((6,)),
            dma((tiles,)), dma((tiles,)), dma((blocks,)), dma((blocks,)), dma((tiles, nx, 2)), dma((tiles, 2)),
            dma((tiles, 2, 2)), dma((tiles,)), dma((nz, 2)),
            dma((wide // 2,)), dma((wide // 2,)), dma((wide,)),
            dma((nz, nx)), dma((nz, nx)), dma((nx, nz)), dma((nz, nx)),
            dma((nz,)), dma((nx,)), dma((nz,)), dma((nx,)),
        ],
        compiler_params=pltpu.CompilerParams(
            vmem_limit_bytes=62 * 1024 * 1024, collective_id=0, has_side_effects=True
        ),
        cost_estimate=pl.CostEstimate(
            flops=10 * blocks * blocks * rows * sub * HEAD, bytes_accessed=1 << 22, transcendentals=0
        ),
        name="attention",
    )(q, g, k, v, logits, x)


def finish_body(
    heads, low_hbm, kv_hbm, w_hbm, dq_out, dk_out, dv_out, w_out, low, kv, w, dq, dk, dv, in_sem, out_sem
):
    halves = kv.shape[0] // heads
    hk = kv.shape[2]
    loads = [
        pltpu.make_async_copy(src, dst, in_sem.at[n])
        for n, (src, dst) in enumerate(((low_hbm, low), (kv_hbm, kv), (w_hbm, w)))
    ]
    for copy in loads:
        copy.start()
    stores = [
        pltpu.make_async_copy(src, dst, out_sem.at[n])
        for n, (src, dst) in enumerate(((dq, dq_out), (dk, dk_out), (dv, dv_out), (w, w_out)))
    ]
    loads[0].wait()
    dq[...] = low[...].astype(jnp.float32)
    stores[0].start()
    loads[1].wait()
    for i, grad in enumerate((dk, dv)):
        for h in range(heads):
            for m in range(halves):
                grad[m * hk : (m + 1) * hk, h * HEAD : (h + 1) * HEAD] = kv[h * halves + m, i].astype(jnp.float32)
        stores[1 + i].start()
    loads[2].wait()
    stores[3].start()
    for copy in stores:
        copy.wait()


def finish(heads, low, kv, w):
    anywhere = pl.BlockSpec(memory_space=pl.ANY)
    f32 = jnp.float32
    grad = jax.ShapeDtypeStruct(low.shape, f32)
    return pl.pallas_call(
        lambda *refs: finish_body(heads, *refs),
        out_shape=(grad, grad, grad, jax.ShapeDtypeStruct(w.shape, f32)),
        in_specs=[anywhere] * 3,
        out_specs=(anywhere,) * 4,
        scratch_shapes=[
            pltpu.VMEM(low.shape, LOW), pltpu.VMEM(kv.shape, LOW), pltpu.VMEM(w.shape, f32),
            pltpu.VMEM(low.shape, f32), pltpu.VMEM(low.shape, f32), pltpu.VMEM(low.shape, f32),
            pltpu.SemaphoreType.DMA((3,)), pltpu.SemaphoreType.DMA((4,)),
        ],
        compiler_params=pltpu.CompilerParams(vmem_limit_bytes=62 * 1024 * 1024),
        name="finish",
    )(low, kv, w)


def local(queries, keys, values, forget_logits, layer_input, out_grad):
    heads = queries.shape[1] // HEAD
    blocks = lax.axis_size("sp")
    wide = lax.axis_size("tp")
    pieces = attention(blocks, wide, queries, out_grad, keys, values, forget_logits.T, layer_input)
    return finish(heads, *pieces)


def solution(mesh):
    spec = P("sp", "tp")
    return jax.shard_map(
        local, mesh=mesh, in_specs=(spec,) * 6, out_specs=(spec,) * 4, check_vma=False
    )
```

```python
import jax
import jax.numpy as jnp
from jax import lax
from jax.experimental import pallas as pl
from jax.experimental.pallas import tpu as pltpu
from jax.sharding import PartitionSpec as P

HEAD = 128
LOG2E = 1.4426950408889634
SCALE = HEAD ** (-0.5)
LOW = jnp.bfloat16
NX = 4


def nt(a, b):
    return lax.dot_general(a, b, (((1,), (1,)), ((), ())), preferred_element_type=jnp.float32)


def nn(a, b):
    return lax.dot_general(a, b, (((1,), (0,)), ((), ())), preferred_element_type=jnp.float32)


def kernel_body(
    heads, wide,
    q_hbm, g_hbm, k_hbm, v_hbm, logits_hbm, x_hbm,
    low_out, kv_out, w_out,
    q_in, g_in, k_in, v_in, logits, gate_in, w_sum, kv, qg, gates, kt, bias, wbuf, mrow, grads, acc, stat, stat_got,
    dq_stage, part_stage, mid, red, fin, dq_got, kv_got,
    x_all, low, wa_stage, wb_stage, wa_red, wb_red, wa_own, wb_own, wa_fin, wb_fin, wa_got, wb_got,
    in_sem, out_sem, kv_recv, xs_send, col_send, x2_send, qg_recv, q_send, qf_send, gate_send, gate_recv, local_sem,
    stat_send, stat_recv, dq_send, dq_recv, part_send, mid_recv, red_recv, fin_send, fin_recv,
    x_send, xf_send, x_recv, wa_send, wb_send, wa_recv, wb_recv, wa_fsend, wb_fsend, wa_frecv, wb_frecv,
):
    blocks, _, hk, _ = kv.shape
    nx = NX
    nz = blocks // nx
    halves = nz // heads
    sub = qg.shape[2]
    tiles = blocks // 2
    span = w_out.shape[0]
    part_rows = span // 2
    x_width = x_hbm.shape[1]
    column = lax.axis_index("tp")
    me = lax.axis_index("sp")
    z = me // nx
    x = lax.rem(me, nx)
    head = z // halves
    half = lax.rem(z, halves)

    def at(zt, xt):
        return zt * nx + xt

    def near(r, c):
        return lax.rem(z + r, nz), lax.rem(x + c, nx)

    def remote(src, dst, send, recv, target):
        return pltpu.make_async_remote_copy(
            src_ref=src, dst_ref=dst, send_sem=send, recv_sem=recv, device_id={"sp": target}
        )

    def arrived(ref, recv):
        remote(ref, ref, dq_send.at[0], recv, me).wait_recv()

    barrier = pltpu.get_barrier_semaphore()
    for r in range(1, blocks):
        pl.semaphore_signal(barrier, inc=1, device_id={"sp": lax.rem(me + r, blocks)})
    for r in range(1, wide):
        pl.semaphore_signal(barrier, inc=1, device_id={"tp": lax.rem(column + r, wide)})

    def lanes(h):
        return pl.ds(pl.multiple_of(h * HEAD, HEAD), HEAD)

    sent = []

    def go(copy):
        copy.start()
        sent.append(copy)

    kv_in = (k_in, v_in)
    qg_in = (q_in, g_in)

    def kv_source(i, zt):
        begin = pl.multiple_of(lax.rem(zt, halves) * hk, hk)
        return kv_in[i].at[pl.ds(begin, hk), lanes(zt // halves)]

    def q_source(i, zt, xt):
        begin = pl.multiple_of(xt * sub, sub)
        return qg_in[i].at[pl.ds(begin, sub), lanes(zt // halves)]

    loads = [
        pltpu.make_async_copy(src, dst, in_sem.at[n])
        for n, (src, dst) in enumerate(
            ((logits_hbm, logits), (k_hbm, k_in), (v_hbm, v_in), (q_hbm, q_in), (g_hbm, g_in), (x_hbm, x_all.at[column]))
        )
    ]
    for copy in loads:
        copy.start()

    width = 2 * sub
    keys_wide = 2 * hk
    line = lax.broadcasted_iota(jnp.int32, (8, width), 0)

    @pl.loop(0, tiles)
    def _(j):
        grads[0, j] = jnp.zeros((keys_wide, HEAD), jnp.float32)
        grads[1, j] = jnp.zeros((keys_wide, HEAD), jnp.float32)
        stat[j] = jnp.where(line == 0, -1e30, 0.0)

    loads[0].wait()
    chunks = logits.shape[1] // HEAD
    raw = jnp.concatenate(
        [logits[h : h + 1, u * HEAD : (u + 1) * HEAD] for h in range(heads) for u in range(chunks)], axis=0
    )
    logs = (jnp.minimum(raw, 0.0) - jnp.log1p(jnp.exp(-jnp.abs(raw)))) * LOG2E
    upto = lax.broadcasted_iota(jnp.int32, (HEAD, HEAD), 0) <= lax.broadcasted_iota(jnp.int32, (HEAD, HEAD), 1)
    sums = jnp.dot(
        logs, upto.astype(jnp.float32), precision=lax.Precision.HIGHEST, preferred_element_type=jnp.float32
    )
    for h in range(heads):
        base = jnp.zeros((1, HEAD), jnp.float32)
        for u in range(chunks):
            line = sums[h * chunks + u : h * chunks + u + 1]
            gate_in[h, u : u + 1] = line + base
            base = base + jnp.broadcast_to(line[:, HEAD - 1 :], (1, HEAD))
        gate_in[h, chunks:] = jnp.broadcast_to(base, (gate_in.shape[1] - chunks, HEAD))

    for copy in loads[1:]:
        copy.wait()
    own = [pltpu.make_async_copy(kv_source(i, z), kv.at[me, i], local_sem.at[i]) for i in range(2)]
    own += [pltpu.make_async_copy(q_source(i, z, x), qg.at[me, i], local_sem.at[2 + i]) for i in range(2)]
    own += [pltpu.make_async_copy(gate_in.at[head], gates.at[me], local_sem.at[4])]
    for copy in own:
        copy.start()
    for copy in own:
        copy.wait()
    pl.semaphore_wait(barrier, blocks + wide - 2)

    for r in range(nz):
        for c in range(nx):
            if (r, c) == (0, 0):
                continue
            zt, xt = near(r, c)
            go(remote(gate_in.at[zt // halves], gates.at[me], gate_send.at[r, c], gate_recv.at[me], at(zt, xt)))

    def kv_arrived(j, i):
        arrived(kv.at[j, i], kv_recv.at[j, i])

    def round_copy(p, c, i):
        j = at(p, x)
        return remote(kv.at[j, i], kv.at[j, i], xs_send.at[p, c // 2, i], kv_recv.at[j, i], at(z, near(0, c)[1]))

    for i in range(2):
        for c in (1, nx - 1):
            round_copy(z, c, i).start()

    for r in (1, nz - 1, 2):
        zt = near(r, 0)[0]
        for i in range(2):
            go(remote(kv_source(i, zt), kv.at[me, i], col_send.at[r, i], kv_recv.at[me, i], at(zt, x)))

    across = nz - 1 - z
    partner = z + 1 - 2 * half

    def q_plane(r):
        return z if r == 0 else across

    for i in range(2):
        go(remote(q_source(i, z, x), qg.at[me, i], qf_send.at[0, 0, i], qg_recv.at[me, i], at(partner, x)))
    for r in range(heads):
        for c in range(nx):
            if (r, c) == (0, 0):
                continue
            zt, xt = q_plane(r), near(0, c)[1]
            for i in range(2):
                go(remote(q_source(i, zt, xt), qg.at[me, i], q_send.at[r, c, i], qg_recv.at[me, i], at(zt, xt)))

    def x_copy(src, source, target, send):
        return pltpu.make_async_remote_copy(
            src_ref=src, dst_ref=x_all.at[source], send_sem=send, recv_sem=x_recv.at[source], device_id={"tp": target}
        )

    core = lax.rem(column, 2)
    twin = column + 1 - 2 * core
    for r in range(1, wide // 2):
        go(x_copy(x_all.at[column], column, lax.rem(column + 2 * r, wide), x_send.at[r]))
    go(x_copy(x_all.at[column], column, twin, x_send.at[0]))

    def onward_copy(p, i):
        c = nx - 1 if i == 0 else 1
        j = at(p, near(0, c)[1])
        return remote(kv.at[j, i], kv.at[j, i], x2_send.at[p, i], kv_recv.at[j, i], at(z, near(0, nx - c)[1]))

    def column_on(r):
        p = near(r, 0)[0]
        for i in range(2):
            kv_arrived(at(p, x), i)
            for c in (1, nx - 1):
                round_copy(p, c, i).start()

    def second_on(p):
        for i, c in ((0, nx - 1), (1, 1)):
            kv_arrived(at(p, near(0, c)[1]), i)
            onward_copy(p, i).start()

    def q_wait(j):
        for i in range(2):
            arrived(qg.at[j, i], qg_recv.at[j, i])

    def q_on(r, c):
        j = at(q_plane(r), near(0, c)[1])
        q_wait(j)
        for i in range(2):
            go(remote(qg.at[j, i], qg.at[j, i], qf_send.at[r, c, i], qg_recv.at[j, i], at(partner, x)))

    column_on(1)
    column_on(nz - 1)
    for c in range(1, nx):
        if c == 2:
            column_on(2)
        q_on(0, c)
    for r in range(nz):
        for c in range(nx):
            if (r, c) != (0, 0):
                j = at(*near(r, c))
                arrived(gates.at[j], gate_recv.at[j])

    def prepare(j, base):
        per = hk // HEAD
        table = gates[j]
        mine = table[0:per]
        for n in range(1, halves):
            mine = jnp.where(half == n, table[n * per : (n + 1) * per], mine)
        for n in range(per):
            row = mine[n : n + 1] + base
            bias[j, n * HEAD : (n + 1) * HEAD] = jnp.broadcast_to(row, (HEAD, HEAD)).T
        return base + table[halves * per : halves * per + 1]

    lax.fori_loop(0, blocks, prepare, jnp.zeros((1, HEAD), jnp.float32))
    second_on(0)
    second_on(1)
    for c in range(nx):
        q_on(1, c)
    rows = halves * hk
    key_row = lax.broadcasted_iota(jnp.int32, (keys_wide, width), 0)
    query_row = lax.broadcasted_iota(jnp.int32, (keys_wide, width), 1)
    key_pos = jnp.where(key_row >= hk, key_row - hk + rows, key_row) + half * hk
    query_pos = jnp.where(query_row >= sub, query_row - sub + rows, query_row) + x * sub

    def pair(i, j):
        return kv[pl.ds(2 * j, 2), i].reshape(keys_wide, HEAD)

    def queries(i, t):
        return qg[pl.ds(2 * t, 2), i].reshape(width, HEAD)

    def place(t, j):
        return t * (t + 1) // 2 + j

    def scores(j, *group):
        k, v = pair(0, j), pair(1, j)
        column_bias = bias[pl.ds(2 * j, 2)].reshape(keys_wide, HEAD)
        column_bias = jnp.concatenate([column_bias] * (width // HEAD), axis=1)
        states = [stat[t] for t, _ in group]
        results = []
        for (t, masked), state in zip(group, states):
            m, total, terms = state[0:1], state[1:2], state[2:3]
            s = nt(k, queries(0, t)) * (SCALE * LOG2E) - column_bias
            if masked:
                s = jnp.where(key_pos <= query_pos, s, -1e30)
            top = jnp.maximum(m, jnp.max(s, axis=0, keepdims=True))
            w = jnp.exp2(s - top)
            old = jnp.exp2(m - top)
            dp = nt(v, queries(1, t))
            total = total * old + jnp.sum(w, axis=0, keepdims=True)
            terms = terms * old + jnp.sum(w * dp, axis=0, keepdims=True)
            wbuf[place(t, j)] = w
            results.append((top, total, terms))
        for (t, _), (top, total, terms) in zip(group, results):
            mrow[place(t, j)] = jnp.broadcast_to(top, (8, width))
            stat[t] = jnp.concatenate([top, total, terms, jnp.zeros((5, width), jnp.float32)], axis=0)

    def pair_wait(j):
        for u in range(2):
            b = 2 * j + u
            d = lax.rem(lax.rem(b, nx) + nx - x, nx)

            @pl.when((d == 1) | (d == 2))
            def _():
                kv_arrived(b, 0)

            @pl.when((d == nx - 1) | (d == 2))
            def _():
                kv_arrived(b, 1)

        for n in range(2):
            kt[j, :, n * hk : (n + 1) * hk] = kv[2 * j + n, 0].T

    outer = (z == 0) | (z == nz - 1)
    quarter = tiles // 4

    def group(direct, j):
        ends = outer if direct else jnp.logical_not(outer)

        @pl.loop(0, quarter)
        def _(m):
            t = jnp.where(ends, m * 3 * quarter, quarter + m * 2)

            @pl.when(t > j)
            def _():
                scores(j, (t, False), (t + 1, False))

            @pl.when(t == j)
            def _():
                scores(j, (t, True), (t + 1, False))

            @pl.when(t + 1 == j)
            def _():
                scores(j, (t + 1, True))

    def stage_parts(t):
        for n, (u, i) in enumerate(((0, 0), (1, 0), (1, 1), (0, 1))):
            value = grads[i, t, u * hk : (u + 1) * hk]
            part_stage[t, n] = (value * SCALE if i == 0 else value).astype(LOW)

    def backward(t):
        q, g = queries(0, t), queries(1, t)
        arrived(stat_got.at[t], stat_recv.at[t])
        mine = stat[t]
        other = stat_got[t]
        top = jnp.maximum(mine[0:1], other[0:1])
        scale_mine = jnp.exp2(mine[0:1] - top)
        scale_other = jnp.exp2(other[0:1] - top)
        inverse = 1.0 / (mine[1:2] * scale_mine + other[1:2] * scale_other)
        terms = (mine[2:3] * scale_mine + other[2:3] * scale_other) * inverse

        def blocks_of(*pairs):
            added = []
            for j in pairs:
                factor = jnp.exp2(mrow[place(t, j)][0:1] - top) * inverse
                prob = wbuf[place(t, j)] * factor
                ds = (prob * (nt(pair(1, j), g) - terms)).astype(LOW)
                added.append((j, nn(prob.astype(LOW), g), nn(ds, q), nn(kt[j], ds)))
            for j, dv, dk, _ in added:
                grads[1, j] += dv
                grads[0, j] += dk
            acc[...] += sum(term for _, _, _, term in added)

        acc[...] = jnp.zeros((HEAD, width), jnp.float32)
        blocks_of(t)

        @pl.when((t >= tiles // 2) | (t < tiles // 4))
        def _():
            stage_parts(t)

        @pl.loop(0, t // 2)
        def _(n):
            blocks_of(2 * n, 2 * n + 1)

        @pl.when(lax.rem(t, 2) == 1)
        def _():
            blocks_of(t - 1)

        dq_t = (acc[...] * SCALE).T.astype(LOW)
        for n in range(2):
            dq_stage[2 * t + n] = dq_t[n * sub : (n + 1) * sub]

    def stat_copy(t):
        return remote(stat.at[t], stat_got.at[t], stat_send.at[t], stat_recv.at[t], at(partner, x))

    def dq_copy(n):
        return remote(dq_stage.at[n], dq_got.at[z, x], dq_send.at[n], dq_recv.at[me], n)

    hr = hk // 2

    def role(tile):
        return lax.rem(x + nx - 2 * lax.rem(tile, nx // 2), nx)

    def array(tile, c):
        return lax.rem(role(tile) + c, nx)

    def share(tile, n, way):
        u = jnp.where((n == 1) | (n == 2), 1, 0)
        i = n // 2
        value = grads[i, tile, pl.ds(pl.multiple_of(u * hk + way * hr, hr), hr)]
        return value * jnp.where(i == 0, SCALE, 1.0)

    def half_of(tile, n, way):
        return part_stage.at[tile, n, pl.ds(way * hr, hr)]

    def opposite_copy(tile, way):
        n = array(tile, 2)
        return remote(
            half_of(tile, n, way), mid.at[tile, way], part_send.at[tile, n, way], mid_recv.at[tile, way],
            at(z, near(0, nx - 1 if way else 1)[1]),
        )

    def near_copy(tile, side, way):
        c = nx - 1 if side else 1
        n = array(tile, c)
        return remote(
            half_of(tile, n, way), red.at[tile, side, way], part_send.at[tile, n, way], red_recv.at[tile, side, way],
            at(z, near(0, c)[1]),
        )

    def first_sends(tile):
        for way in range(2):
            opposite_copy(tile, way).start()
        near_copy(tile, 0, 1).start()
        near_copy(tile, 1, 0).start()

    def add_on_way(tile):
        for way, c in ((0, 1), (1, nx - 1)):
            n = array(tile, c)
            arrived(mid.at[tile, way], mid_recv.at[tile, way])
            part_stage[tile, n, way * hr : (way + 1) * hr] = (
                share(tile, n, way) + mid[tile, way].astype(jnp.float32)
            ).astype(LOW)

    def second_sends(tile):
        near_copy(tile, 0, 0).start()
        near_copy(tile, 1, 1).start()

    def reduce(tile):
        n = array(tile, 0)
        for way in range(2):
            value = share(tile, n, way)
            for side in range(2):
                arrived(red.at[tile, side, way], red_recv.at[tile, side, way])
                value = value + red[tile, side, way].astype(jnp.float32)
            fin[tile, way * hr : (way + 1) * hr] = value.astype(LOW)

    def fin_owner(tile):
        n = array(tile, 0)
        return 2 * tile + jnp.where((n == 1) | (n == 2), 1, 0), n // 2

    def fin_copy(tile):
        owner, i = fin_owner(tile)
        return remote(fin.at[tile], kv_got.at[z, i], fin_send.at[tile], fin_recv.at[z, i], owner)

    def fin_sends(tile):
        owner, i = fin_owner(tile)

        @pl.when(owner == me)
        def _():
            kv_got[z, i] = fin[tile]

        @pl.when(owner != me)
        def _():
            fin_copy(tile).start()

    def dq_sends(tile):
        for u in range(2):
            n = 2 * tile + u

            @pl.when(n == me)
            def _():
                dq_got[z, x] = dq_stage[n]

            @pl.when(n != me)
            def _():
                dq_copy(n).start()

    def x_on(r):
        return x_copy(
            x_all.at[lax.rem(column + 2 * r, wide)], lax.rem(column + 2 * r, wide), twin, xf_send.at[r]
        )

    @pl.loop(0, tiles // 2)
    def _(j):
        pair_wait(j)
        group(True, j)

        @pl.when(lax.rem(j, 2) == 1)
        def _():
            second_on(2 + j // 2)

    for plane in (partner, nz - 1 - partner):
        for c in range(nx):
            q_wait(at(plane, near(0, c)[1]))

    @pl.loop(0, tiles // 2)
    def _(j):
        group(False, j)

    @pl.loop(tiles // 2, tiles)
    def _(j):
        pair_wait(j)

        odd = lax.rem(tiles - 1 - j, 2)

        @pl.when(odd == 1)
        def _():
            scores(j, (j, True), (j + 1, False))

        @pl.when(odd == 0)
        def _():
            scores(j, (j, True))

        @pl.loop(0, (tiles - 1 - j) // 2)
        def _(n):
            t = j + 1 + odd + 2 * n
            scores(j, (t, False), (t + 1, False))

        stat_copy(j - tiles // 2).start()

        @pl.when(j < tiles - 1)
        def _():
            stat_copy(j).start()

    for r in range(1, wide // 2):
        source = lax.rem(column + 2 * r, wide)
        pltpu.make_async_remote_copy(
            src_ref=x_all.at[source], dst_ref=x_all.at[source], send_sem=xf_send.at[r],
            recv_sem=x_recv.at[source], device_id={"tp": twin},
        ).wait_recv()
        x_on(r).start()
    stat_copy(tiles - 1).start()

    middle, low_tiles = tiles // 4, tiles // 4
    upper = tiles // 2

    def step(s, carry):
        last = middle + upper
        t = jnp.where(
            s < middle, upper - 1 - s, jnp.where(s < last, tiles - 1 + middle - s, last + low_tiles - 1 - s)
        )
        sent_tile = tiles - 1 + middle - s

        def stage(lag, work, begin=upper):
            tile = sent_tile + lag
            pl.when((tile >= begin) & (tile < tiles))(lambda: work(tile))

        stage(4, second_sends)
        backward(t)
        dq_sends(t)
        stage(0, first_sends)
        stage(3, add_on_way)
        return carry

    lax.fori_loop(0, tiles, step, 0)
    for tile in range(upper - 1, low_tiles - 1, -1):
        stage_parts(tile)
    second_sends(5)
    for tile in range(low_tiles - 1, -1, -1):
        first_sends(tile)
    for tile in range(upper - 1, low_tiles - 1, -1):
        first_sends(tile)

    for r in range(nz):
        for c in range(nx):
            if (r, c) != (0, 0):
                zs, xs = near(r, c)
                arrived(dq_got.at[zs, xs], dq_recv.at[at(zs, xs)])
    for h in range(heads):
        for n in range(nx):
            value = dq_got[h * halves, n].astype(jnp.float32)
            for m in range(1, halves):
                value = value + dq_got[h * halves + m, n].astype(jnp.float32)
            low[n * sub : (n + 1) * sub, h * HEAD : (h + 1) * HEAD] = value.astype(LOW)
    low_copy = pltpu.make_async_copy(low, low_out, out_sem.at[0])
    for r in range(wide // 2):
        source = lax.rem(twin + 2 * r, wide)
        pltpu.make_async_remote_copy(
            src_ref=x_all.at[source], dst_ref=x_all.at[source], send_sem=x_send.at[0],
            recv_sem=x_recv.at[source], device_id={"tp": twin},
        ).wait_recv()

    def term(c):
        begin = c * span
        xs = x_all[begin // x_width, :, pl.ds(pl.multiple_of(lax.rem(begin, x_width), span), span)]
        return lax.dot_general(xs, low[...], (((0,), (0,)), ((), ())), preferred_element_type=jnp.float32)

    waiting = []

    def flush():
        for copy in waiting:
            go(copy)
        waiting.clear()

    between = {
        1: (lambda: add_on_way(4), lambda: reduce(7)),
        3: (lambda: second_sends(4), lambda: fin_sends(7), lambda: add_on_way(1)),
        5: (lambda: second_sends(1), lambda: reduce(6), lambda: add_on_way(0)),
        7: (lambda: second_sends(0), lambda: fin_sends(6), lambda: add_on_way(3)),
        9: (lambda: second_sends(3), lambda: reduce(5), lambda: add_on_way(2)),
        11: (lambda: second_sends(2), lambda: fin_sends(5), lambda: reduce(4)),
        13: (lambda: fin_sends(4),),
    }
    order = [(r, c) for r in range(1, nz) for c in range(1, nx)]
    order += [(0, c) for c in range(1, nx)] + [(r, 0) for r in range(1, nz)] + [(0, 0)]
    for count, (r, c) in enumerate(order):
        for work in between.get(count, ()):
            work()
        zt, xt = near(r, c)
        value = term(at(zt, xt))
        fresh = []
        if c:
            wa_stage[r, c] = value[:part_rows].astype(LOW)
            fresh.append(
                remote(wa_stage.at[r, c], wa_red.at[x, zt], wa_send.at[r, c], wa_recv.at[x, zt], at(z, xt))
            )
        else:
            wa_own[r] = value[:part_rows]
        if r:
            wb_stage[r, c] = value[part_rows:].astype(LOW)
            fresh.append(
                remote(wb_stage.at[r, c], wb_red.at[z, xt], wb_send.at[r, c], wb_recv.at[z, xt], at(zt, x))
            )
        else:
            wb_own[c] = value[part_rows:]
        flush()
        waiting.extend(fresh)
    flush()
    low_copy.start()

    @pl.loop(0, 4)
    def _(n):
        reduce(3 - n)

        @pl.when(n > 0)
        def _():
            fin_sends(4 - n)


    for n in list(range(1, nz)) + [0]:
        if n == 2:
            fin_sends(0)
        zt = near(n, 0)[0]
        value = wa_own[n]
        for c in range(1, nx):
            xs = near(0, c)[1]
            arrived(wa_red.at[xs, zt], wa_recv.at[xs, zt])
            value = value + wa_red[xs, zt].astype(jnp.float32)
        fresh = []
        if n:
            wa_fin[n] = value.astype(LOW)
            fresh.append(remote(wa_fin.at[n], wa_got.at[z], wa_fsend.at[n], wa_frecv.at[z], at(zt, x)))
        else:
            w_sum[:part_rows] = value
        xt = near(0, n)[1]
        value = wb_own[n]
        for r in range(1, nz):
            zs = near(r, 0)[0]
            arrived(wb_red.at[zs, xt], wb_recv.at[zs, xt])
            value = value + wb_red[zs, xt].astype(jnp.float32)
        if n:
            wb_fin[n] = value.astype(LOW)
            fresh.append(remote(wb_fin.at[n], wb_got.at[x], wb_fsend.at[n], wb_frecv.at[x], at(z, xt)))
        else:
            w_sum[part_rows:] = value
        flush()
        waiting.extend(fresh)
    flush()

    my_tile = me // 2
    for r in range(nz):
        zs = near(r, 0)[0]
        for i in range(2):
            if r == 0:
                owner, mine = fin_owner(my_tile)

                @pl.when(jnp.logical_not((owner == me) & (mine == i)))
                def _():
                    arrived(kv_got.at[zs, i], fin_recv.at[zs, i])
            else:
                arrived(kv_got.at[zs, i], fin_recv.at[zs, i])
    kv_copy = pltpu.make_async_copy(kv_got, kv_out, out_sem.at[1])
    kv_copy.start()
    for n in range(1, nz):
        zs = near(n, 0)[0]
        arrived(wa_got.at[zs], wa_frecv.at[zs])
        w_sum[:part_rows] += wa_got[zs].astype(jnp.float32)
        xs = near(0, n)[1]
        arrived(wb_got.at[xs], wb_frecv.at[xs])
        w_sum[part_rows:] += wb_got[xs].astype(jnp.float32)

    w_copy = pltpu.make_async_copy(w_sum, w_out, out_sem.at[2])
    w_copy.start()
    low_copy.wait()
    kv_copy.wait()
    for copy in sent:
        copy.wait_send()
    for r in range(1, wide // 2):
        x_on(r).wait_send()

    @pl.loop(0, nz)
    def _(p):
        for i in range(2):
            for c in (1, nx - 1):
                round_copy(p, c, i).wait_send()
            onward_copy(p, i).wait_send()

    @pl.loop(0, tiles)
    def _(t):
        stat_copy(t).wait_send()

    @pl.loop(0, blocks)
    def _(n):
        @pl.when(n != me)
        def _():
            dq_copy(n).wait_send()

    @pl.loop(0, tiles)
    def _(tile):
        for way in range(2):
            opposite_copy(tile, way).wait_send()
            for side in range(2):
                near_copy(tile, side, way).wait_send()

        @pl.when(fin_owner(tile)[0] != me)
        def _():
            fin_copy(tile).wait_send()

    w_copy.wait()


def attention(blocks, wide, q, g, k, v, logits, x):
    rows, cols = k.shape
    heads = cols // HEAD
    nx = NX
    nz = blocks // nx
    halves = nz // heads
    hk = rows // halves
    sub = rows // nx
    tiles = blocks // 2
    anywhere = pl.BlockSpec(memory_space=pl.ANY)
    f32 = jnp.float32
    dma = pltpu.SemaphoreType.DMA
    span = x.shape[1] * wide // blocks
    part = span // 2
    return pl.pallas_call(
        lambda *refs: kernel_body(heads, wide, *refs),
        out_shape=(
            jax.ShapeDtypeStruct((rows, cols), LOW),
            jax.ShapeDtypeStruct((nz, 2, hk, HEAD), LOW),
            jax.ShapeDtypeStruct((span, cols), f32),
        ),
        in_specs=[anywhere] * 6,
        out_specs=(anywhere,) * 3,
        scratch_shapes=[
            pltpu.VMEM((rows, cols), LOW),
            pltpu.VMEM((rows, cols), LOW),
            pltpu.VMEM((rows, cols), LOW),
            pltpu.VMEM((rows, cols), LOW),
            pltpu.VMEM((heads, rows), f32),
            pltpu.VMEM((heads, 8, HEAD), f32),
            pltpu.VMEM((span, cols), f32),
            pltpu.VMEM((blocks, 2, hk, HEAD), LOW),
            pltpu.VMEM((blocks, 2, sub, HEAD), LOW),
            pltpu.VMEM((blocks, 8, HEAD), f32),
            pltpu.VMEM((tiles, HEAD, 2 * hk), LOW),
            pltpu.VMEM((blocks, hk, HEAD), f32),
            pltpu.VMEM((tiles * (tiles + 1) // 2, 2 * hk, 2 * sub), f32),
            pltpu.VMEM((tiles * (tiles + 1) // 2, 8, 2 * sub), f32),
            pltpu.VMEM((2, tiles, 2 * hk, HEAD), f32),
            pltpu.VMEM((HEAD, 2 * sub), f32),
            pltpu.VMEM((tiles, 8, 2 * sub), f32),
            pltpu.VMEM((tiles, 8, 2 * sub), f32),
            pltpu.VMEM((blocks, sub, HEAD), LOW),
            pltpu.VMEM((tiles, nx, hk, HEAD), LOW),
            pltpu.VMEM((tiles, 2, hk // 2, HEAD), LOW),
            pltpu.VMEM((tiles, 2, 2, hk // 2, HEAD), LOW),
            pltpu.VMEM((tiles, hk, HEAD), LOW),
            pltpu.VMEM((nz, nx, sub, HEAD), LOW),
            pltpu.VMEM((nz, 2, hk, HEAD), LOW),
            pltpu.VMEM((wide, rows, x.shape[1]), LOW),
            pltpu.VMEM((rows, cols), LOW),
            pltpu.VMEM((nz, nx, part, cols), LOW),
            pltpu.VMEM((nz, nx, part, cols), LOW),
            pltpu.VMEM((nx, nz, part, cols), LOW),
            pltpu.VMEM((nz, nx, part, cols), LOW),
            pltpu.VMEM((nz, part, cols), f32),
            pltpu.VMEM((nx, part, cols), f32),
            pltpu.VMEM((nz, part, cols), LOW),
            pltpu.VMEM((nx, part, cols), LOW),
            pltpu.VMEM((nz, part, cols), LOW),
            pltpu.VMEM((nx, part, cols), LOW),
            dma((6,)), dma((3,)),
            dma((blocks, 2)), dma((nz, 2, 2)), dma((nz, 2)), dma((nz, 2)), dma((blocks, 2)), dma((heads, nx, 2)),
            dma((heads, nx, 2)), dma((nz, nx)), dma((blocks,)), dma((6,)),
            dma((tiles,)), dma((tiles,)), dma((blocks,)), dma((blocks,)), dma((tiles, nx, 2)), dma((tiles, 2)),
            dma((tiles, 2, 2)), dma((tiles,)), dma((nz, 2)),
            dma((wide // 2,)), dma((wide // 2,)), dma((wide,)),
            dma((nz, nx)), dma((nz, nx)), dma((nx, nz)), dma((nz, nx)),
            dma((nz,)), dma((nx,)), dma((nz,)), dma((nx,)),
        ],
        compiler_params=pltpu.CompilerParams(
            vmem_limit_bytes=62 * 1024 * 1024, collective_id=0, has_side_effects=True
        ),
        cost_estimate=pl.CostEstimate(
            flops=10 * blocks * blocks * rows * sub * HEAD, bytes_accessed=1 << 22, transcendentals=0
        ),
        name="attention",
    )(q, g, k, v, logits, x)


def finish_body(
    heads, low_hbm, kv_hbm, w_hbm, dq_out, dk_out, dv_out, w_out, low, kv, w, dq, dk, dv, in_sem, out_sem
):
    halves = kv.shape[0] // heads
    hk = kv.shape[2]
    loads = [
        pltpu.make_async_copy(src, dst, in_sem.at[n])
        for n, (src, dst) in enumerate(((low_hbm, low), (kv_hbm, kv), (w_hbm, w)))
    ]
    for copy in loads:
        copy.start()
    stores = [
        pltpu.make_async_copy(src, dst, out_sem.at[n])
        for n, (src, dst) in enumerate(((dq, dq_out), (dk, dk_out), (dv, dv_out), (w, w_out)))
    ]
    loads[0].wait()
    dq[...] = low[...].astype(jnp.float32)
    stores[0].start()
    loads[1].wait()
    for i, grad in enumerate((dk, dv)):
        for h in range(heads):
            for m in range(halves):
                grad[m * hk : (m + 1) * hk, h * HEAD : (h + 1) * HEAD] = kv[h * halves + m, i].astype(jnp.float32)
        stores[1 + i].start()
    loads[2].wait()
    stores[3].start()
    for copy in stores:
        copy.wait()


def finish(heads, low, kv, w):
    anywhere = pl.BlockSpec(memory_space=pl.ANY)
    f32 = jnp.float32
    grad = jax.ShapeDtypeStruct(low.shape, f32)
    return pl.pallas_call(
        lambda *refs: finish_body(heads, *refs),
        out_shape=(grad, grad, grad, jax.ShapeDtypeStruct(w.shape, f32)),
        in_specs=[anywhere] * 3,
        out_specs=(anywhere,) * 4,
        scratch_shapes=[
            pltpu.VMEM(low.shape, LOW), pltpu.VMEM(kv.shape, LOW), pltpu.VMEM(w.shape, f32),
            pltpu.VMEM(low.shape, f32), pltpu.VMEM(low.shape, f32), pltpu.VMEM(low.shape, f32),
            pltpu.SemaphoreType.DMA((3,)), pltpu.SemaphoreType.DMA((4,)),
        ],
        compiler_params=pltpu.CompilerParams(vmem_limit_bytes=62 * 1024 * 1024),
        name="finish",
    )(low, kv, w)


def local(queries, keys, values, forget_logits, layer_input, out_grad):
    heads = queries.shape[1] // HEAD
    blocks = lax.axis_size("sp")
    wide = lax.axis_size("tp")
    pieces = attention(blocks, wide, queries, out_grad, keys, values, forget_logits.T, layer_input)
    return finish(heads, *pieces)


def solution(mesh):
    spec = P("sp", "tp")
    return jax.shard_map(
        local, mesh=mesh, in_specs=(spec,) * 6, out_specs=(spec,) * 4, check_vma=False
    )
```

```python
import jax
import jax.numpy as jnp
from jax import lax
from jax.experimental import pallas as pl
from jax.experimental.pallas import tpu as pltpu
from jax.sharding import PartitionSpec as P

HEAD = 128
LOG2E = 1.4426950408889634
SCALE = HEAD ** (-0.5)
LOW = jnp.bfloat16
NX = 4


def nt(a, b):
    return lax.dot_general(a, b, (((1,), (1,)), ((), ())), preferred_element_type=jnp.float32)


def nn(a, b):
    return lax.dot_general(a, b, (((1,), (0,)), ((), ())), preferred_element_type=jnp.float32)


def kernel_body(
    heads, wide,
    q_hbm, g_hbm, k_hbm, v_hbm, logits_hbm, x_hbm,
    low_out, kv_out, w_out,
    q_in, g_in, k_in, v_in, logits, gate_in, w_sum, kv, qg, gates, kt, bias, wbuf, mrow, grads, acc, stat, stat_got,
    dq_stage, part_stage, mid, red, fin, dq_got, kv_got,
    x_all, low, wa_stage, wb_stage, wa_red, wb_red, wa_own, wb_own, wa_fin, wb_fin, wa_got, wb_got,
    in_sem, out_sem, kv_recv, xs_send, col_send, x2_send, qg_recv, q_send, qf_send, gate_send, gate_recv, local_sem,
    stat_send, stat_recv, dq_send, dq_recv, part_send, mid_recv, red_recv, fin_send, fin_recv,
    x_send, xf_send, x_recv, wa_send, wb_send, wa_recv, wb_recv, wa_fsend, wb_fsend, wa_frecv, wb_frecv,
):
    blocks, _, hk, _ = kv.shape
    nx = NX
    nz = blocks // nx
    halves = nz // heads
    sub = qg.shape[2]
    tiles = blocks // 2
    span = w_out.shape[0]
    part_rows = span // 2
    x_width = x_hbm.shape[1]
    column = lax.axis_index("tp")
    me = lax.axis_index("sp")
    z = me // nx
    x = lax.rem(me, nx)
    head = z // halves
    half = lax.rem(z, halves)

    def at(zt, xt):
        return zt * nx + xt

    def near(r, c):
        return lax.rem(z + r, nz), lax.rem(x + c, nx)

    def remote(src, dst, send, recv, target):
        return pltpu.make_async_remote_copy(
            src_ref=src, dst_ref=dst, send_sem=send, recv_sem=recv, device_id={"sp": target}
        )

    def arrived(ref, recv):
        remote(ref, ref, dq_send.at[0], recv, me).wait_recv()

    barrier = pltpu.get_barrier_semaphore()
    for r in range(1, blocks):
        pl.semaphore_signal(barrier, inc=1, device_id={"sp": lax.rem(me + r, blocks)})
    for r in range(1, wide):
        pl.semaphore_signal(barrier, inc=1, device_id={"tp": lax.rem(column + r, wide)})

    def lanes(h):
        return pl.ds(pl.multiple_of(h * HEAD, HEAD), HEAD)

    sent = []

    def go(copy):
        copy.start()
        sent.append(copy)

    kv_in = (k_in, v_in)
    qg_in = (q_in, g_in)

    def kv_source(i, zt):
        begin = pl.multiple_of(lax.rem(zt, halves) * hk, hk)
        return kv_in[i].at[pl.ds(begin, hk), lanes(zt // halves)]

    def q_source(i, zt, xt):
        begin = pl.multiple_of(xt * sub, sub)
        return qg_in[i].at[pl.ds(begin, sub), lanes(zt // halves)]

    loads = [
        pltpu.make_async_copy(src, dst, in_sem.at[n])
        for n, (src, dst) in enumerate(
            ((logits_hbm, logits), (k_hbm, k_in), (v_hbm, v_in), (q_hbm, q_in), (g_hbm, g_in), (x_hbm, x_all.at[column]))
        )
    ]
    for copy in loads:
        copy.start()

    width = 2 * sub
    keys_wide = 2 * hk
    line = lax.broadcasted_iota(jnp.int32, (8, width), 0)

    @pl.loop(0, tiles)
    def _(j):
        grads[0, j] = jnp.zeros((keys_wide, HEAD), jnp.float32)
        grads[1, j] = jnp.zeros((keys_wide, HEAD), jnp.float32)
        stat[j] = jnp.where(line == 0, -1e30, 0.0)

    loads[0].wait()
    chunks = logits.shape[1] // HEAD
    raw = jnp.concatenate(
        [logits[h : h + 1, u * HEAD : (u + 1) * HEAD] for h in range(heads) for u in range(chunks)], axis=0
    )
    logs = (jnp.minimum(raw, 0.0) - jnp.log1p(jnp.exp(-jnp.abs(raw)))) * LOG2E
    upto = lax.broadcasted_iota(jnp.int32, (HEAD, HEAD), 0) <= lax.broadcasted_iota(jnp.int32, (HEAD, HEAD), 1)
    sums = jnp.dot(
        logs, upto.astype(jnp.float32), precision=lax.Precision.HIGHEST, preferred_element_type=jnp.float32
    )
    for h in range(heads):
        base = jnp.zeros((1, HEAD), jnp.float32)
        for u in range(chunks):
            line = sums[h * chunks + u : h * chunks + u + 1]
            gate_in[h, u : u + 1] = line + base
            base = base + jnp.broadcast_to(line[:, HEAD - 1 :], (1, HEAD))
        gate_in[h, chunks:] = jnp.broadcast_to(base, (gate_in.shape[1] - chunks, HEAD))

    for copy in loads[1:]:
        copy.wait()
    own = [pltpu.make_async_copy(kv_source(i, z), kv.at[me, i], local_sem.at[i]) for i in range(2)]
    own += [pltpu.make_async_copy(q_source(i, z, x), qg.at[me, i], local_sem.at[2 + i]) for i in range(2)]
    own += [pltpu.make_async_copy(gate_in.at[head], gates.at[me], local_sem.at[4])]
    for copy in own:
        copy.start()
    for copy in own:
        copy.wait()
    pl.semaphore_wait(barrier, blocks + wide - 2)

    for r in range(nz):
        for c in range(nx):
            if (r, c) == (0, 0):
                continue
            zt, xt = near(r, c)
            go(remote(gate_in.at[zt // halves], gates.at[me], gate_send.at[r, c], gate_recv.at[me], at(zt, xt)))

    def kv_arrived(j, i):
        arrived(kv.at[j, i], kv_recv.at[j, i])

    def round_copy(p, c, i):
        j = at(p, x)
        return remote(kv.at[j, i], kv.at[j, i], xs_send.at[p, c // 2, i], kv_recv.at[j, i], at(z, near(0, c)[1]))

    for i in range(2):
        for c in (1, nx - 1):
            round_copy(z, c, i).start()

    for r in (1, nz - 1, 2):
        zt = near(r, 0)[0]
        for i in range(2):
            go(remote(kv_source(i, zt), kv.at[me, i], col_send.at[r, i], kv_recv.at[me, i], at(zt, x)))

    across = nz - 1 - z
    partner = z + 1 - 2 * half

    def q_plane(r):
        return z if r == 0 else across

    for i in range(2):
        go(remote(q_source(i, z, x), qg.at[me, i], qf_send.at[0, 0, i], qg_recv.at[me, i], at(partner, x)))
    for r in range(heads):
        for c in range(nx):
            if (r, c) == (0, 0):
                continue
            zt, xt = q_plane(r), near(0, c)[1]
            for i in range(2):
                go(remote(q_source(i, zt, xt), qg.at[me, i], q_send.at[r, c, i], qg_recv.at[me, i], at(zt, xt)))

    def x_copy(src, source, target, send):
        return pltpu.make_async_remote_copy(
            src_ref=src, dst_ref=x_all.at[source], send_sem=send, recv_sem=x_recv.at[source], device_id={"tp": target}
        )

    core = lax.rem(column, 2)
    twin = column + 1 - 2 * core
    for r in range(1, wide // 2):
        go(x_copy(x_all.at[column], column, lax.rem(column + 2 * r, wide), x_send.at[r]))
    go(x_copy(x_all.at[column], column, twin, x_send.at[0]))

    def onward_copy(p, i):
        c = nx - 1 if i == 0 else 1
        j = at(p, near(0, c)[1])
        return remote(kv.at[j, i], kv.at[j, i], x2_send.at[p, i], kv_recv.at[j, i], at(z, near(0, nx - c)[1]))

    def column_on(r):
        p = near(r, 0)[0]
        for i in range(2):
            kv_arrived(at(p, x), i)
            for c in (1, nx - 1):
                round_copy(p, c, i).start()

    def second_on(p):
        for i, c in ((0, nx - 1), (1, 1)):
            kv_arrived(at(p, near(0, c)[1]), i)
            onward_copy(p, i).start()

    def q_wait(j):
        for i in range(2):
            arrived(qg.at[j, i], qg_recv.at[j, i])

    def q_on(r, c):
        j = at(q_plane(r), near(0, c)[1])
        q_wait(j)
        for i in range(2):
            go(remote(qg.at[j, i], qg.at[j, i], qf_send.at[r, c, i], qg_recv.at[j, i], at(partner, x)))

    column_on(1)
    column_on(nz - 1)
    for c in range(1, nx):
        if c == 2:
            column_on(2)
        q_on(0, c)
    for r in range(nz):
        for c in range(nx):
            if (r, c) != (0, 0):
                j = at(*near(r, c))
                arrived(gates.at[j], gate_recv.at[j])

    def prepare(j, base):
        per = hk // HEAD
        table = gates[j]
        mine = table[0:per]
        for n in range(1, halves):
            mine = jnp.where(half == n, table[n * per : (n + 1) * per], mine)
        for n in range(per):
            row = mine[n : n + 1] + base
            bias[j, n * HEAD : (n + 1) * HEAD] = jnp.broadcast_to(row, (HEAD, HEAD)).T
        return base + table[halves * per : halves * per + 1]

    lax.fori_loop(0, blocks, prepare, jnp.zeros((1, HEAD), jnp.float32))
    second_on(0)
    second_on(1)
    for c in range(nx):
        q_on(1, c)
    rows = halves * hk
    key_row = lax.broadcasted_iota(jnp.int32, (keys_wide, width), 0)
    query_row = lax.broadcasted_iota(jnp.int32, (keys_wide, width), 1)
    key_pos = jnp.where(key_row >= hk, key_row - hk + rows, key_row) + half * hk
    query_pos = jnp.where(query_row >= sub, query_row - sub + rows, query_row) + x * sub

    def pair(i, j):
        return kv[pl.ds(2 * j, 2), i].reshape(keys_wide, HEAD)

    def queries(i, t):
        return qg[pl.ds(2 * t, 2), i].reshape(width, HEAD)

    def place(t, j):
        return t * (t + 1) // 2 + j

    def scores(j, *group):
        k, v = pair(0, j), pair(1, j)
        column_bias = bias[pl.ds(2 * j, 2)].reshape(keys_wide, HEAD)
        column_bias = jnp.concatenate([column_bias] * (width // HEAD), axis=1)
        states = [stat[t] for t, _ in group]
        results = []
        for (t, masked), state in zip(group, states):
            m, total, terms = state[0:1], state[1:2], state[2:3]
            s = nt(k, queries(0, t)) * (SCALE * LOG2E) - column_bias
            if masked:
                s = jnp.where(key_pos <= query_pos, s, -1e30)
            top = jnp.maximum(m, jnp.max(s, axis=0, keepdims=True))
            w = jnp.exp2(s - top)
            old = jnp.exp2(m - top)
            dp = nt(v, queries(1, t))
            total = total * old + jnp.sum(w, axis=0, keepdims=True)
            terms = terms * old + jnp.sum(w * dp, axis=0, keepdims=True)
            wbuf[place(t, j)] = w
            results.append((top, total, terms))
        for (t, _), (top, total, terms) in zip(group, results):
            mrow[place(t, j)] = jnp.broadcast_to(top, (8, width))
            stat[t] = jnp.concatenate([top, total, terms, jnp.zeros((5, width), jnp.float32)], axis=0)

    def pair_wait(j):
        for u in range(2):
            b = 2 * j + u
            d = lax.rem(lax.rem(b, nx) + nx - x, nx)

            @pl.when((d == 1) | (d == 2))
            def _():
                kv_arrived(b, 0)

            @pl.when((d == nx - 1) | (d == 2))
            def _():
                kv_arrived(b, 1)

        for n in range(2):
            kt[j, :, n * hk : (n + 1) * hk] = kv[2 * j + n, 0].T

    outer = (z == 0) | (z == nz - 1)
    quarter = tiles // 4

    def group(direct, j):
        ends = outer if direct else jnp.logical_not(outer)

        @pl.loop(0, quarter)
        def _(m):
            t = jnp.where(ends, m * 3 * quarter, quarter + m * 2)

            @pl.when(t > j)
            def _():
                scores(j, (t, False), (t + 1, False))

            @pl.when(t == j)
            def _():
                scores(j, (t, True), (t + 1, False))

            @pl.when(t + 1 == j)
            def _():
                scores(j, (t + 1, True))

    def stage_parts(t):
        for n, (u, i) in enumerate(((0, 0), (1, 0), (1, 1), (0, 1))):
            value = grads[i, t, u * hk : (u + 1) * hk]
            part_stage[t, n] = (value * SCALE if i == 0 else value).astype(LOW)

    def backward(t):
        q, g = queries(0, t), queries(1, t)
        arrived(stat_got.at[t], stat_recv.at[t])
        mine = stat[t]
        other = stat_got[t]
        top = jnp.maximum(mine[0:1], other[0:1])
        scale_mine = jnp.exp2(mine[0:1] - top)
        scale_other = jnp.exp2(other[0:1] - top)
        inverse = 1.0 / (mine[1:2] * scale_mine + other[1:2] * scale_other)
        terms = (mine[2:3] * scale_mine + other[2:3] * scale_other) * inverse

        def blocks_of(*pairs):
            added = []
            for j in pairs:
                factor = jnp.exp2(mrow[place(t, j)][0:1] - top) * inverse
                prob = wbuf[place(t, j)] * factor
                ds = (prob * (nt(pair(1, j), g) - terms)).astype(LOW)
                added.append((j, nn(prob.astype(LOW), g), nn(ds, q), nn(kt[j], ds)))
            for j, dv, dk, _ in added:
                grads[1, j] += dv
                grads[0, j] += dk
            acc[...] += sum(term for _, _, _, term in added)

        acc[...] = jnp.zeros((HEAD, width), jnp.float32)
        blocks_of(t)

        @pl.when((t >= tiles // 2) | (t < tiles // 4))
        def _():
            stage_parts(t)

        @pl.loop(0, t // 2)
        def _(n):
            blocks_of(2 * n, 2 * n + 1)

        @pl.when(lax.rem(t, 2) == 1)
        def _():
            blocks_of(t - 1)

        dq_t = (acc[...] * SCALE).T.astype(LOW)
        for n in range(2):
            dq_stage[2 * t + n] = dq_t[n * sub : (n + 1) * sub]

    def stat_copy(t):
        return remote(stat.at[t], stat_got.at[t], stat_send.at[t], stat_recv.at[t], at(partner, x))

    def dq_copy(n):
        return remote(dq_stage.at[n], dq_got.at[z, x], dq_send.at[n], dq_recv.at[me], n)

    hr = hk // 2

    def role(tile):
        return lax.rem(x + nx - 2 * lax.rem(tile, nx // 2), nx)

    def array(tile, c):
        return lax.rem(role(tile) + c, nx)

    def share(tile, n, way):
        u = jnp.where((n == 1) | (n == 2), 1, 0)
        i = n // 2
        value = grads[i, tile, pl.ds(pl.multiple_of(u * hk + way * hr, hr), hr)]
        return value * jnp.where(i == 0, SCALE, 1.0)

    def half_of(tile, n, way):
        return part_stage.at[tile, n, pl.ds(way * hr, hr)]

    def opposite_copy(tile, way):
        n = array(tile, 2)
        return remote(
            half_of(tile, n, way), mid.at[tile, way], part_send.at[tile, n, way], mid_recv.at[tile, way],
            at(z, near(0, nx - 1 if way else 1)[1]),
        )

    def near_copy(tile, side, way):
        c = nx - 1 if side else 1
        n = array(tile, c)
        return remote(
            half_of(tile, n, way), red.at[tile, side, way], part_send.at[tile, n, way], red_recv.at[tile, side, way],
            at(z, near(0, c)[1]),
        )

    def first_sends(tile):
        for way in range(2):
            opposite_copy(tile, way).start()
        near_copy(tile, 0, 1).start()
        near_copy(tile, 1, 0).start()

    def add_on_way(tile):
        for way, c in ((0, 1), (1, nx - 1)):
            n = array(tile, c)
            arrived(mid.at[tile, way], mid_recv.at[tile, way])
            part_stage[tile, n, way * hr : (way + 1) * hr] = (
                share(tile, n, way) + mid[tile, way].astype(jnp.float32)
            ).astype(LOW)

    def second_sends(tile):
        near_copy(tile, 0, 0).start()
        near_copy(tile, 1, 1).start()

    def reduce(tile):
        n = array(tile, 0)
        for way in range(2):
            value = share(tile, n, way)
            for side in range(2):
                arrived(red.at[tile, side, way], red_recv.at[tile, side, way])
                value = value + red[tile, side, way].astype(jnp.float32)
            fin[tile, way * hr : (way + 1) * hr] = value.astype(LOW)

    def fin_owner(tile):
        n = array(tile, 0)
        return 2 * tile + jnp.where((n == 1) | (n == 2), 1, 0), n // 2

    def fin_copy(tile):
        owner, i = fin_owner(tile)
        return remote(fin.at[tile], kv_got.at[z, i], fin_send.at[tile], fin_recv.at[z, i], owner)

    def fin_sends(tile):
        owner, i = fin_owner(tile)

        @pl.when(owner == me)
        def _():
            kv_got[z, i] = fin[tile]

        @pl.when(owner != me)
        def _():
            fin_copy(tile).start()

    def dq_sends(tile):
        for u in range(2):
            n = 2 * tile + u

            @pl.when(n == me)
            def _():
                dq_got[z, x] = dq_stage[n]

            @pl.when(n != me)
            def _():
                dq_copy(n).start()

    def x_on(r):
        return x_copy(
            x_all.at[lax.rem(column + 2 * r, wide)], lax.rem(column + 2 * r, wide), twin, xf_send.at[r]
        )

    @pl.loop(0, tiles // 2)
    def _(j):
        pair_wait(j)
        group(True, j)

        @pl.when(lax.rem(j, 2) == 1)
        def _():
            second_on(2 + j // 2)

    for plane in (partner, nz - 1 - partner):
        for c in range(nx):
            q_wait(at(plane, near(0, c)[1]))

    @pl.loop(0, tiles // 2)
    def _(j):
        group(False, j)

    @pl.loop(0, tiles // 2)
    def _(t):
        stat_copy(t).start()

    @pl.loop(tiles // 2, tiles)
    def _(j):
        pair_wait(j)

        odd = lax.rem(tiles - 1 - j, 2)

        @pl.when(odd == 1)
        def _():
            scores(j, (j, True), (j + 1, False))

        @pl.when(odd == 0)
        def _():
            scores(j, (j, True))

        @pl.loop(0, (tiles - 1 - j) // 2)
        def _(n):
            t = j + 1 + odd + 2 * n
            scores(j, (t, False), (t + 1, False))

        @pl.when(j < tiles - 1)
        def _():
            stat_copy(j).start()

    for r in range(1, wide // 2):
        source = lax.rem(column + 2 * r, wide)
        pltpu.make_async_remote_copy(
            src_ref=x_all.at[source], dst_ref=x_all.at[source], send_sem=xf_send.at[r],
            recv_sem=x_recv.at[source], device_id={"tp": twin},
        ).wait_recv()
        x_on(r).start()
    stat_copy(tiles - 1).start()

    middle, low_tiles = tiles // 4, tiles // 4
    upper = tiles // 2

    def step(s, carry):
        last = middle + upper
        t = jnp.where(
            s < middle, upper - 1 - s, jnp.where(s < last, tiles - 1 + middle - s, last + low_tiles - 1 - s)
        )
        sent_tile = tiles - 1 + middle - s

        def stage(lag, work, begin=upper):
            tile = sent_tile + lag
            pl.when((tile >= begin) & (tile < tiles))(lambda: work(tile))

        stage(4, second_sends)
        backward(t)
        dq_sends(t)
        stage(0, first_sends)
        stage(3, add_on_way)
        return carry

    lax.fori_loop(0, tiles, step, 0)
    for tile in range(upper - 1, low_tiles - 1, -1):
        stage_parts(tile)
    second_sends(5)
    for tile in range(upper - 1, -1, -1):
        first_sends(tile)
    add_on_way(4)
    reduce(7)
    second_sends(4)
    add_on_way(3)
    fin_sends(7)
    add_on_way(2)
    second_sends(3)
    reduce(6)
    second_sends(2)
    add_on_way(1)
    fin_sends(6)
    add_on_way(0)
    second_sends(1)
    reduce(5)
    second_sends(0)
    reduce(4)
    fin_sends(5)

    for r in range(nz):
        for c in range(nx):
            if (r, c) != (0, 0):
                zs, xs = near(r, c)
                arrived(dq_got.at[zs, xs], dq_recv.at[at(zs, xs)])
    for h in range(heads):
        for n in range(nx):
            value = dq_got[h * halves, n].astype(jnp.float32)
            for m in range(1, halves):
                value = value + dq_got[h * halves + m, n].astype(jnp.float32)
            low[n * sub : (n + 1) * sub, h * HEAD : (h + 1) * HEAD] = value.astype(LOW)
    low_copy = pltpu.make_async_copy(low, low_out, out_sem.at[0])
    fin_sends(4)
    for r in range(wide // 2):
        source = lax.rem(twin + 2 * r, wide)
        pltpu.make_async_remote_copy(
            src_ref=x_all.at[source], dst_ref=x_all.at[source], send_sem=x_send.at[0],
            recv_sem=x_recv.at[source], device_id={"tp": twin},
        ).wait_recv()

    def term(c):
        begin = c * span
        xs = x_all[begin // x_width, :, pl.ds(pl.multiple_of(lax.rem(begin, x_width), span), span)]
        return lax.dot_general(xs, low[...], (((0,), (0,)), ((), ())), preferred_element_type=jnp.float32)

    waiting = []

    def flush():
        for copy in waiting:
            go(copy)
        waiting.clear()

    order = [(r, c) for r in range(1, nz) for c in range(1, nx)]
    order += [(0, c) for c in range(1, nx)] + [(r, 0) for r in range(1, nz)] + [(0, 0)]
    for r, c in order:
        zt, xt = near(r, c)
        value = term(at(zt, xt))
        fresh = []
        if c:
            wa_stage[r, c] = value[:part_rows].astype(LOW)
            fresh.append(
                remote(wa_stage.at[r, c], wa_red.at[x, zt], wa_send.at[r, c], wa_recv.at[x, zt], at(z, xt))
            )
        else:
            wa_own[r] = value[:part_rows]
        if r:
            wb_stage[r, c] = value[part_rows:].astype(LOW)
            fresh.append(
                remote(wb_stage.at[r, c], wb_red.at[z, xt], wb_send.at[r, c], wb_recv.at[z, xt], at(zt, x))
            )
        else:
            wb_own[c] = value[part_rows:]
        flush()
        waiting.extend(fresh)
    flush()
    low_copy.start()

    @pl.loop(0, 4)
    def _(n):
        reduce(3 - n)

        @pl.when(n > 0)
        def _():
            fin_sends(4 - n)


    for n in list(range(1, nz)) + [0]:
        if n == 2:
            fin_sends(0)
        zt = near(n, 0)[0]
        value = wa_own[n]
        for c in range(1, nx):
            xs = near(0, c)[1]
            arrived(wa_red.at[xs, zt], wa_recv.at[xs, zt])
            value = value + wa_red[xs, zt].astype(jnp.float32)
        fresh = []
        if n:
            wa_fin[n] = value.astype(LOW)
            fresh.append(remote(wa_fin.at[n], wa_got.at[z], wa_fsend.at[n], wa_frecv.at[z], at(zt, x)))
        else:
            w_sum[:part_rows] = value
        xt = near(0, n)[1]
        value = wb_own[n]
        for r in range(1, nz):
            zs = near(r, 0)[0]
            arrived(wb_red.at[zs, xt], wb_recv.at[zs, xt])
            value = value + wb_red[zs, xt].astype(jnp.float32)
        if n:
            wb_fin[n] = value.astype(LOW)
            fresh.append(remote(wb_fin.at[n], wb_got.at[x], wb_fsend.at[n], wb_frecv.at[x], at(z, xt)))
        else:
            w_sum[part_rows:] = value
        flush()
        waiting.extend(fresh)
    flush()

    my_tile = me // 2
    for r in range(nz):
        zs = near(r, 0)[0]
        for i in range(2):
            if r == 0:
                owner, mine = fin_owner(my_tile)

                @pl.when(jnp.logical_not((owner == me) & (mine == i)))
                def _():
                    arrived(kv_got.at[zs, i], fin_recv.at[zs, i])
            else:
                arrived(kv_got.at[zs, i], fin_recv.at[zs, i])
    kv_copy = pltpu.make_async_copy(kv_got, kv_out, out_sem.at[1])
    kv_copy.start()
    for n in range(1, nz):
        zs = near(n, 0)[0]
        arrived(wa_got.at[zs], wa_frecv.at[zs])
        w_sum[:part_rows] += wa_got[zs].astype(jnp.float32)
        xs = near(0, n)[1]
        arrived(wb_got.at[xs], wb_frecv.at[xs])
        w_sum[part_rows:] += wb_got[xs].astype(jnp.float32)

    w_copy = pltpu.make_async_copy(w_sum, w_out, out_sem.at[2])
    w_copy.start()
    low_copy.wait()
    kv_copy.wait()
    for copy in sent:
        copy.wait_send()
    for r in range(1, wide // 2):
        x_on(r).wait_send()

    @pl.loop(0, nz)
    def _(p):
        for i in range(2):
            for c in (1, nx - 1):
                round_copy(p, c, i).wait_send()
            onward_copy(p, i).wait_send()

    @pl.loop(0, tiles)
    def _(t):
        stat_copy(t).wait_send()

    @pl.loop(0, blocks)
    def _(n):
        @pl.when(n != me)
        def _():
            dq_copy(n).wait_send()

    @pl.loop(0, tiles)
    def _(tile):
        for way in range(2):
            opposite_copy(tile, way).wait_send()
            for side in range(2):
                near_copy(tile, side, way).wait_send()

        @pl.when(fin_owner(tile)[0] != me)
        def _():
            fin_copy(tile).wait_send()

    w_copy.wait()


def attention(blocks, wide, q, g, k, v, logits, x):
    rows, cols = k.shape
    heads = cols // HEAD
    nx = NX
    nz = blocks // nx
    halves = nz // heads
    hk = rows // halves
    sub = rows // nx
    tiles = blocks // 2
    anywhere = pl.BlockSpec(memory_space=pl.ANY)
    f32 = jnp.float32
    dma = pltpu.SemaphoreType.DMA
    span = x.shape[1] * wide // blocks
    part = span // 2
    return pl.pallas_call(
        lambda *refs: kernel_body(heads, wide, *refs),
        out_shape=(
            jax.ShapeDtypeStruct((rows, cols), LOW),
            jax.ShapeDtypeStruct((nz, 2, hk, HEAD), LOW),
            jax.ShapeDtypeStruct((span, cols), f32),
        ),
        in_specs=[anywhere] * 6,
        out_specs=(anywhere,) * 3,
        scratch_shapes=[
            pltpu.VMEM((rows, cols), LOW),
            pltpu.VMEM((rows, cols), LOW),
            pltpu.VMEM((rows, cols), LOW),
            pltpu.VMEM((rows, cols), LOW),
            pltpu.VMEM((heads, rows), f32),
            pltpu.VMEM((heads, 8, HEAD), f32),
            pltpu.VMEM((span, cols), f32),
            pltpu.VMEM((blocks, 2, hk, HEAD), LOW),
            pltpu.VMEM((blocks, 2, sub, HEAD), LOW),
            pltpu.VMEM((blocks, 8, HEAD), f32),
            pltpu.VMEM((tiles, HEAD, 2 * hk), LOW),
            pltpu.VMEM((blocks, hk, HEAD), f32),
            pltpu.VMEM((tiles * (tiles + 1) // 2, 2 * hk, 2 * sub), f32),
            pltpu.VMEM((tiles * (tiles + 1) // 2, 8, 2 * sub), f32),
            pltpu.VMEM((2, tiles, 2 * hk, HEAD), f32),
            pltpu.VMEM((HEAD, 2 * sub), f32),
            pltpu.VMEM((tiles, 8, 2 * sub), f32),
            pltpu.VMEM((tiles, 8, 2 * sub), f32),
            pltpu.VMEM((blocks, sub, HEAD), LOW),
            pltpu.VMEM((tiles, nx, hk, HEAD), LOW),
            pltpu.VMEM((tiles, 2, hk // 2, HEAD), LOW),
            pltpu.VMEM((tiles, 2, 2, hk // 2, HEAD), LOW),
            pltpu.VMEM((tiles, hk, HEAD), LOW),
            pltpu.VMEM((nz, nx, sub, HEAD), LOW),
            pltpu.VMEM((nz, 2, hk, HEAD), LOW),
            pltpu.VMEM((wide, rows, x.shape[1]), LOW),
            pltpu.VMEM((rows, cols), LOW),
            pltpu.VMEM((nz, nx, part, cols), LOW),
            pltpu.VMEM((nz, nx, part, cols), LOW),
            pltpu.VMEM((nx, nz, part, cols), LOW),
            pltpu.VMEM((nz, nx, part, cols), LOW),
            pltpu.VMEM((nz, part, cols), f32),
            pltpu.VMEM((nx, part, cols), f32),
            pltpu.VMEM((nz, part, cols), LOW),
            pltpu.VMEM((nx, part, cols), LOW),
            pltpu.VMEM((nz, part, cols), LOW),
            pltpu.VMEM((nx, part, cols), LOW),
            dma((6,)), dma((3,)),
            dma((blocks, 2)), dma((nz, 2, 2)), dma((nz, 2)), dma((nz, 2)), dma((blocks, 2)), dma((heads, nx, 2)),
            dma((heads, nx, 2)), dma((nz, nx)), dma((blocks,)), dma((6,)),
            dma((tiles,)), dma((tiles,)), dma((blocks,)), dma((blocks,)), dma((tiles, nx, 2)), dma((tiles, 2)),
            dma((tiles, 2, 2)), dma((tiles,)), dma((nz, 2)),
            dma((wide // 2,)), dma((wide // 2,)), dma((wide,)),
            dma((nz, nx)), dma((nz, nx)), dma((nx, nz)), dma((nz, nx)),
            dma((nz,)), dma((nx,)), dma((nz,)), dma((nx,)),
        ],
        compiler_params=pltpu.CompilerParams(
            vmem_limit_bytes=62 * 1024 * 1024, collective_id=0, has_side_effects=True
        ),
        cost_estimate=pl.CostEstimate(
            flops=10 * blocks * blocks * rows * sub * HEAD, bytes_accessed=1 << 22, transcendentals=0
        ),
        name="attention",
    )(q, g, k, v, logits, x)


def finish_body(
    heads, low_hbm, kv_hbm, w_hbm, dq_out, dk_out, dv_out, w_out, low, kv, w, dq, dk, dv, in_sem, out_sem
):
    halves = kv.shape[0] // heads
    hk = kv.shape[2]
    loads = [
        pltpu.make_async_copy(src, dst, in_sem.at[n])
        for n, (src, dst) in enumerate(((low_hbm, low), (kv_hbm, kv), (w_hbm, w)))
    ]
    for copy in loads:
        copy.start()
    stores = [
        pltpu.make_async_copy(src, dst, out_sem.at[n])
        for n, (src, dst) in enumerate(((dq, dq_out), (dk, dk_out), (dv, dv_out), (w, w_out)))
    ]
    loads[0].wait()
    dq[...] = low[...].astype(jnp.float32)
    stores[0].start()
    loads[1].wait()
    for i, grad in enumerate((dk, dv)):
        for h in range(heads):
            for m in range(halves):
                grad[m * hk : (m + 1) * hk, h * HEAD : (h + 1) * HEAD] = kv[h * halves + m, i].astype(jnp.float32)
        stores[1 + i].start()
    loads[2].wait()
    stores[3].start()
    for copy in stores:
        copy.wait()


def finish(heads, low, kv, w):
    anywhere = pl.BlockSpec(memory_space=pl.ANY)
    f32 = jnp.float32
    grad = jax.ShapeDtypeStruct(low.shape, f32)
    return pl.pallas_call(
        lambda *refs: finish_body(heads, *refs),
        out_shape=(grad, grad, grad, jax.ShapeDtypeStruct(w.shape, f32)),
        in_specs=[anywhere] * 3,
        out_specs=(anywhere,) * 4,
        scratch_shapes=[
            pltpu.VMEM(low.shape, LOW), pltpu.VMEM(kv.shape, LOW), pltpu.VMEM(w.shape, f32),
            pltpu.VMEM(low.shape, f32), pltpu.VMEM(low.shape, f32), pltpu.VMEM(low.shape, f32),
            pltpu.SemaphoreType.DMA((3,)), pltpu.SemaphoreType.DMA((4,)),
        ],
        compiler_params=pltpu.CompilerParams(vmem_limit_bytes=62 * 1024 * 1024),
        name="finish",
    )(low, kv, w)


def local(queries, keys, values, forget_logits, layer_input, out_grad):
    heads = queries.shape[1] // HEAD
    blocks = lax.axis_size("sp")
    wide = lax.axis_size("tp")
    pieces = attention(blocks, wide, queries, out_grad, keys, values, forget_logits.T, layer_input)
    return finish(heads, *pieces)


def solution(mesh):
    spec = P("sp", "tp")
    return jax.shard_map(
        local, mesh=mesh, in_specs=(spec,) * 6, out_specs=(spec,) * 4, check_vma=False
    )
```

```python
import jax
import jax.numpy as jnp
from jax import lax
from jax.experimental import pallas as pl
from jax.experimental.pallas import tpu as pltpu
from jax.sharding import PartitionSpec as P

HEAD = 128
LOG2E = 1.4426950408889634
SCALE = HEAD ** (-0.5)
LOW = jnp.bfloat16
NX = 4


def nt(a, b):
    return lax.dot_general(a, b, (((1,), (1,)), ((), ())), preferred_element_type=jnp.float32)


def nn(a, b):
    return lax.dot_general(a, b, (((1,), (0,)), ((), ())), preferred_element_type=jnp.float32)


def kernel_body(
    heads, wide,
    q_hbm, g_hbm, k_hbm, v_hbm, logits_hbm, x_hbm,
    low_out, kv_out, w_out,
    q_in, g_in, k_in, v_in, logits, gate_in, w_sum, kv, qg, gates, kt, bias, wbuf, mrow, grads, acc, stat, stat_got,
    dq_stage, part_stage, mid, red, fin, dq_got, kv_got,
    x_all, low, wa_stage, wb_stage, wa_red, wb_red, wa_own, wb_own, wa_fin, wb_fin, wa_got, wb_got,
    in_sem, out_sem, kv_recv, xs_send, col_send, x2_send, qg_recv, q_send, qf_send, gate_send, gate_recv, local_sem,
    stat_send, stat_recv, dq_send, dq_recv, part_send, mid_recv, red_recv, fin_send, fin_recv,
    x_send, xf_send, x_recv, wa_send, wb_send, wa_recv, wb_recv, wa_fsend, wb_fsend, wa_frecv, wb_frecv,
):
    blocks, _, hk, _ = kv.shape
    nx = NX
    nz = blocks // nx
    halves = nz // heads
    sub = qg.shape[2]
    tiles = blocks // 2
    span = w_out.shape[0]
    part_rows = span // 2
    x_width = x_hbm.shape[1]
    column = lax.axis_index("tp")
    me = lax.axis_index("sp")
    z = me // nx
    x = lax.rem(me, nx)
    head = z // halves
    half = lax.rem(z, halves)

    def at(zt, xt):
        return zt * nx + xt

    def near(r, c):
        return lax.rem(z + r, nz), lax.rem(x + c, nx)

    def remote(src, dst, send, recv, target):
        return pltpu.make_async_remote_copy(
            src_ref=src, dst_ref=dst, send_sem=send, recv_sem=recv, device_id={"sp": target}
        )

    def arrived(ref, recv):
        remote(ref, ref, dq_send.at[0], recv, me).wait_recv()

    barrier = pltpu.get_barrier_semaphore()
    for r in range(1, blocks):
        pl.semaphore_signal(barrier, inc=1, device_id={"sp": lax.rem(me + r, blocks)})
    for r in range(1, wide):
        pl.semaphore_signal(barrier, inc=1, device_id={"tp": lax.rem(column + r, wide)})

    def lanes(h):
        return pl.ds(pl.multiple_of(h * HEAD, HEAD), HEAD)

    sent = []

    def go(copy):
        copy.start()
        sent.append(copy)

    kv_in = (k_in, v_in)
    qg_in = (q_in, g_in)

    def kv_source(i, zt):
        begin = pl.multiple_of(lax.rem(zt, halves) * hk, hk)
        return kv_in[i].at[pl.ds(begin, hk), lanes(zt // halves)]

    def q_source(i, zt, xt):
        begin = pl.multiple_of(xt * sub, sub)
        return qg_in[i].at[pl.ds(begin, sub), lanes(zt // halves)]

    loads = [
        pltpu.make_async_copy(src, dst, in_sem.at[n])
        for n, (src, dst) in enumerate(
            ((logits_hbm, logits), (k_hbm, k_in), (v_hbm, v_in), (q_hbm, q_in), (g_hbm, g_in), (x_hbm, x_all.at[column]))
        )
    ]
    for copy in loads:
        copy.start()

    width = 2 * sub
    keys_wide = 2 * hk
    line = lax.broadcasted_iota(jnp.int32, (8, width), 0)

    @pl.loop(0, tiles)
    def _(j):
        grads[0, j] = jnp.zeros((keys_wide, HEAD), jnp.float32)
        grads[1, j] = jnp.zeros((keys_wide, HEAD), jnp.float32)
        stat[j] = jnp.where(line == 0, -1e30, 0.0)

    loads[0].wait()
    chunks = logits.shape[1] // HEAD
    raw = jnp.concatenate(
        [logits[h : h + 1, u * HEAD : (u + 1) * HEAD] for h in range(heads) for u in range(chunks)], axis=0
    )
    logs = (jnp.minimum(raw, 0.0) - jnp.log1p(jnp.exp(-jnp.abs(raw)))) * LOG2E
    upto = lax.broadcasted_iota(jnp.int32, (HEAD, HEAD), 0) <= lax.broadcasted_iota(jnp.int32, (HEAD, HEAD), 1)
    sums = jnp.dot(
        logs, upto.astype(jnp.float32), precision=lax.Precision.HIGHEST, preferred_element_type=jnp.float32
    )
    for h in range(heads):
        base = jnp.zeros((1, HEAD), jnp.float32)
        for u in range(chunks):
            line = sums[h * chunks + u : h * chunks + u + 1]
            gate_in[h, u : u + 1] = line + base
            base = base + jnp.broadcast_to(line[:, HEAD - 1 :], (1, HEAD))
        gate_in[h, chunks:] = jnp.broadcast_to(base, (gate_in.shape[1] - chunks, HEAD))

    for copy in loads[1:]:
        copy.wait()
    own = [pltpu.make_async_copy(kv_source(i, z), kv.at[me, i], local_sem.at[i]) for i in range(2)]
    own += [pltpu.make_async_copy(q_source(i, z, x), qg.at[me, i], local_sem.at[2 + i]) for i in range(2)]
    own += [pltpu.make_async_copy(gate_in.at[head], gates.at[me], local_sem.at[4])]
    for copy in own:
        copy.start()
    for copy in own:
        copy.wait()
    pl.semaphore_wait(barrier, blocks + wide - 2)

    for r in range(nz):
        for c in range(nx):
            if (r, c) == (0, 0):
                continue
            zt, xt = near(r, c)
            go(remote(gate_in.at[zt // halves], gates.at[me], gate_send.at[r, c], gate_recv.at[me], at(zt, xt)))

    def kv_arrived(j, i):
        arrived(kv.at[j, i], kv_recv.at[j, i])

    def round_copy(p, c, i):
        j = at(p, x)
        return remote(kv.at[j, i], kv.at[j, i], xs_send.at[p, c // 2, i], kv_recv.at[j, i], at(z, near(0, c)[1]))

    for i in range(2):
        for c in (1, nx - 1):
            round_copy(z, c, i).start()

    for r in (1, nz - 1, 2):
        zt = near(r, 0)[0]
        for i in range(2):
            go(remote(kv_source(i, zt), kv.at[me, i], col_send.at[r, i], kv_recv.at[me, i], at(zt, x)))

    across = nz - 1 - z
    partner = z + 1 - 2 * half

    def q_plane(r):
        return z if r == 0 else across

    for i in range(2):
        go(remote(q_source(i, z, x), qg.at[me, i], qf_send.at[0, 0, i], qg_recv.at[me, i], at(partner, x)))
    for r in range(heads):
        for c in range(nx):
            if (r, c) == (0, 0):
                continue
            zt, xt = q_plane(r), near(0, c)[1]
            for i in range(2):
                go(remote(q_source(i, zt, xt), qg.at[me, i], q_send.at[r, c, i], qg_recv.at[me, i], at(zt, xt)))

    def x_copy(src, source, target, send):
        return pltpu.make_async_remote_copy(
            src_ref=src, dst_ref=x_all.at[source], send_sem=send, recv_sem=x_recv.at[source], device_id={"tp": target}
        )

    core = lax.rem(column, 2)
    twin = column + 1 - 2 * core
    for r in range(1, wide // 2):
        go(x_copy(x_all.at[column], column, lax.rem(column + 2 * r, wide), x_send.at[r]))
    go(x_copy(x_all.at[column], column, twin, x_send.at[0]))

    def onward_copy(p, i):
        c = nx - 1 if i == 0 else 1
        j = at(p, near(0, c)[1])
        return remote(kv.at[j, i], kv.at[j, i], x2_send.at[p, i], kv_recv.at[j, i], at(z, near(0, nx - c)[1]))

    def column_on(r):
        p = near(r, 0)[0]
        for i in range(2):
            kv_arrived(at(p, x), i)
            for c in (1, nx - 1):
                round_copy(p, c, i).start()

    def second_on(p):
        for i, c in ((0, nx - 1), (1, 1)):
            kv_arrived(at(p, near(0, c)[1]), i)
            onward_copy(p, i).start()

    def q_wait(j):
        for i in range(2):
            arrived(qg.at[j, i], qg_recv.at[j, i])

    def q_on(r, c):
        j = at(q_plane(r), near(0, c)[1])
        q_wait(j)
        for i in range(2):
            go(remote(qg.at[j, i], qg.at[j, i], qf_send.at[r, c, i], qg_recv.at[j, i], at(partner, x)))

    column_on(1)
    column_on(nz - 1)
    for c in range(1, nx):
        if c == 2:
            column_on(2)
        q_on(0, c)
    for r in range(nz):
        for c in range(nx):
            if (r, c) != (0, 0):
                j = at(*near(r, c))
                arrived(gates.at[j], gate_recv.at[j])

    def prepare(j, base):
        per = hk // HEAD
        table = gates[j]
        mine = table[0:per]
        for n in range(1, halves):
            mine = jnp.where(half == n, table[n * per : (n + 1) * per], mine)
        for n in range(per):
            row = mine[n : n + 1] + base
            bias[j, n * HEAD : (n + 1) * HEAD] = jnp.broadcast_to(row, (HEAD, HEAD)).T
        return base + table[halves * per : halves * per + 1]

    lax.fori_loop(0, blocks, prepare, jnp.zeros((1, HEAD), jnp.float32))
    second_on(0)
    second_on(1)
    for c in range(nx):
        q_on(1, c)
    rows = halves * hk
    key_row = lax.broadcasted_iota(jnp.int32, (keys_wide, width), 0)
    query_row = lax.broadcasted_iota(jnp.int32, (keys_wide, width), 1)
    key_pos = jnp.where(key_row >= hk, key_row - hk + rows, key_row) + half * hk
    query_pos = jnp.where(query_row >= sub, query_row - sub + rows, query_row) + x * sub

    def pair(i, j):
        return kv[pl.ds(2 * j, 2), i].reshape(keys_wide, HEAD)

    def queries(i, t):
        return qg[pl.ds(2 * t, 2), i].reshape(width, HEAD)

    def place(t, j):
        return t * (t + 1) // 2 + j

    def scores(j, *group):
        k, v = pair(0, j), pair(1, j)
        column_bias = bias[pl.ds(2 * j, 2)].reshape(keys_wide, HEAD)
        column_bias = jnp.concatenate([column_bias] * (width // HEAD), axis=1)
        states = [stat[t] for t, _ in group]
        results = []
        for (t, masked), state in zip(group, states):
            m, total, terms = state[0:1], state[1:2], state[2:3]
            s = nt(k, queries(0, t)) * (SCALE * LOG2E) - column_bias
            if masked:
                s = jnp.where(key_pos <= query_pos, s, -1e30)
            top = jnp.maximum(m, jnp.max(s, axis=0, keepdims=True))
            w = jnp.exp2(s - top)
            old = jnp.exp2(m - top)
            dp = nt(v, queries(1, t))
            total = total * old + jnp.sum(w, axis=0, keepdims=True)
            terms = terms * old + jnp.sum(w * dp, axis=0, keepdims=True)
            wbuf[place(t, j)] = w
            results.append((top, total, terms))
        for (t, _), (top, total, terms) in zip(group, results):
            mrow[place(t, j)] = jnp.broadcast_to(top, (8, width))
            stat[t] = jnp.concatenate([top, total, terms, jnp.zeros((5, width), jnp.float32)], axis=0)

    def pair_wait(j):
        for u in range(2):
            b = 2 * j + u
            d = lax.rem(lax.rem(b, nx) + nx - x, nx)

            @pl.when((d == 1) | (d == 2))
            def _():
                kv_arrived(b, 0)

            @pl.when((d == nx - 1) | (d == 2))
            def _():
                kv_arrived(b, 1)

        for n in range(2):
            kt[j, :, n * hk : (n + 1) * hk] = kv[2 * j + n, 0].T

    outer = (z == 0) | (z == nz - 1)
    quarter = tiles // 4

    def group(direct, j):
        ends = outer if direct else jnp.logical_not(outer)

        @pl.loop(0, quarter)
        def _(m):
            t = jnp.where(ends, m * 3 * quarter, quarter + m * 2)

            @pl.when(t > j)
            def _():
                scores(j, (t, False), (t + 1, False))

            @pl.when(t == j)
            def _():
                scores(j, (t, True), (t + 1, False))

            @pl.when(t + 1 == j)
            def _():
                scores(j, (t + 1, True))

    def stage_parts(t):
        for n, (u, i) in enumerate(((0, 0), (1, 0), (1, 1), (0, 1))):
            value = grads[i, t, u * hk : (u + 1) * hk]
            part_stage[t, n] = (value * SCALE if i == 0 else value).astype(LOW)

    def backward(t):
        q, g = queries(0, t), queries(1, t)
        arrived(stat_got.at[t], stat_recv.at[t])
        mine = stat[t]
        other = stat_got[t]
        top = jnp.maximum(mine[0:1], other[0:1])
        scale_mine = jnp.exp2(mine[0:1] - top)
        scale_other = jnp.exp2(other[0:1] - top)
        inverse = 1.0 / (mine[1:2] * scale_mine + other[1:2] * scale_other)
        terms = (mine[2:3] * scale_mine + other[2:3] * scale_other) * inverse

        def blocks_of(*pairs):
            added = []
            for j in pairs:
                factor = jnp.exp2(mrow[place(t, j)][0:1] - top) * inverse
                prob = wbuf[place(t, j)] * factor
                ds = (prob * (nt(pair(1, j), g) - terms)).astype(LOW)
                added.append((j, nn(prob.astype(LOW), g), nn(ds, q), nn(kt[j], ds)))
            for j, dv, dk, _ in added:
                grads[1, j] += dv
                grads[0, j] += dk
            acc[...] += sum(term for _, _, _, term in added)

        acc[...] = jnp.zeros((HEAD, width), jnp.float32)
        blocks_of(t)

        @pl.when((t >= tiles // 2) | (t < tiles // 4))
        def _():
            stage_parts(t)

        @pl.loop(0, t // 2)
        def _(n):
            blocks_of(2 * n, 2 * n + 1)

        @pl.when(lax.rem(t, 2) == 1)
        def _():
            blocks_of(t - 1)

        dq_t = (acc[...] * SCALE).T.astype(LOW)
        for n in range(2):
            dq_stage[2 * t + n] = dq_t[n * sub : (n + 1) * sub]

    def stat_copy(t):
        return remote(stat.at[t], stat_got.at[t], stat_send.at[t], stat_recv.at[t], at(partner, x))

    def dq_copy(n):
        return remote(dq_stage.at[n], dq_got.at[z, x], dq_send.at[n], dq_recv.at[me], n)

    hr = hk // 2

    def role(tile):
        return lax.rem(x + nx - 2 * lax.rem(tile, nx // 2), nx)

    def array(tile, c):
        return lax.rem(role(tile) + c, nx)

    def share(tile, n, way):
        u = jnp.where((n == 1) | (n == 2), 1, 0)
        i = n // 2
        value = grads[i, tile, pl.ds(pl.multiple_of(u * hk + way * hr, hr), hr)]
        return value * jnp.where(i == 0, SCALE, 1.0)

    def half_of(tile, n, way):
        return part_stage.at[tile, n, pl.ds(way * hr, hr)]

    def opposite_copy(tile, way):
        n = array(tile, 2)
        return remote(
            half_of(tile, n, way), mid.at[tile, way], part_send.at[tile, n, way], mid_recv.at[tile, way],
            at(z, near(0, nx - 1 if way else 1)[1]),
        )

    def near_copy(tile, side, way):
        c = nx - 1 if side else 1
        n = array(tile, c)
        return remote(
            half_of(tile, n, way), red.at[tile, side, way], part_send.at[tile, n, way], red_recv.at[tile, side, way],
            at(z, near(0, c)[1]),
        )

    def first_sends(tile):
        for way in range(2):
            opposite_copy(tile, way).start()
        near_copy(tile, 0, 1).start()
        near_copy(tile, 1, 0).start()

    def add_on_way(tile):
        for way, c in ((0, 1), (1, nx - 1)):
            n = array(tile, c)
            arrived(mid.at[tile, way], mid_recv.at[tile, way])
            part_stage[tile, n, way * hr : (way + 1) * hr] = (
                share(tile, n, way) + mid[tile, way].astype(jnp.float32)
            ).astype(LOW)

    def second_sends(tile):
        near_copy(tile, 0, 0).start()
        near_copy(tile, 1, 1).start()

    def reduce(tile):
        n = array(tile, 0)
        for way in range(2):
            value = share(tile, n, way)
            for side in range(2):
                arrived(red.at[tile, side, way], red_recv.at[tile, side, way])
                value = value + red[tile, side, way].astype(jnp.float32)
            fin[tile, way * hr : (way + 1) * hr] = value.astype(LOW)

    def fin_owner(tile):
        n = array(tile, 0)
        return 2 * tile + jnp.where((n == 1) | (n == 2), 1, 0), n // 2

    def fin_copy(tile):
        owner, i = fin_owner(tile)
        return remote(fin.at[tile], kv_got.at[z, i], fin_send.at[tile], fin_recv.at[z, i], owner)

    def fin_sends(tile):
        owner, i = fin_owner(tile)

        @pl.when(owner == me)
        def _():
            kv_got[z, i] = fin[tile]

        @pl.when(owner != me)
        def _():
            fin_copy(tile).start()

    def dq_sends(tile):
        for u in range(2):
            n = 2 * tile + u

            @pl.when(n == me)
            def _():
                dq_got[z, x] = dq_stage[n]

            @pl.when(n != me)
            def _():
                dq_copy(n).start()

    def x_on(r):
        return x_copy(
            x_all.at[lax.rem(column + 2 * r, wide)], lax.rem(column + 2 * r, wide), twin, xf_send.at[r]
        )

    @pl.loop(0, tiles // 2)
    def _(j):
        pair_wait(j)
        group(True, j)

        @pl.when(lax.rem(j, 2) == 1)
        def _():
            second_on(2 + j // 2)

    for plane in (partner, nz - 1 - partner):
        for c in range(nx):
            q_wait(at(plane, near(0, c)[1]))

    @pl.loop(0, tiles // 2)
    def _(j):
        group(False, j)

    @pl.loop(0, tiles // 2)
    def _(t):
        stat_copy(t).start()

    @pl.loop(tiles // 2, tiles)
    def _(j):
        pair_wait(j)

        odd = lax.rem(tiles - 1 - j, 2)

        @pl.when(odd == 1)
        def _():
            scores(j, (j, True), (j + 1, False))

        @pl.when(odd == 0)
        def _():
            scores(j, (j, True))

        @pl.loop(0, (tiles - 1 - j) // 2)
        def _(n):
            t = j + 1 + odd + 2 * n
            scores(j, (t, False), (t + 1, False))

        @pl.when(j < tiles - 1)
        def _():
            stat_copy(j).start()

    for r in range(1, wide // 2):
        source = lax.rem(column + 2 * r, wide)
        pltpu.make_async_remote_copy(
            src_ref=x_all.at[source], dst_ref=x_all.at[source], send_sem=xf_send.at[r],
            recv_sem=x_recv.at[source], device_id={"tp": twin},
        ).wait_recv()
        x_on(r).start()
    stat_copy(tiles - 1).start()

    middle, low_tiles = tiles // 4, tiles // 4
    upper = tiles // 2

    def step(s, carry):
        last = middle + upper
        t = jnp.where(
            s < middle, upper - 1 - s, jnp.where(s < last, tiles - 1 + middle - s, last + low_tiles - 1 - s)
        )
        sent_tile = tiles - 1 + middle - s

        def stage(lag, work, begin=upper):
            tile = sent_tile + lag
            pl.when((tile >= begin) & (tile < tiles))(lambda: work(tile))

        stage(4, second_sends)
        backward(t)
        dq_sends(t)
        stage(0, first_sends)
        stage(3, add_on_way)
        return carry

    lax.fori_loop(0, tiles, step, 0)
    for tile in range(upper - 1, low_tiles - 1, -1):
        stage_parts(tile)
    second_sends(5)
    for tile in range(upper - 1, -1, -1):
        first_sends(tile)
    add_on_way(4)
    add_on_way(3)
    second_sends(4)
    add_on_way(2)
    second_sends(3)
    add_on_way(1)
    second_sends(2)
    add_on_way(0)
    second_sends(1)
    reduce(7)
    second_sends(0)
    fin_sends(7)

    for r in range(nz):
        for c in range(nx):
            if (r, c) != (0, 0):
                zs, xs = near(r, c)
                arrived(dq_got.at[zs, xs], dq_recv.at[at(zs, xs)])
    for h in range(heads):
        for n in range(nx):
            value = dq_got[h * halves, n].astype(jnp.float32)
            for m in range(1, halves):
                value = value + dq_got[h * halves + m, n].astype(jnp.float32)
            low[n * sub : (n + 1) * sub, h * HEAD : (h + 1) * HEAD] = value.astype(LOW)
    low_copy = pltpu.make_async_copy(low, low_out, out_sem.at[0])
    for r in range(wide // 2):
        source = lax.rem(twin + 2 * r, wide)
        pltpu.make_async_remote_copy(
            src_ref=x_all.at[source], dst_ref=x_all.at[source], send_sem=x_send.at[0],
            recv_sem=x_recv.at[source], device_id={"tp": twin},
        ).wait_recv()

    def term(c):
        begin = c * span
        xs = x_all[begin // x_width, :, pl.ds(pl.multiple_of(lax.rem(begin, x_width), span), span)]
        return lax.dot_general(xs, low[...], (((0,), (0,)), ((), ())), preferred_element_type=jnp.float32)

    waiting = []

    def flush():
        for copy in waiting:
            go(copy)
        waiting.clear()

    between = {
        2: (lambda: reduce(6),),
        5: (lambda: fin_sends(6), lambda: reduce(5)),
        8: (lambda: fin_sends(5), lambda: reduce(4)),
        11: (lambda: fin_sends(4), lambda: reduce(3)),
        14: (lambda: fin_sends(3),),
    }
    order = [(r, c) for r in range(1, nz) for c in range(1, nx)]
    order += [(0, c) for c in range(1, nx)] + [(r, 0) for r in range(1, nz)] + [(0, 0)]
    for count, (r, c) in enumerate(order):
        for work in between.get(count, ()):
            work()
        zt, xt = near(r, c)
        value = term(at(zt, xt))
        fresh = []
        if c:
            wa_stage[r, c] = value[:part_rows].astype(LOW)
            fresh.append(
                remote(wa_stage.at[r, c], wa_red.at[x, zt], wa_send.at[r, c], wa_recv.at[x, zt], at(z, xt))
            )
        else:
            wa_own[r] = value[:part_rows]
        if r:
            wb_stage[r, c] = value[part_rows:].astype(LOW)
            fresh.append(
                remote(wb_stage.at[r, c], wb_red.at[z, xt], wb_send.at[r, c], wb_recv.at[z, xt], at(zt, x))
            )
        else:
            wb_own[c] = value[part_rows:]
        flush()
        waiting.extend(fresh)
    flush()
    low_copy.start()

    @pl.loop(0, 3)
    def _(n):
        reduce(2 - n)

        @pl.when(n > 0)
        def _():
            fin_sends(3 - n)


    for n in list(range(1, nz)) + [0]:
        if n == 2:
            fin_sends(0)
        zt = near(n, 0)[0]
        value = wa_own[n]
        for c in range(1, nx):
            xs = near(0, c)[1]
            arrived(wa_red.at[xs, zt], wa_recv.at[xs, zt])
            value = value + wa_red[xs, zt].astype(jnp.float32)
        fresh = []
        if n:
            wa_fin[n] = value.astype(LOW)
            fresh.append(remote(wa_fin.at[n], wa_got.at[z], wa_fsend.at[n], wa_frecv.at[z], at(zt, x)))
        else:
            w_sum[:part_rows] = value
        xt = near(0, n)[1]
        value = wb_own[n]
        for r in range(1, nz):
            zs = near(r, 0)[0]
            arrived(wb_red.at[zs, xt], wb_recv.at[zs, xt])
            value = value + wb_red[zs, xt].astype(jnp.float32)
        if n:
            wb_fin[n] = value.astype(LOW)
            fresh.append(remote(wb_fin.at[n], wb_got.at[x], wb_fsend.at[n], wb_frecv.at[x], at(z, xt)))
        else:
            w_sum[part_rows:] = value
        flush()
        waiting.extend(fresh)
    flush()

    my_tile = me // 2
    for r in range(nz):
        zs = near(r, 0)[0]
        for i in range(2):
            if r == 0:
                owner, mine = fin_owner(my_tile)

                @pl.when(jnp.logical_not((owner == me) & (mine == i)))
                def _():
                    arrived(kv_got.at[zs, i], fin_recv.at[zs, i])
            else:
                arrived(kv_got.at[zs, i], fin_recv.at[zs, i])
    kv_copy = pltpu.make_async_copy(kv_got, kv_out, out_sem.at[1])
    kv_copy.start()
    for n in range(1, nz):
        zs = near(n, 0)[0]
        arrived(wa_got.at[zs], wa_frecv.at[zs])
        w_sum[:part_rows] += wa_got[zs].astype(jnp.float32)
        xs = near(0, n)[1]
        arrived(wb_got.at[xs], wb_frecv.at[xs])
        w_sum[part_rows:] += wb_got[xs].astype(jnp.float32)

    w_copy = pltpu.make_async_copy(w_sum, w_out, out_sem.at[2])
    w_copy.start()
    low_copy.wait()
    kv_copy.wait()
    for copy in sent:
        copy.wait_send()
    for r in range(1, wide // 2):
        x_on(r).wait_send()

    @pl.loop(0, nz)
    def _(p):
        for i in range(2):
            for c in (1, nx - 1):
                round_copy(p, c, i).wait_send()
            onward_copy(p, i).wait_send()

    @pl.loop(0, tiles)
    def _(t):
        stat_copy(t).wait_send()

    @pl.loop(0, blocks)
    def _(n):
        @pl.when(n != me)
        def _():
            dq_copy(n).wait_send()

    @pl.loop(0, tiles)
    def _(tile):
        for way in range(2):
            opposite_copy(tile, way).wait_send()
            for side in range(2):
                near_copy(tile, side, way).wait_send()

        @pl.when(fin_owner(tile)[0] != me)
        def _():
            fin_copy(tile).wait_send()

    w_copy.wait()


def attention(blocks, wide, q, g, k, v, logits, x):
    rows, cols = k.shape
    heads = cols // HEAD
    nx = NX
    nz = blocks // nx
    halves = nz // heads
    hk = rows // halves
    sub = rows // nx
    tiles = blocks // 2
    anywhere = pl.BlockSpec(memory_space=pl.ANY)
    f32 = jnp.float32
    dma = pltpu.SemaphoreType.DMA
    span = x.shape[1] * wide // blocks
    part = span // 2
    return pl.pallas_call(
        lambda *refs: kernel_body(heads, wide, *refs),
        out_shape=(
            jax.ShapeDtypeStruct((rows, cols), LOW),
            jax.ShapeDtypeStruct((nz, 2, hk, HEAD), LOW),
            jax.ShapeDtypeStruct((span, cols), f32),
        ),
        in_specs=[anywhere] * 6,
        out_specs=(anywhere,) * 3,
        scratch_shapes=[
            pltpu.VMEM((rows, cols), LOW),
            pltpu.VMEM((rows, cols), LOW),
            pltpu.VMEM((rows, cols), LOW),
            pltpu.VMEM((rows, cols), LOW),
            pltpu.VMEM((heads, rows), f32),
            pltpu.VMEM((heads, 8, HEAD), f32),
            pltpu.VMEM((span, cols), f32),
            pltpu.VMEM((blocks, 2, hk, HEAD), LOW),
            pltpu.VMEM((blocks, 2, sub, HEAD), LOW),
            pltpu.VMEM((blocks, 8, HEAD), f32),
            pltpu.VMEM((tiles, HEAD, 2 * hk), LOW),
            pltpu.VMEM((blocks, hk, HEAD), f32),
            pltpu.VMEM((tiles * (tiles + 1) // 2, 2 * hk, 2 * sub), f32),
            pltpu.VMEM((tiles * (tiles + 1) // 2, 8, 2 * sub), f32),
            pltpu.VMEM((2, tiles, 2 * hk, HEAD), f32),
            pltpu.VMEM((HEAD, 2 * sub), f32),
            pltpu.VMEM((tiles, 8, 2 * sub), f32),
            pltpu.VMEM((tiles, 8, 2 * sub), f32),
            pltpu.VMEM((blocks, sub, HEAD), LOW),
            pltpu.VMEM((tiles, nx, hk, HEAD), LOW),
            pltpu.VMEM((tiles, 2, hk // 2, HEAD), LOW),
            pltpu.VMEM((tiles, 2, 2, hk // 2, HEAD), LOW),
            pltpu.VMEM((tiles, hk, HEAD), LOW),
            pltpu.VMEM((nz, nx, sub, HEAD), LOW),
            pltpu.VMEM((nz, 2, hk, HEAD), LOW),
            pltpu.VMEM((wide, rows, x.shape[1]), LOW),
            pltpu.VMEM((rows, cols), LOW),
            pltpu.VMEM((nz, nx, part, cols), LOW),
            pltpu.VMEM((nz, nx, part, cols), LOW),
            pltpu.VMEM((nx, nz, part, cols), LOW),
            pltpu.VMEM((nz, nx, part, cols), LOW),
            pltpu.VMEM((nz, part, cols), f32),
            pltpu.VMEM((nx, part, cols), f32),
            pltpu.VMEM((nz, part, cols), LOW),
            pltpu.VMEM((nx, part, cols), LOW),
            pltpu.VMEM((nz, part, cols), LOW),
            pltpu.VMEM((nx, part, cols), LOW),
            dma((6,)), dma((3,)),
            dma((blocks, 2)), dma((nz, 2, 2)), dma((nz, 2)), dma((nz, 2)), dma((blocks, 2)), dma((heads, nx, 2)),
            dma((heads, nx, 2)), dma((nz, nx)), dma((blocks,)), dma((6,)),
            dma((tiles,)), dma((tiles,)), dma((blocks,)), dma((blocks,)), dma((tiles, nx, 2)), dma((tiles, 2)),
            dma((tiles, 2, 2)), dma((tiles,)), dma((nz, 2)),
            dma((wide // 2,)), dma((wide // 2,)), dma((wide,)),
            dma((nz, nx)), dma((nz, nx)), dma((nx, nz)), dma((nz, nx)),
            dma((nz,)), dma((nx,)), dma((nz,)), dma((nx,)),
        ],
        compiler_params=pltpu.CompilerParams(
            vmem_limit_bytes=62 * 1024 * 1024, collective_id=0, has_side_effects=True
        ),
        cost_estimate=pl.CostEstimate(
            flops=10 * blocks * blocks * rows * sub * HEAD, bytes_accessed=1 << 22, transcendentals=0
        ),
        name="attention",
    )(q, g, k, v, logits, x)


def finish_body(
    heads, low_hbm, kv_hbm, w_hbm, dq_out, dk_out, dv_out, w_out, low, kv, w, dq, dk, dv, in_sem, out_sem
):
    halves = kv.shape[0] // heads
    hk = kv.shape[2]
    loads = [
        pltpu.make_async_copy(src, dst, in_sem.at[n])
        for n, (src, dst) in enumerate(((low_hbm, low), (kv_hbm, kv), (w_hbm, w)))
    ]
    for copy in loads:
        copy.start()
    stores = [
        pltpu.make_async_copy(src, dst, out_sem.at[n])
        for n, (src, dst) in enumerate(((dq, dq_out), (dk, dk_out), (dv, dv_out), (w, w_out)))
    ]
    loads[0].wait()
    dq[...] = low[...].astype(jnp.float32)
    stores[0].start()
    loads[1].wait()
    for i, grad in enumerate((dk, dv)):
        for h in range(heads):
            for m in range(halves):
                grad[m * hk : (m + 1) * hk, h * HEAD : (h + 1) * HEAD] = kv[h * halves + m, i].astype(jnp.float32)
        stores[1 + i].start()
    loads[2].wait()
    stores[3].start()
    for copy in stores:
        copy.wait()


def finish(heads, low, kv, w):
    anywhere = pl.BlockSpec(memory_space=pl.ANY)
    f32 = jnp.float32
    grad = jax.ShapeDtypeStruct(low.shape, f32)
    return pl.pallas_call(
        lambda *refs: finish_body(heads, *refs),
        out_shape=(grad, grad, grad, jax.ShapeDtypeStruct(w.shape, f32)),
        in_specs=[anywhere] * 3,
        out_specs=(anywhere,) * 4,
        scratch_shapes=[
            pltpu.VMEM(low.shape, LOW), pltpu.VMEM(kv.shape, LOW), pltpu.VMEM(w.shape, f32),
            pltpu.VMEM(low.shape, f32), pltpu.VMEM(low.shape, f32), pltpu.VMEM(low.shape, f32),
            pltpu.SemaphoreType.DMA((3,)), pltpu.SemaphoreType.DMA((4,)),
        ],
        compiler_params=pltpu.CompilerParams(vmem_limit_bytes=62 * 1024 * 1024),
        name="finish",
    )(low, kv, w)


def local(queries, keys, values, forget_logits, layer_input, out_grad):
    heads = queries.shape[1] // HEAD
    blocks = lax.axis_size("sp")
    wide = lax.axis_size("tp")
    pieces = attention(blocks, wide, queries, out_grad, keys, values, forget_logits.T, layer_input)
    return finish(heads, *pieces)


def solution(mesh):
    spec = P("sp", "tp")
    return jax.shard_map(
        local, mesh=mesh, in_specs=(spec,) * 6, out_specs=(spec,) * 4, check_vma=False
    )
```

```python
import jax
import jax.numpy as jnp
from jax import lax
from jax.experimental import pallas as pl
from jax.experimental.pallas import tpu as pltpu
from jax.sharding import PartitionSpec as P

HEAD = 128
LOG2E = 1.4426950408889634
SCALE = HEAD ** (-0.5)
LOW = jnp.bfloat16
NX = 4


def nt(a, b):
    return lax.dot_general(a, b, (((1,), (1,)), ((), ())), preferred_element_type=jnp.float32)


def nn(a, b):
    return lax.dot_general(a, b, (((1,), (0,)), ((), ())), preferred_element_type=jnp.float32)


def kernel_body(
    heads, wide,
    q_hbm, g_hbm, k_hbm, v_hbm, logits_hbm, x_hbm,
    low_out, kv_out, w_out,
    q_in, g_in, k_in, v_in, logits, gate_in, w_sum, kv, qg, gates, kt, bias, wbuf, mrow, grads, acc, stat, stat_got,
    dq_stage, part_stage, mid, red, fin, dq_got, kv_got,
    x_all, low, wa_stage, wb_stage, wa_red, wb_red, wa_own, wb_own, wa_fin, wb_fin, wa_got, wb_got,
    in_sem, out_sem, kv_recv, xs_send, col_send, x2_send, qg_recv, q_send, qf_send, gate_send, gate_recv, local_sem,
    stat_send, stat_recv, dq_send, dq_recv, part_send, mid_recv, red_recv, fin_send, fin_recv,
    x_send, xf_send, x_recv, wa_send, wb_send, wa_recv, wb_recv, wa_fsend, wb_fsend, wa_frecv, wb_frecv,
):
    blocks, _, hk, _ = kv.shape
    nx = NX
    nz = blocks // nx
    halves = nz // heads
    sub = qg.shape[2]
    tiles = blocks // 2
    span = w_out.shape[0]
    part_rows = wa_own.shape[1]
    x_width = x_hbm.shape[1]
    column = lax.axis_index("tp")
    me = lax.axis_index("sp")
    z = me // nx
    x = lax.rem(me, nx)
    head = z // halves
    half = lax.rem(z, halves)

    def at(zt, xt):
        return zt * nx + xt

    def near(r, c):
        return lax.rem(z + r, nz), lax.rem(x + c, nx)

    def remote(src, dst, send, recv, target):
        return pltpu.make_async_remote_copy(
            src_ref=src, dst_ref=dst, send_sem=send, recv_sem=recv, device_id={"sp": target}
        )

    def arrived(ref, recv):
        remote(ref, ref, dq_send.at[0], recv, me).wait_recv()

    barrier = pltpu.get_barrier_semaphore()
    for r in range(1, blocks):
        pl.semaphore_signal(barrier, inc=1, device_id={"sp": lax.rem(me + r, blocks)})
    for r in range(1, wide):
        pl.semaphore_signal(barrier, inc=1, device_id={"tp": lax.rem(column + r, wide)})

    def lanes(h):
        return pl.ds(pl.multiple_of(h * HEAD, HEAD), HEAD)

    sent = []

    def go(copy):
        copy.start()
        sent.append(copy)

    kv_in = (k_in, v_in)
    qg_in = (q_in, g_in)

    def kv_source(i, zt):
        begin = pl.multiple_of(lax.rem(zt, halves) * hk, hk)
        return kv_in[i].at[pl.ds(begin, hk), lanes(zt // halves)]

    def q_source(i, zt, xt):
        begin = pl.multiple_of(xt * sub, sub)
        return qg_in[i].at[pl.ds(begin, sub), lanes(zt // halves)]

    loads = [
        pltpu.make_async_copy(src, dst, in_sem.at[n])
        for n, (src, dst) in enumerate(
            ((logits_hbm, logits), (k_hbm, k_in), (v_hbm, v_in), (q_hbm, q_in), (g_hbm, g_in), (x_hbm, x_all.at[column]))
        )
    ]
    for copy in loads:
        copy.start()

    width = 2 * sub
    keys_wide = 2 * hk
    line = lax.broadcasted_iota(jnp.int32, (8, width), 0)

    @pl.loop(0, tiles)
    def _(j):
        grads[0, j] = jnp.zeros((keys_wide, HEAD), jnp.float32)
        grads[1, j] = jnp.zeros((keys_wide, HEAD), jnp.float32)
        stat[j] = jnp.where(line == 0, -1e30, 0.0)

    loads[0].wait()
    chunks = logits.shape[1] // HEAD
    raw = jnp.concatenate(
        [logits[h : h + 1, u * HEAD : (u + 1) * HEAD] for h in range(heads) for u in range(chunks)], axis=0
    )
    logs = (jnp.minimum(raw, 0.0) - jnp.log1p(jnp.exp(-jnp.abs(raw)))) * LOG2E
    upto = lax.broadcasted_iota(jnp.int32, (HEAD, HEAD), 0) <= lax.broadcasted_iota(jnp.int32, (HEAD, HEAD), 1)
    sums = jnp.dot(
        logs, upto.astype(jnp.float32), precision=lax.Precision.HIGHEST, preferred_element_type=jnp.float32
    )
    for h in range(heads):
        base = jnp.zeros((1, HEAD), jnp.float32)
        for u in range(chunks):
            line = sums[h * chunks + u : h * chunks + u + 1]
            gate_in[h, u : u + 1] = line + base
            base = base + jnp.broadcast_to(line[:, HEAD - 1 :], (1, HEAD))
        gate_in[h, chunks:] = jnp.broadcast_to(base, (gate_in.shape[1] - chunks, HEAD))

    for copy in loads[1:]:
        copy.wait()
    own = [pltpu.make_async_copy(kv_source(i, z), kv.at[me, i], local_sem.at[i]) for i in range(2)]
    own += [pltpu.make_async_copy(q_source(i, z, x), qg.at[me, i], local_sem.at[2 + i]) for i in range(2)]
    own += [pltpu.make_async_copy(gate_in.at[head], gates.at[me], local_sem.at[4])]
    for copy in own:
        copy.start()
    for copy in own:
        copy.wait()
    pl.semaphore_wait(barrier, blocks + wide - 2)

    for r in range(nz):
        for c in range(nx):
            if (r, c) == (0, 0):
                continue
            zt, xt = near(r, c)
            go(remote(gate_in.at[zt // halves], gates.at[me], gate_send.at[r, c], gate_recv.at[me], at(zt, xt)))

    def kv_arrived(j, i):
        arrived(kv.at[j, i], kv_recv.at[j, i])

    def round_copy(p, c, i):
        j = at(p, x)
        return remote(kv.at[j, i], kv.at[j, i], xs_send.at[p, c // 2, i], kv_recv.at[j, i], at(z, near(0, c)[1]))

    for i in range(2):
        for c in (1, nx - 1):
            round_copy(z, c, i).start()

    for r in (1, nz - 1, 2):
        zt = near(r, 0)[0]
        for i in range(2):
            go(remote(kv_source(i, zt), kv.at[me, i], col_send.at[r, i], kv_recv.at[me, i], at(zt, x)))

    across = nz - 1 - z
    partner = z + 1 - 2 * half

    def q_plane(r):
        return z if r == 0 else across

    for i in range(2):
        go(remote(q_source(i, z, x), qg.at[me, i], qf_send.at[0, 0, i], qg_recv.at[me, i], at(partner, x)))
    for r in range(heads):
        for c in range(nx):
            if (r, c) == (0, 0):
                continue
            zt, xt = q_plane(r), near(0, c)[1]
            for i in range(2):
                go(remote(q_source(i, zt, xt), qg.at[me, i], q_send.at[r, c, i], qg_recv.at[me, i], at(zt, xt)))

    def x_copy(src, source, target, send):
        return pltpu.make_async_remote_copy(
            src_ref=src, dst_ref=x_all.at[source], send_sem=send, recv_sem=x_recv.at[source], device_id={"tp": target}
        )

    core = lax.rem(column, 2)
    twin = column + 1 - 2 * core
    for r in range(1, wide // 2):
        go(x_copy(x_all.at[column], column, lax.rem(column + 2 * r, wide), x_send.at[r]))
    go(x_copy(x_all.at[column], column, twin, x_send.at[0]))

    def onward_copy(p, i):
        c = nx - 1 if i == 0 else 1
        j = at(p, near(0, c)[1])
        return remote(kv.at[j, i], kv.at[j, i], x2_send.at[p, i], kv_recv.at[j, i], at(z, near(0, nx - c)[1]))

    def column_on(r):
        p = near(r, 0)[0]
        for i in range(2):
            kv_arrived(at(p, x), i)
            for c in (1, nx - 1):
                round_copy(p, c, i).start()

    def second_on(p):
        for i, c in ((0, nx - 1), (1, 1)):
            kv_arrived(at(p, near(0, c)[1]), i)
            onward_copy(p, i).start()

    def q_wait(j):
        for i in range(2):
            arrived(qg.at[j, i], qg_recv.at[j, i])

    def q_on(r, c):
        j = at(q_plane(r), near(0, c)[1])
        q_wait(j)
        for i in range(2):
            go(remote(qg.at[j, i], qg.at[j, i], qf_send.at[r, c, i], qg_recv.at[j, i], at(partner, x)))

    column_on(1)
    column_on(nz - 1)
    for c in range(1, nx):
        if c == 2:
            column_on(2)
        q_on(0, c)
    for r in range(nz):
        for c in range(nx):
            if (r, c) != (0, 0):
                j = at(*near(r, c))
                arrived(gates.at[j], gate_recv.at[j])

    def prepare(j, base):
        per = hk // HEAD
        table = gates[j]
        mine = table[0:per]
        for n in range(1, halves):
            mine = jnp.where(half == n, table[n * per : (n + 1) * per], mine)
        for n in range(per):
            row = mine[n : n + 1] + base
            bias[j, n * HEAD : (n + 1) * HEAD] = jnp.broadcast_to(row, (HEAD, HEAD)).T
        return base + table[halves * per : halves * per + 1]

    lax.fori_loop(0, blocks, prepare, jnp.zeros((1, HEAD), jnp.float32))
    second_on(0)
    second_on(1)
    for c in range(nx):
        q_on(1, c)
    rows = halves * hk
    key_row = lax.broadcasted_iota(jnp.int32, (keys_wide, width), 0)
    query_row = lax.broadcasted_iota(jnp.int32, (keys_wide, width), 1)
    key_pos = jnp.where(key_row >= hk, key_row - hk + rows, key_row) + half * hk
    query_pos = jnp.where(query_row >= sub, query_row - sub + rows, query_row) + x * sub

    def pair(i, j):
        return kv[pl.ds(2 * j, 2), i].reshape(keys_wide, HEAD)

    def queries(i, t):
        return qg[pl.ds(2 * t, 2), i].reshape(width, HEAD)

    def place(t, j):
        return t * (t + 1) // 2 + j

    def scores(j, *group):
        k, v = pair(0, j), pair(1, j)
        column_bias = bias[pl.ds(2 * j, 2)].reshape(keys_wide, HEAD)
        column_bias = jnp.concatenate([column_bias] * (width // HEAD), axis=1)
        states = [stat[t] for t, _ in group]
        results = []
        for (t, masked), state in zip(group, states):
            m, total, terms = state[0:1], state[1:2], state[2:3]
            s = nt(k, queries(0, t)) * (SCALE * LOG2E) - column_bias
            if masked:
                s = jnp.where(key_pos <= query_pos, s, -1e30)
            top = jnp.maximum(m, jnp.max(s, axis=0, keepdims=True))
            w = jnp.exp2(s - top)
            old = jnp.exp2(m - top)
            dp = nt(v, queries(1, t))
            total = total * old + jnp.sum(w, axis=0, keepdims=True)
            terms = terms * old + jnp.sum(w * dp, axis=0, keepdims=True)
            wbuf[place(t, j)] = w
            results.append((top, total, terms))
        for (t, _), (top, total, terms) in zip(group, results):
            mrow[place(t, j)] = jnp.broadcast_to(top, (8, width))
            stat[t] = jnp.concatenate([top, total, terms, jnp.zeros((5, width), jnp.float32)], axis=0)

    def pair_wait(j):
        for u in range(2):
            b = 2 * j + u
            d = lax.rem(lax.rem(b, nx) + nx - x, nx)

            @pl.when((d == 1) | (d == 2))
            def _():
                kv_arrived(b, 0)

            @pl.when((d == nx - 1) | (d == 2))
            def _():
                kv_arrived(b, 1)

        for n in range(2):
            kt[j, :, n * hk : (n + 1) * hk] = kv[2 * j + n, 0].T

    outer = (z == 0) | (z == nz - 1)
    quarter = tiles // 4

    def group(direct, j):
        ends = outer if direct else jnp.logical_not(outer)

        @pl.loop(0, quarter)
        def _(m):
            t = jnp.where(ends, m * 3 * quarter, quarter + m * 2)

            @pl.when(t > j)
            def _():
                scores(j, (t, False), (t + 1, False))

            @pl.when(t == j)
            def _():
                scores(j, (t, True), (t + 1, False))

            @pl.when(t + 1 == j)
            def _():
                scores(j, (t + 1, True))

    def stage_parts(t):
        for n, (u, i) in enumerate(((0, 0), (1, 0), (1, 1), (0, 1))):
            value = grads[i, t, u * hk : (u + 1) * hk]
            part_stage[t, n] = (value * SCALE if i == 0 else value).astype(LOW)

    def backward(t):
        q, g = queries(0, t), queries(1, t)
        arrived(stat_got.at[t], stat_recv.at[t])
        mine = stat[t]
        other = stat_got[t]
        top = jnp.maximum(mine[0:1], other[0:1])
        scale_mine = jnp.exp2(mine[0:1] - top)
        scale_other = jnp.exp2(other[0:1] - top)
        inverse = 1.0 / (mine[1:2] * scale_mine + other[1:2] * scale_other)
        terms = (mine[2:3] * scale_mine + other[2:3] * scale_other) * inverse

        def blocks_of(*pairs):
            added = []
            for j in pairs:
                factor = jnp.exp2(mrow[place(t, j)][0:1] - top) * inverse
                prob = wbuf[place(t, j)] * factor
                ds = (prob * (nt(pair(1, j), g) - terms)).astype(LOW)
                added.append((j, nn(prob.astype(LOW), g), nn(ds, q), nn(kt[j], ds)))
            for j, dv, dk, _ in added:
                grads[1, j] += dv
                grads[0, j] += dk
            acc[...] += sum(term for _, _, _, term in added)

        acc[...] = jnp.zeros((HEAD, width), jnp.float32)
        blocks_of(t)

        @pl.when((t >= tiles // 2) | (t < tiles // 4))
        def _():
            stage_parts(t)

        @pl.loop(0, t // 2)
        def _(n):
            blocks_of(2 * n, 2 * n + 1)

        @pl.when(lax.rem(t, 2) == 1)
        def _():
            blocks_of(t - 1)

        dq_t = (acc[...] * SCALE).T.astype(LOW)
        for n in range(2):
            dq_stage[2 * t + n] = dq_t[n * sub : (n + 1) * sub]

    def stat_copy(t):
        return remote(stat.at[t], stat_got.at[t], stat_send.at[t], stat_recv.at[t], at(partner, x))

    def dq_copy(n):
        return remote(dq_stage.at[n], dq_got.at[z, x], dq_send.at[n], dq_recv.at[me], n)

    hr = hk // 2

    def role(tile):
        return lax.rem(x + nx - 2 * lax.rem(tile, nx // 2), nx)

    def array(tile, c):
        return lax.rem(role(tile) + c, nx)

    def share(tile, n, way):
        u = jnp.where((n == 1) | (n == 2), 1, 0)
        i = n // 2
        value = grads[i, tile, pl.ds(pl.multiple_of(u * hk + way * hr, hr), hr)]
        return value * jnp.where(i == 0, SCALE, 1.0)

    def half_of(tile, n, way):
        return part_stage.at[tile, n, pl.ds(way * hr, hr)]

    def opposite_copy(tile, way):
        n = array(tile, 2)
        return remote(
            half_of(tile, n, way), mid.at[tile, way], part_send.at[tile, n, way], mid_recv.at[tile, way],
            at(z, near(0, nx - 1 if way else 1)[1]),
        )

    def near_copy(tile, side, way):
        c = nx - 1 if side else 1
        n = array(tile, c)
        return remote(
            half_of(tile, n, way), red.at[tile, side, way], part_send.at[tile, n, way], red_recv.at[tile, side, way],
            at(z, near(0, c)[1]),
        )

    def first_sends(tile):
        for way in range(2):
            opposite_copy(tile, way).start()
        near_copy(tile, 0, 1).start()
        near_copy(tile, 1, 0).start()

    def add_on_way(tile):
        for way, c in ((0, 1), (1, nx - 1)):
            n = array(tile, c)
            arrived(mid.at[tile, way], mid_recv.at[tile, way])
            part_stage[tile, n, way * hr : (way + 1) * hr] = (
                share(tile, n, way) + mid[tile, way].astype(jnp.float32)
            ).astype(LOW)

    def second_sends(tile):
        near_copy(tile, 0, 0).start()
        near_copy(tile, 1, 1).start()

    def reduce(tile):
        n = array(tile, 0)
        for way in range(2):
            value = share(tile, n, way)
            for side in range(2):
                arrived(red.at[tile, side, way], red_recv.at[tile, side, way])
                value = value + red[tile, side, way].astype(jnp.float32)
            fin[tile, way * hr : (way + 1) * hr] = value.astype(LOW)

    def fin_owner(tile):
        n = array(tile, 0)
        return 2 * tile + jnp.where((n == 1) | (n == 2), 1, 0), n // 2

    def fin_copy(tile):
        owner, i = fin_owner(tile)
        return remote(fin.at[tile], kv_got.at[z, i], fin_send.at[tile], fin_recv.at[z, i], owner)

    def fin_sends(tile):
        owner, i = fin_owner(tile)

        @pl.when(owner == me)
        def _():
            kv_got[z, i] = fin[tile]

        @pl.when(owner != me)
        def _():
            fin_copy(tile).start()

    def dq_sends(tile):
        for u in range(2):
            n = 2 * tile + u

            @pl.when(n == me)
            def _():
                dq_got[z, x] = dq_stage[n]

            @pl.when(n != me)
            def _():
                dq_copy(n).start()

    def x_on(r):
        return x_copy(
            x_all.at[lax.rem(column + 2 * r, wide)], lax.rem(column + 2 * r, wide), twin, xf_send.at[r]
        )

    @pl.loop(0, tiles // 2)
    def _(j):
        pair_wait(j)
        group(True, j)

        @pl.when(lax.rem(j, 2) == 1)
        def _():
            second_on(2 + j // 2)

    for plane in (partner, nz - 1 - partner):
        for c in range(nx):
            q_wait(at(plane, near(0, c)[1]))

    @pl.loop(0, tiles // 2)
    def _(j):
        group(False, j)

    @pl.loop(0, tiles // 2)
    def _(t):
        stat_copy(t).start()

    @pl.loop(tiles // 2, tiles)
    def _(j):
        pair_wait(j)

        odd = lax.rem(tiles - 1 - j, 2)

        @pl.when(odd == 1)
        def _():
            scores(j, (j, True), (j + 1, False))

        @pl.when(odd == 0)
        def _():
            scores(j, (j, True))

        @pl.loop(0, (tiles - 1 - j) // 2)
        def _(n):
            t = j + 1 + odd + 2 * n
            scores(j, (t, False), (t + 1, False))

        @pl.when(j < tiles - 1)
        def _():
            stat_copy(j).start()

    for r in range(1, wide // 2):
        source = lax.rem(column + 2 * r, wide)
        pltpu.make_async_remote_copy(
            src_ref=x_all.at[source], dst_ref=x_all.at[source], send_sem=xf_send.at[r],
            recv_sem=x_recv.at[source], device_id={"tp": twin},
        ).wait_recv()
        x_on(r).start()
    stat_copy(tiles - 1).start()

    middle, low_tiles = tiles // 4, tiles // 4
    upper = tiles // 2

    def step(s, carry):
        last = middle + upper
        t = jnp.where(
            s < middle, upper - 1 - s, jnp.where(s < last, tiles - 1 + middle - s, last + low_tiles - 1 - s)
        )
        sent_tile = tiles - 1 + middle - s

        def stage(lag, work, begin=upper):
            tile = sent_tile + lag
            pl.when((tile >= begin) & (tile < tiles))(lambda: work(tile))

        stage(4, second_sends)
        backward(t)
        dq_sends(t)
        stage(0, first_sends)
        stage(3, add_on_way)
        return carry

    lax.fori_loop(0, tiles, step, 0)
    for tile in range(upper - 1, low_tiles - 1, -1):
        stage_parts(tile)
    second_sends(5)
    for tile in range(upper - 1, -1, -1):
        first_sends(tile)
    add_on_way(4)
    add_on_way(3)
    second_sends(4)
    add_on_way(2)
    second_sends(3)
    add_on_way(1)
    second_sends(2)
    add_on_way(0)
    second_sends(1)
    reduce(7)
    second_sends(0)
    fin_sends(7)

    for r in range(nz):
        for c in range(nx):
            if (r, c) != (0, 0):
                zs, xs = near(r, c)
                arrived(dq_got.at[zs, xs], dq_recv.at[at(zs, xs)])
    for h in range(heads):
        for n in range(nx):
            value = dq_got[h * halves, n].astype(jnp.float32)
            for m in range(1, halves):
                value = value + dq_got[h * halves + m, n].astype(jnp.float32)
            low[n * sub : (n + 1) * sub, h * HEAD : (h + 1) * HEAD] = value.astype(LOW)
    low_copy = pltpu.make_async_copy(low, low_out, out_sem.at[0])
    for r in range(wide // 2):
        source = lax.rem(twin + 2 * r, wide)
        pltpu.make_async_remote_copy(
            src_ref=x_all.at[source], dst_ref=x_all.at[source], send_sem=x_send.at[0],
            recv_sem=x_recv.at[source], device_id={"tp": twin},
        ).wait_recv()

    def term(c):
        begin = c * span
        xs = x_all[begin // x_width, :, pl.ds(pl.multiple_of(lax.rem(begin, x_width), span), span)]
        return lax.dot_general(xs, low[...], (((0,), (0,)), ((), ())), preferred_element_type=jnp.float32)

    waiting = []

    def flush():
        for copy in waiting:
            go(copy)
        waiting.clear()

    between = {
        2: (lambda: reduce(6),),
        5: (lambda: fin_sends(6), lambda: reduce(5)),
        8: (lambda: fin_sends(5), lambda: reduce(4)),
        11: (lambda: fin_sends(4), lambda: reduce(3)),
        14: (lambda: fin_sends(3),),
    }
    order = [(r, c) for r in range(1, nz) for c in range(1, nx)]
    order += [(0, c) for c in range(1, nx)] + [(r, 0) for r in range(1, nz)] + [(0, 0)]
    for count, (r, c) in enumerate(order):
        for work in between.get(count, ()):
            work()
        zt, xt = near(r, c)
        value = term(at(zt, xt))
        fresh = []
        if c:
            wa_stage[r, c] = value[:part_rows].astype(LOW)
            fresh.append(
                remote(wa_stage.at[r, c], wa_red.at[x, zt], wa_send.at[r, c], wa_recv.at[x, zt], at(z, xt))
            )
        else:
            wa_own[r] = value[:part_rows]
        if r:
            wb_stage[r, c] = value[part_rows:].astype(LOW)
            fresh.append(
                remote(wb_stage.at[r, c], wb_red.at[z, xt], wb_send.at[r, c], wb_recv.at[z, xt], at(zt, x))
            )
        else:
            wb_own[c] = value[part_rows:]
        flush()
        waiting.extend(fresh)
    flush()
    low_copy.start()

    @pl.loop(0, 3)
    def _(n):
        reduce(2 - n)

        @pl.when(n > 0)
        def _():
            fin_sends(3 - n)


    for n in list(range(1, nz)) + [0]:
        if n == 2:
            fin_sends(0)
        zt = near(n, 0)[0]
        value = wa_own[n]
        for c in range(1, nx):
            xs = near(0, c)[1]
            arrived(wa_red.at[xs, zt], wa_recv.at[xs, zt])
            value = value + wa_red[xs, zt].astype(jnp.float32)
        fresh = []
        if n:
            wa_fin[n] = value.astype(LOW)
            fresh.append(remote(wa_fin.at[n], wa_got.at[z], wa_fsend.at[n], wa_frecv.at[z], at(zt, x)))
        else:
            w_sum[:part_rows] = value
        xt = near(0, n)[1]
        value = wb_own[n]
        for r in range(1, nz):
            zs = near(r, 0)[0]
            arrived(wb_red.at[zs, xt], wb_recv.at[zs, xt])
            value = value + wb_red[zs, xt].astype(jnp.float32)
        if n:
            wb_fin[n] = value.astype(LOW)
            fresh.append(remote(wb_fin.at[n], wb_got.at[x], wb_fsend.at[n], wb_frecv.at[x], at(z, xt)))
        else:
            w_sum[part_rows:] = value
        flush()
        waiting.extend(fresh)
    flush()

    my_tile = me // 2
    for r in range(nz):
        zs = near(r, 0)[0]
        for i in range(2):
            if r == 0:
                owner, mine = fin_owner(my_tile)

                @pl.when(jnp.logical_not((owner == me) & (mine == i)))
                def _():
                    arrived(kv_got.at[zs, i], fin_recv.at[zs, i])
            else:
                arrived(kv_got.at[zs, i], fin_recv.at[zs, i])
    kv_copy = pltpu.make_async_copy(kv_got, kv_out, out_sem.at[1])
    kv_copy.start()
    for n in range(1, nz):
        zs = near(n, 0)[0]
        arrived(wa_got.at[zs], wa_frecv.at[zs])
        w_sum[:part_rows] += wa_got[zs].astype(jnp.float32)
        xs = near(0, n)[1]
        arrived(wb_got.at[xs], wb_frecv.at[xs])
        w_sum[part_rows:] += wb_got[xs].astype(jnp.float32)

    w_copy = pltpu.make_async_copy(w_sum, w_out, out_sem.at[2])
    w_copy.start()
    low_copy.wait()
    kv_copy.wait()
    for copy in sent:
        copy.wait_send()
    for r in range(1, wide // 2):
        x_on(r).wait_send()

    @pl.loop(0, nz)
    def _(p):
        for i in range(2):
            for c in (1, nx - 1):
                round_copy(p, c, i).wait_send()
            onward_copy(p, i).wait_send()

    @pl.loop(0, tiles)
    def _(t):
        stat_copy(t).wait_send()

    @pl.loop(0, blocks)
    def _(n):
        @pl.when(n != me)
        def _():
            dq_copy(n).wait_send()

    @pl.loop(0, tiles)
    def _(tile):
        for way in range(2):
            opposite_copy(tile, way).wait_send()
            for side in range(2):
                near_copy(tile, side, way).wait_send()

        @pl.when(fin_owner(tile)[0] != me)
        def _():
            fin_copy(tile).wait_send()

    w_copy.wait()


def attention(blocks, wide, q, g, k, v, logits, x):
    rows, cols = k.shape
    heads = cols // HEAD
    nx = NX
    nz = blocks // nx
    halves = nz // heads
    hk = rows // halves
    sub = rows // nx
    tiles = blocks // 2
    anywhere = pl.BlockSpec(memory_space=pl.ANY)
    f32 = jnp.float32
    dma = pltpu.SemaphoreType.DMA
    span = x.shape[1] * wide // blocks
    part = span * 3 // 8
    rest = span - part
    return pl.pallas_call(
        lambda *refs: kernel_body(heads, wide, *refs),
        out_shape=(
            jax.ShapeDtypeStruct((rows, cols), LOW),
            jax.ShapeDtypeStruct((nz, 2, hk, HEAD), LOW),
            jax.ShapeDtypeStruct((span, cols), f32),
        ),
        in_specs=[anywhere] * 6,
        out_specs=(anywhere,) * 3,
        scratch_shapes=[
            pltpu.VMEM((rows, cols), LOW),
            pltpu.VMEM((rows, cols), LOW),
            pltpu.VMEM((rows, cols), LOW),
            pltpu.VMEM((rows, cols), LOW),
            pltpu.VMEM((heads, rows), f32),
            pltpu.VMEM((heads, 8, HEAD), f32),
            pltpu.VMEM((span, cols), f32),
            pltpu.VMEM((blocks, 2, hk, HEAD), LOW),
            pltpu.VMEM((blocks, 2, sub, HEAD), LOW),
            pltpu.VMEM((blocks, 8, HEAD), f32),
            pltpu.VMEM((tiles, HEAD, 2 * hk), LOW),
            pltpu.VMEM((blocks, hk, HEAD), f32),
            pltpu.VMEM((tiles * (tiles + 1) // 2, 2 * hk, 2 * sub), f32),
            pltpu.VMEM((tiles * (tiles + 1) // 2, 8, 2 * sub), f32),
            pltpu.VMEM((2, tiles, 2 * hk, HEAD), f32),
            pltpu.VMEM((HEAD, 2 * sub), f32),
            pltpu.VMEM((tiles, 8, 2 * sub), f32),
            pltpu.VMEM((tiles, 8, 2 * sub), f32),
            pltpu.VMEM((blocks, sub, HEAD), LOW),
            pltpu.VMEM((tiles, nx, hk, HEAD), LOW),
            pltpu.VMEM((tiles, 2, hk // 2, HEAD), LOW),
            pltpu.VMEM((tiles, 2, 2, hk // 2, HEAD), LOW),
            pltpu.VMEM((tiles, hk, HEAD), LOW),
            pltpu.VMEM((nz, nx, sub, HEAD), LOW),
            pltpu.VMEM((nz, 2, hk, HEAD), LOW),
            pltpu.VMEM((wide, rows, x.shape[1]), LOW),
            pltpu.VMEM((rows, cols), LOW),
            pltpu.VMEM((nz, nx, part, cols), LOW),
            pltpu.VMEM((nz, nx, rest, cols), LOW),
            pltpu.VMEM((nx, nz, part, cols), LOW),
            pltpu.VMEM((nz, nx, rest, cols), LOW),
            pltpu.VMEM((nz, part, cols), f32),
            pltpu.VMEM((nx, rest, cols), f32),
            pltpu.VMEM((nz, part, cols), LOW),
            pltpu.VMEM((nx, rest, cols), LOW),
            pltpu.VMEM((nz, part, cols), LOW),
            pltpu.VMEM((nx, rest, cols), LOW),
            dma((6,)), dma((3,)),
            dma((blocks, 2)), dma((nz, 2, 2)), dma((nz, 2)), dma((nz, 2)), dma((blocks, 2)), dma((heads, nx, 2)),
            dma((heads, nx, 2)), dma((nz, nx)), dma((blocks,)), dma((6,)),
            dma((tiles,)), dma((tiles,)), dma((blocks,)), dma((blocks,)), dma((tiles, nx, 2)), dma((tiles, 2)),
            dma((tiles, 2, 2)), dma((tiles,)), dma((nz, 2)),
            dma((wide // 2,)), dma((wide // 2,)), dma((wide,)),
            dma((nz, nx)), dma((nz, nx)), dma((nx, nz)), dma((nz, nx)),
            dma((nz,)), dma((nx,)), dma((nz,)), dma((nx,)),
        ],
        compiler_params=pltpu.CompilerParams(
            vmem_limit_bytes=62 * 1024 * 1024, collective_id=0, has_side_effects=True
        ),
        cost_estimate=pl.CostEstimate(
            flops=10 * blocks * blocks * rows * sub * HEAD, bytes_accessed=1 << 22, transcendentals=0
        ),
        name="attention",
    )(q, g, k, v, logits, x)


def finish_body(
    heads, low_hbm, kv_hbm, w_hbm, dq_out, dk_out, dv_out, w_out, low, kv, w, dq, dk, dv, in_sem, out_sem
):
    halves = kv.shape[0] // heads
    hk = kv.shape[2]
    loads = [
        pltpu.make_async_copy(src, dst, in_sem.at[n])
        for n, (src, dst) in enumerate(((low_hbm, low), (kv_hbm, kv), (w_hbm, w)))
    ]
    for copy in loads:
        copy.start()
    stores = [
        pltpu.make_async_copy(src, dst, out_sem.at[n])
        for n, (src, dst) in enumerate(((dq, dq_out), (dk, dk_out), (dv, dv_out), (w, w_out)))
    ]
    loads[0].wait()
    dq[...] = low[...].astype(jnp.float32)
    stores[0].start()
    loads[1].wait()
    for i, grad in enumerate((dk, dv)):
        for h in range(heads):
            for m in range(halves):
                grad[m * hk : (m + 1) * hk, h * HEAD : (h + 1) * HEAD] = kv[h * halves + m, i].astype(jnp.float32)
        stores[1 + i].start()
    loads[2].wait()
    stores[3].start()
    for copy in stores:
        copy.wait()


def finish(heads, low, kv, w):
    anywhere = pl.BlockSpec(memory_space=pl.ANY)
    f32 = jnp.float32
    grad = jax.ShapeDtypeStruct(low.shape, f32)
    return pl.pallas_call(
        lambda *refs: finish_body(heads, *refs),
        out_shape=(grad, grad, grad, jax.ShapeDtypeStruct(w.shape, f32)),
        in_specs=[anywhere] * 3,
        out_specs=(anywhere,) * 4,
        scratch_shapes=[
            pltpu.VMEM(low.shape, LOW), pltpu.VMEM(kv.shape, LOW), pltpu.VMEM(w.shape, f32),
            pltpu.VMEM(low.shape, f32), pltpu.VMEM(low.shape, f32), pltpu.VMEM(low.shape, f32),
            pltpu.SemaphoreType.DMA((3,)), pltpu.SemaphoreType.DMA((4,)),
        ],
        compiler_params=pltpu.CompilerParams(vmem_limit_bytes=62 * 1024 * 1024),
        name="finish",
    )(low, kv, w)


def local(queries, keys, values, forget_logits, layer_input, out_grad):
    heads = queries.shape[1] // HEAD
    blocks = lax.axis_size("sp")
    wide = lax.axis_size("tp")
    pieces = attention(blocks, wide, queries, out_grad, keys, values, forget_logits.T, layer_input)
    return finish(heads, *pieces)


def solution(mesh):
    spec = P("sp", "tp")
    return jax.shard_map(
        local, mesh=mesh, in_specs=(spec,) * 6, out_specs=(spec,) * 4, check_vma=False
    )
```

```python
import jax
import jax.numpy as jnp
from jax import lax
from jax.experimental import pallas as pl
from jax.experimental.pallas import tpu as pltpu
from jax.sharding import PartitionSpec as P

HEAD = 128
LOG2E = 1.4426950408889634
SCALE = HEAD ** (-0.5)
LOW = jnp.bfloat16
NX = 4


def nt(a, b):
    return lax.dot_general(a, b, (((1,), (1,)), ((), ())), preferred_element_type=jnp.float32)


def nn(a, b):
    return lax.dot_general(a, b, (((1,), (0,)), ((), ())), preferred_element_type=jnp.float32)


def kernel_body(
    heads, wide,
    q_hbm, g_hbm, k_hbm, v_hbm, logits_hbm, x_hbm,
    low_out, kv_out, w_out,
    q_in, g_in, k_in, v_in, logits, gate_in, w_sum, kv, qg, gates, kt, bias, wbuf, mrow, grads, acc, stat, stat_got,
    dq_stage, part_stage, mid, red, fin, dq_got, kv_got,
    x_all, low, wa_stage, wb_stage, wa_red, wb_red, wa_own, wb_own, wa_fin, wb_fin, wa_got, wb_got,
    in_sem, out_sem, kv_recv, xs_send, col_send, x2_send, qg_recv, q_send, qf_send, gate_send, gate_recv, local_sem,
    stat_send, stat_recv, dq_send, dq_recv, part_send, mid_recv, red_recv, fin_send, fin_recv,
    x_send, xf_send, x_recv, wa_send, wb_send, wa_recv, wb_recv, wa_fsend, wb_fsend, wa_frecv, wb_frecv,
):
    blocks, _, hk, _ = kv.shape
    nx = NX
    nz = blocks // nx
    halves = nz // heads
    sub = qg.shape[2]
    tiles = blocks // 2
    span = w_out.shape[0]
    part_rows = wa_own.shape[1]
    x_width = x_hbm.shape[1]
    column = lax.axis_index("tp")
    me = lax.axis_index("sp")
    z = me // nx
    x = lax.rem(me, nx)
    head = z // halves
    half = lax.rem(z, halves)

    def at(zt, xt):
        return zt * nx + xt

    def near(r, c):
        return lax.rem(z + r, nz), lax.rem(x + c, nx)

    def remote(src, dst, send, recv, target):
        return pltpu.make_async_remote_copy(
            src_ref=src, dst_ref=dst, send_sem=send, recv_sem=recv, device_id={"sp": target}
        )

    def arrived(ref, recv):
        remote(ref, ref, dq_send.at[0], recv, me).wait_recv()

    barrier = pltpu.get_barrier_semaphore()
    for r in range(1, blocks):
        pl.semaphore_signal(barrier, inc=1, device_id={"sp": lax.rem(me + r, blocks)})
    for r in range(1, wide):
        pl.semaphore_signal(barrier, inc=1, device_id={"tp": lax.rem(column + r, wide)})

    def lanes(h):
        return pl.ds(pl.multiple_of(h * HEAD, HEAD), HEAD)

    sent = []

    def go(copy):
        copy.start()
        sent.append(copy)

    kv_in = (k_in, v_in)
    qg_in = (q_in, g_in)

    def kv_source(i, zt):
        begin = pl.multiple_of(lax.rem(zt, halves) * hk, hk)
        return kv_in[i].at[pl.ds(begin, hk), lanes(zt // halves)]

    def q_source(i, zt, xt):
        begin = pl.multiple_of(xt * sub, sub)
        return qg_in[i].at[pl.ds(begin, sub), lanes(zt // halves)]

    loads = [
        pltpu.make_async_copy(src, dst, in_sem.at[n])
        for n, (src, dst) in enumerate(
            ((logits_hbm, logits), (k_hbm, k_in), (v_hbm, v_in), (q_hbm, q_in), (g_hbm, g_in), (x_hbm, x_all.at[column]))
        )
    ]
    for copy in loads:
        copy.start()

    width = 2 * sub
    keys_wide = 2 * hk
    line = lax.broadcasted_iota(jnp.int32, (8, width), 0)

    @pl.loop(0, tiles)
    def _(j):
        grads[0, j] = jnp.zeros((keys_wide, HEAD), jnp.float32)
        grads[1, j] = jnp.zeros((keys_wide, HEAD), jnp.float32)
        stat[j] = jnp.where(line == 0, -1e30, 0.0)

    loads[0].wait()
    chunks = logits.shape[1] // HEAD
    raw = jnp.concatenate(
        [logits[h : h + 1, u * HEAD : (u + 1) * HEAD] for h in range(heads) for u in range(chunks)], axis=0
    )
    logs = (jnp.minimum(raw, 0.0) - jnp.log1p(jnp.exp(-jnp.abs(raw)))) * LOG2E
    upto = lax.broadcasted_iota(jnp.int32, (HEAD, HEAD), 0) <= lax.broadcasted_iota(jnp.int32, (HEAD, HEAD), 1)
    sums = jnp.dot(
        logs, upto.astype(jnp.float32), precision=lax.Precision.HIGHEST, preferred_element_type=jnp.float32
    )
    for h in range(heads):
        base = jnp.zeros((1, HEAD), jnp.float32)
        for u in range(chunks):
            line = sums[h * chunks + u : h * chunks + u + 1]
            gate_in[h, u : u + 1] = line + base
            base = base + jnp.broadcast_to(line[:, HEAD - 1 :], (1, HEAD))
        gate_in[h, chunks:] = jnp.broadcast_to(base, (gate_in.shape[1] - chunks, HEAD))

    for copy in loads[1:]:
        copy.wait()
    own = [pltpu.make_async_copy(kv_source(i, z), kv.at[me, i], local_sem.at[i]) for i in range(2)]
    own += [pltpu.make_async_copy(q_source(i, z, x), qg.at[me, i], local_sem.at[2 + i]) for i in range(2)]
    own += [pltpu.make_async_copy(gate_in.at[head], gates.at[me], local_sem.at[4])]
    for copy in own:
        copy.start()
    for copy in own:
        copy.wait()
    pl.semaphore_wait(barrier, blocks + wide - 2)

    for r in range(nz):
        for c in range(nx):
            if (r, c) == (0, 0):
                continue
            zt, xt = near(r, c)
            go(remote(gate_in.at[zt // halves], gates.at[me], gate_send.at[r, c], gate_recv.at[me], at(zt, xt)))

    def kv_arrived(j, i):
        arrived(kv.at[j, i], kv_recv.at[j, i])

    def round_copy(p, c, i):
        j = at(p, x)
        return remote(kv.at[j, i], kv.at[j, i], xs_send.at[p, c // 2, i], kv_recv.at[j, i], at(z, near(0, c)[1]))

    for i in range(2):
        for c in (1, nx - 1):
            round_copy(z, c, i).start()

    for r in (1, nz - 1, 2):
        zt = near(r, 0)[0]
        for i in range(2):
            go(remote(kv_source(i, zt), kv.at[me, i], col_send.at[r, i], kv_recv.at[me, i], at(zt, x)))

    across = nz - 1 - z
    partner = z + 1 - 2 * half

    def q_plane(r):
        return z if r == 0 else across

    for i in range(2):
        go(remote(q_source(i, z, x), qg.at[me, i], qf_send.at[0, 0, i], qg_recv.at[me, i], at(partner, x)))
    for r in range(heads):
        for c in range(nx):
            if (r, c) == (0, 0):
                continue
            zt, xt = q_plane(r), near(0, c)[1]
            for i in range(2):
                go(remote(q_source(i, zt, xt), qg.at[me, i], q_send.at[r, c, i], qg_recv.at[me, i], at(zt, xt)))

    def x_copy(src, source, target, send):
        return pltpu.make_async_remote_copy(
            src_ref=src, dst_ref=x_all.at[source], send_sem=send, recv_sem=x_recv.at[source], device_id={"tp": target}
        )

    core = lax.rem(column, 2)
    twin = column + 1 - 2 * core
    for r in range(1, wide // 2):
        go(x_copy(x_all.at[column], column, lax.rem(column + 2 * r, wide), x_send.at[r]))
    go(x_copy(x_all.at[column], column, twin, x_send.at[0]))

    def onward_copy(p, i):
        c = nx - 1 if i == 0 else 1
        j = at(p, near(0, c)[1])
        return remote(kv.at[j, i], kv.at[j, i], x2_send.at[p, i], kv_recv.at[j, i], at(z, near(0, nx - c)[1]))

    def column_on(r):
        p = near(r, 0)[0]
        for i in range(2):
            kv_arrived(at(p, x), i)
            for c in (1, nx - 1):
                round_copy(p, c, i).start()

    def second_on(p):
        for i, c in ((0, nx - 1), (1, 1)):
            kv_arrived(at(p, near(0, c)[1]), i)
            onward_copy(p, i).start()

    def q_wait(j):
        for i in range(2):
            arrived(qg.at[j, i], qg_recv.at[j, i])

    def q_on(r, c):
        j = at(q_plane(r), near(0, c)[1])
        q_wait(j)
        for i in range(2):
            go(remote(qg.at[j, i], qg.at[j, i], qf_send.at[r, c, i], qg_recv.at[j, i], at(partner, x)))

    column_on(1)
    column_on(nz - 1)
    for c in range(1, nx):
        if c == 2:
            column_on(2)
        q_on(0, c)
    for r in range(nz):
        for c in range(nx):
            if (r, c) != (0, 0):
                j = at(*near(r, c))
                arrived(gates.at[j], gate_recv.at[j])

    def prepare(j, base):
        per = hk // HEAD
        table = gates[j]
        mine = table[0:per]
        for n in range(1, halves):
            mine = jnp.where(half == n, table[n * per : (n + 1) * per], mine)
        for n in range(per):
            row = mine[n : n + 1] + base
            bias[j, n * HEAD : (n + 1) * HEAD] = jnp.broadcast_to(row, (HEAD, HEAD)).T
        return base + table[halves * per : halves * per + 1]

    lax.fori_loop(0, blocks, prepare, jnp.zeros((1, HEAD), jnp.float32))
    second_on(0)
    second_on(1)
    for c in range(nx):
        q_on(1, c)
    rows = halves * hk
    key_row = lax.broadcasted_iota(jnp.int32, (keys_wide, width), 0)
    query_row = lax.broadcasted_iota(jnp.int32, (keys_wide, width), 1)
    key_pos = jnp.where(key_row >= hk, key_row - hk + rows, key_row) + half * hk
    query_pos = jnp.where(query_row >= sub, query_row - sub + rows, query_row) + x * sub

    def pair(i, j):
        return kv[pl.ds(2 * j, 2), i].reshape(keys_wide, HEAD)

    def queries(i, t):
        return qg[pl.ds(2 * t, 2), i].reshape(width, HEAD)

    def place(t, j):
        return t * (t + 1) // 2 + j

    def scores(j, *group):
        k, v = pair(0, j), pair(1, j)
        column_bias = bias[pl.ds(2 * j, 2)].reshape(keys_wide, HEAD)
        column_bias = jnp.concatenate([column_bias] * (width // HEAD), axis=1)
        states = [stat[t] for t, _ in group]
        results = []
        for (t, masked), state in zip(group, states):
            m, total, terms = state[0:1], state[1:2], state[2:3]
            s = nt(k, queries(0, t)) * (SCALE * LOG2E) - column_bias
            if masked:
                s = jnp.where(key_pos <= query_pos, s, -1e30)
            top = jnp.maximum(m, jnp.max(s, axis=0, keepdims=True))
            w = jnp.exp2(s - top)
            old = jnp.exp2(m - top)
            dp = nt(v, queries(1, t))
            total = total * old + jnp.sum(w, axis=0, keepdims=True)
            terms = terms * old + jnp.sum(w * dp, axis=0, keepdims=True)
            wbuf[place(t, j)] = w
            results.append((top, total, terms))
        for (t, _), (top, total, terms) in zip(group, results):
            mrow[place(t, j)] = jnp.broadcast_to(top, (8, width))
            stat[t] = jnp.concatenate([top, total, terms, jnp.zeros((5, width), jnp.float32)], axis=0)

    def pair_wait(j):
        for u in range(2):
            b = 2 * j + u
            d = lax.rem(lax.rem(b, nx) + nx - x, nx)

            @pl.when((d == 1) | (d == 2))
            def _():
                kv_arrived(b, 0)

            @pl.when((d == nx - 1) | (d == 2))
            def _():
                kv_arrived(b, 1)

        for n in range(2):
            kt[j, :, n * hk : (n + 1) * hk] = kv[2 * j + n, 0].T

    outer = (z == 0) | (z == nz - 1)
    quarter = tiles // 4

    def group(direct, j):
        ends = outer if direct else jnp.logical_not(outer)

        @pl.loop(0, quarter)
        def _(m):
            t = jnp.where(ends, m * 3 * quarter, quarter + m * 2)

            @pl.when(t > j)
            def _():
                scores(j, (t, False), (t + 1, False))

            @pl.when(t == j)
            def _():
                scores(j, (t, True), (t + 1, False))

            @pl.when(t + 1 == j)
            def _():
                scores(j, (t + 1, True))

    def stage_parts(t):
        for n, (u, i) in enumerate(((0, 0), (1, 0), (1, 1), (0, 1))):
            value = grads[i, t, u * hk : (u + 1) * hk]
            part_stage[t, n] = (value * SCALE if i == 0 else value).astype(LOW)

    def backward(t):
        q, g = queries(0, t), queries(1, t)
        arrived(stat_got.at[t], stat_recv.at[t])
        mine = stat[t]
        other = stat_got[t]
        top = jnp.maximum(mine[0:1], other[0:1])
        scale_mine = jnp.exp2(mine[0:1] - top)
        scale_other = jnp.exp2(other[0:1] - top)
        inverse = 1.0 / (mine[1:2] * scale_mine + other[1:2] * scale_other)
        terms = (mine[2:3] * scale_mine + other[2:3] * scale_other) * inverse

        def blocks_of(*pairs):
            added = []
            for j in pairs:
                factor = jnp.exp2(mrow[place(t, j)][0:1] - top) * inverse
                prob = wbuf[place(t, j)] * factor
                ds = (prob * (nt(pair(1, j), g) - terms)).astype(LOW)
                added.append((j, nn(prob.astype(LOW), g), nn(ds, q), nn(kt[j], ds)))
            for j, dv, dk, _ in added:
                grads[1, j] += dv
                grads[0, j] += dk
            acc[...] += sum(term for _, _, _, term in added)

        acc[...] = jnp.zeros((HEAD, width), jnp.float32)
        blocks_of(t)

        @pl.when((t >= tiles // 2) | (t < tiles // 4))
        def _():
            stage_parts(t)

        @pl.loop(0, t // 2)
        def _(n):
            blocks_of(2 * n, 2 * n + 1)

        @pl.when(lax.rem(t, 2) == 1)
        def _():
            blocks_of(t - 1)

        dq_t = (acc[...] * SCALE).T.astype(LOW)
        for n in range(2):
            dq_stage[2 * t + n] = dq_t[n * sub : (n + 1) * sub]

    def stat_copy(t):
        return remote(stat.at[t], stat_got.at[t], stat_send.at[t], stat_recv.at[t], at(partner, x))

    def dq_copy(n):
        return remote(dq_stage.at[n], dq_got.at[z, x], dq_send.at[n], dq_recv.at[me], n)

    hr = hk // 2

    def role(tile):
        return lax.rem(x + nx - 2 * lax.rem(tile, nx // 2), nx)

    def array(tile, c):
        return lax.rem(role(tile) + c, nx)

    def share(tile, n, way):
        u = jnp.where((n == 1) | (n == 2), 1, 0)
        i = n // 2
        value = grads[i, tile, pl.ds(pl.multiple_of(u * hk + way * hr, hr), hr)]
        return value * jnp.where(i == 0, SCALE, 1.0)

    def half_of(tile, n, way):
        return part_stage.at[tile, n, pl.ds(way * hr, hr)]

    def opposite_copy(tile, way):
        n = array(tile, 2)
        return remote(
            half_of(tile, n, way), mid.at[tile, way], part_send.at[tile, n, way], mid_recv.at[tile, way],
            at(z, near(0, nx - 1 if way else 1)[1]),
        )

    def near_copy(tile, side, way):
        c = nx - 1 if side else 1
        n = array(tile, c)
        return remote(
            half_of(tile, n, way), red.at[tile, side, way], part_send.at[tile, n, way], red_recv.at[tile, side, way],
            at(z, near(0, c)[1]),
        )

    def first_sends(tile):
        for way in range(2):
            opposite_copy(tile, way).start()
        near_copy(tile, 0, 1).start()
        near_copy(tile, 1, 0).start()

    def add_on_way(tile):
        for way, c in ((0, 1), (1, nx - 1)):
            n = array(tile, c)
            arrived(mid.at[tile, way], mid_recv.at[tile, way])
            part_stage[tile, n, way * hr : (way + 1) * hr] = (
                share(tile, n, way) + mid[tile, way].astype(jnp.float32)
            ).astype(LOW)

    def second_sends(tile):
        near_copy(tile, 0, 0).start()
        near_copy(tile, 1, 1).start()

    def reduce(tile):
        n = array(tile, 0)
        for way in range(2):
            value = share(tile, n, way)
            for side in range(2):
                arrived(red.at[tile, side, way], red_recv.at[tile, side, way])
                value = value + red[tile, side, way].astype(jnp.float32)
            fin[tile, way * hr : (way + 1) * hr] = value.astype(LOW)

    def fin_owner(tile):
        n = array(tile, 0)
        return 2 * tile + jnp.where((n == 1) | (n == 2), 1, 0), n // 2

    def fin_copy(tile):
        owner, i = fin_owner(tile)
        return remote(fin.at[tile], kv_got.at[z, i], fin_send.at[tile], fin_recv.at[z, i], owner)

    def fin_sends(tile):
        owner, i = fin_owner(tile)

        @pl.when(owner == me)
        def _():
            kv_got[z, i] = fin[tile]

        @pl.when(owner != me)
        def _():
            fin_copy(tile).start()

    def dq_sends(tile):
        for u in range(2):
            n = 2 * tile + u

            @pl.when(n == me)
            def _():
                dq_got[z, x] = dq_stage[n]

            @pl.when(n != me)
            def _():
                dq_copy(n).start()

    def x_on(r):
        return x_copy(
            x_all.at[lax.rem(column + 2 * r, wide)], lax.rem(column + 2 * r, wide), twin, xf_send.at[r]
        )

    @pl.loop(0, tiles // 2)
    def _(j):
        pair_wait(j)
        group(True, j)

        @pl.when(lax.rem(j, 2) == 1)
        def _():
            second_on(2 + j // 2)

    for plane in (partner, nz - 1 - partner):
        for c in range(nx):
            q_wait(at(plane, near(0, c)[1]))

    @pl.loop(0, tiles // 2)
    def _(j):
        group(False, j)

    @pl.loop(0, tiles // 2)
    def _(t):
        stat_copy(t).start()

    @pl.loop(tiles // 2, tiles)
    def _(j):
        pair_wait(j)

        odd = lax.rem(tiles - 1 - j, 2)

        @pl.when(odd == 1)
        def _():
            scores(j, (j, True), (j + 1, False))

        @pl.when(odd == 0)
        def _():
            scores(j, (j, True))

        @pl.loop(0, (tiles - 1 - j) // 2)
        def _(n):
            t = j + 1 + odd + 2 * n
            scores(j, (t, False), (t + 1, False))

        @pl.when(j < tiles - 1)
        def _():
            stat_copy(j).start()

    for r in range(1, wide // 2):
        source = lax.rem(column + 2 * r, wide)
        pltpu.make_async_remote_copy(
            src_ref=x_all.at[source], dst_ref=x_all.at[source], send_sem=xf_send.at[r],
            recv_sem=x_recv.at[source], device_id={"tp": twin},
        ).wait_recv()
        x_on(r).start()
    stat_copy(tiles - 1).start()

    middle, low_tiles = tiles // 4, tiles // 4
    upper = tiles // 2

    def step(s, carry):
        last = middle + upper
        t = jnp.where(
            s < middle, upper - 1 - s, jnp.where(s < last, tiles - 1 + middle - s, last + low_tiles - 1 - s)
        )
        sent_tile = tiles - 1 + middle - s

        def stage(lag, work, begin=upper):
            tile = sent_tile + lag
            pl.when((tile >= begin) & (tile < tiles))(lambda: work(tile))

        stage(4, second_sends)
        backward(t)
        dq_sends(t)
        stage(0, first_sends)
        stage(3, add_on_way)
        return carry

    lax.fori_loop(0, tiles, step, 0)
    for tile in range(upper - 1, low_tiles - 1, -1):
        stage_parts(tile)
    second_sends(5)
    for tile in range(upper - 1, -1, -1):
        first_sends(tile)
    add_on_way(4)
    add_on_way(3)
    second_sends(4)
    add_on_way(2)
    second_sends(3)
    add_on_way(1)
    second_sends(2)
    add_on_way(0)
    second_sends(1)
    reduce(7)
    second_sends(0)
    fin_sends(7)

    for r in range(nz):
        for c in range(nx):
            if (r, c) != (0, 0):
                zs, xs = near(r, c)
                arrived(dq_got.at[zs, xs], dq_recv.at[at(zs, xs)])
    for h in range(heads):
        for n in range(nx):
            value = dq_got[h * halves, n].astype(jnp.float32)
            for m in range(1, halves):
                value = value + dq_got[h * halves + m, n].astype(jnp.float32)
            low[n * sub : (n + 1) * sub, h * HEAD : (h + 1) * HEAD] = value.astype(LOW)
    low_copy = pltpu.make_async_copy(low, low_out, out_sem.at[0])
    for r in range(wide // 2):
        source = lax.rem(twin + 2 * r, wide)
        pltpu.make_async_remote_copy(
            src_ref=x_all.at[source], dst_ref=x_all.at[source], send_sem=x_send.at[0],
            recv_sem=x_recv.at[source], device_id={"tp": twin},
        ).wait_recv()

    def term(c):
        begin = c * span
        xs = x_all[begin // x_width, :, pl.ds(pl.multiple_of(lax.rem(begin, x_width), span), span)]
        return lax.dot_general(xs, low[...], (((0,), (0,)), ((), ())), preferred_element_type=jnp.float32)

    waiting = []

    def flush():
        for copy in waiting:
            go(copy)
        waiting.clear()

    between = {
        2: (lambda: reduce(6),),
        5: (lambda: fin_sends(6), lambda: reduce(5)),
        8: (lambda: fin_sends(5), lambda: reduce(4)),
        11: (lambda: fin_sends(4), lambda: reduce(3)),
        14: (lambda: fin_sends(3),),
    }
    order = [(r, c) for r in range(1, nz) for c in range(1, nx)]
    order += [(0, c) for c in range(1, nx)] + [(r, 0) for r in range(1, nz)] + [(0, 0)]
    for count, (r, c) in enumerate(order):
        for work in between.get(count, ()):
            work()
        zt, xt = near(r, c)
        value = term(at(zt, xt))
        fresh = []
        if c:
            wa_stage[r, c] = value[:part_rows].astype(LOW)
            fresh.append(
                remote(wa_stage.at[r, c], wa_red.at[x, zt], wa_send.at[r, c], wa_recv.at[x, zt], at(z, xt))
            )
        else:
            wa_own[r] = value[:part_rows]
        if r:
            wb_stage[r, c] = value[part_rows:].astype(LOW)
            fresh.append(
                remote(wb_stage.at[r, c], wb_red.at[z, xt], wb_send.at[r, c], wb_recv.at[z, xt], at(zt, x))
            )
        else:
            wb_own[c] = value[part_rows:]
        flush()
        waiting.extend(fresh)
    flush()
    low_copy.start()

    @pl.loop(0, 3)
    def _(n):
        reduce(2 - n)

        @pl.when(n > 0)
        def _():
            fin_sends(3 - n)


    for n in list(range(1, nz)) + [0]:
        if n == 2:
            fin_sends(0)
        zt = near(n, 0)[0]
        value = wa_own[n]
        for c in range(1, nx):
            xs = near(0, c)[1]
            arrived(wa_red.at[xs, zt], wa_recv.at[xs, zt])
            value = value + wa_red[xs, zt].astype(jnp.float32)
        fresh = []
        if n:
            wa_fin[n] = value.astype(LOW)
            fresh.append(remote(wa_fin.at[n], wa_got.at[z], wa_fsend.at[n], wa_frecv.at[z], at(zt, x)))
        else:
            w_sum[:part_rows] = value
        xt = near(0, n)[1]
        value = wb_own[n]
        for r in range(1, nz):
            zs = near(r, 0)[0]
            arrived(wb_red.at[zs, xt], wb_recv.at[zs, xt])
            value = value + wb_red[zs, xt].astype(jnp.float32)
        if n:
            wb_fin[n] = value.astype(LOW)
            fresh.append(remote(wb_fin.at[n], wb_got.at[x], wb_fsend.at[n], wb_frecv.at[x], at(z, xt)))
        else:
            w_sum[part_rows:] = value
        flush()
        waiting.extend(fresh)
    flush()

    my_tile = me // 2
    for r in range(nz):
        zs = near(r, 0)[0]
        for i in range(2):
            if r == 0:
                owner, mine = fin_owner(my_tile)

                @pl.when(jnp.logical_not((owner == me) & (mine == i)))
                def _():
                    arrived(kv_got.at[zs, i], fin_recv.at[zs, i])
            else:
                arrived(kv_got.at[zs, i], fin_recv.at[zs, i])
    kv_copy = pltpu.make_async_copy(kv_got, kv_out, out_sem.at[1])
    kv_copy.start()
    for n in range(1, nz):
        zs = near(n, 0)[0]
        arrived(wa_got.at[zs], wa_frecv.at[zs])
        w_sum[:part_rows] += wa_got[zs].astype(jnp.float32)
        xs = near(0, n)[1]
        arrived(wb_got.at[xs], wb_frecv.at[xs])
        w_sum[part_rows:] += wb_got[xs].astype(jnp.float32)

    w_copy = pltpu.make_async_copy(w_sum, w_out, out_sem.at[2])
    w_copy.start()
    low_copy.wait()
    kv_copy.wait()
    for copy in sent:
        copy.wait_send()
    for r in range(1, wide // 2):
        x_on(r).wait_send()

    @pl.loop(0, nz)
    def _(p):
        for i in range(2):
            for c in (1, nx - 1):
                round_copy(p, c, i).wait_send()
            onward_copy(p, i).wait_send()

    @pl.loop(0, tiles)
    def _(t):
        stat_copy(t).wait_send()

    @pl.loop(0, blocks)
    def _(n):
        @pl.when(n != me)
        def _():
            dq_copy(n).wait_send()

    @pl.loop(0, tiles)
    def _(tile):
        for way in range(2):
            opposite_copy(tile, way).wait_send()
            for side in range(2):
                near_copy(tile, side, way).wait_send()

        @pl.when(fin_owner(tile)[0] != me)
        def _():
            fin_copy(tile).wait_send()

    w_copy.wait()


def attention(blocks, wide, q, g, k, v, logits, x):
    rows, cols = k.shape
    heads = cols // HEAD
    nx = NX
    nz = blocks // nx
    halves = nz // heads
    hk = rows // halves
    sub = rows // nx
    tiles = blocks // 2
    anywhere = pl.BlockSpec(memory_space=pl.ANY)
    f32 = jnp.float32
    dma = pltpu.SemaphoreType.DMA
    span = x.shape[1] * wide // blocks
    part = span * 5 // 8
    rest = span - part
    return pl.pallas_call(
        lambda *refs: kernel_body(heads, wide, *refs),
        out_shape=(
            jax.ShapeDtypeStruct((rows, cols), LOW),
            jax.ShapeDtypeStruct((nz, 2, hk, HEAD), LOW),
            jax.ShapeDtypeStruct((span, cols), f32),
        ),
        in_specs=[anywhere] * 6,
        out_specs=(anywhere,) * 3,
        scratch_shapes=[
            pltpu.VMEM((rows, cols), LOW),
            pltpu.VMEM((rows, cols), LOW),
            pltpu.VMEM((rows, cols), LOW),
            pltpu.VMEM((rows, cols), LOW),
            pltpu.VMEM((heads, rows), f32),
            pltpu.VMEM((heads, 8, HEAD), f32),
            pltpu.VMEM((span, cols), f32),
            pltpu.VMEM((blocks, 2, hk, HEAD), LOW),
            pltpu.VMEM((blocks, 2, sub, HEAD), LOW),
            pltpu.VMEM((blocks, 8, HEAD), f32),
            pltpu.VMEM((tiles, HEAD, 2 * hk), LOW),
            pltpu.VMEM((blocks, hk, HEAD), f32),
            pltpu.VMEM((tiles * (tiles + 1) // 2, 2 * hk, 2 * sub), f32),
            pltpu.VMEM((tiles * (tiles + 1) // 2, 8, 2 * sub), f32),
            pltpu.VMEM((2, tiles, 2 * hk, HEAD), f32),
            pltpu.VMEM((HEAD, 2 * sub), f32),
            pltpu.VMEM((tiles, 8, 2 * sub), f32),
            pltpu.VMEM((tiles, 8, 2 * sub), f32),
            pltpu.VMEM((blocks, sub, HEAD), LOW),
            pltpu.VMEM((tiles, nx, hk, HEAD), LOW),
            pltpu.VMEM((tiles, 2, hk // 2, HEAD), LOW),
            pltpu.VMEM((tiles, 2, 2, hk // 2, HEAD), LOW),
            pltpu.VMEM((tiles, hk, HEAD), LOW),
            pltpu.VMEM((nz, nx, sub, HEAD), LOW),
            pltpu.VMEM((nz, 2, hk, HEAD), LOW),
            pltpu.VMEM((wide, rows, x.shape[1]), LOW),
            pltpu.VMEM((rows, cols), LOW),
            pltpu.VMEM((nz, nx, part, cols), LOW),
            pltpu.VMEM((nz, nx, rest, cols), LOW),
            pltpu.VMEM((nx, nz, part, cols), LOW),
            pltpu.VMEM((nz, nx, rest, cols), LOW),
            pltpu.VMEM((nz, part, cols), f32),
            pltpu.VMEM((nx, rest, cols), f32),
            pltpu.VMEM((nz, part, cols), LOW),
            pltpu.VMEM((nx, rest, cols), LOW),
            pltpu.VMEM((nz, part, cols), LOW),
            pltpu.VMEM((nx, rest, cols), LOW),
            dma((6,)), dma((3,)),
            dma((blocks, 2)), dma((nz, 2, 2)), dma((nz, 2)), dma((nz, 2)), dma((blocks, 2)), dma((heads, nx, 2)),
            dma((heads, nx, 2)), dma((nz, nx)), dma((blocks,)), dma((6,)),
            dma((tiles,)), dma((tiles,)), dma((blocks,)), dma((blocks,)), dma((tiles, nx, 2)), dma((tiles, 2)),
            dma((tiles, 2, 2)), dma((tiles,)), dma((nz, 2)),
            dma((wide // 2,)), dma((wide // 2,)), dma((wide,)),
            dma((nz, nx)), dma((nz, nx)), dma((nx, nz)), dma((nz, nx)),
            dma((nz,)), dma((nx,)), dma((nz,)), dma((nx,)),
        ],
        compiler_params=pltpu.CompilerParams(
            vmem_limit_bytes=62 * 1024 * 1024, collective_id=0, has_side_effects=True
        ),
        cost_estimate=pl.CostEstimate(
            flops=10 * blocks * blocks * rows * sub * HEAD, bytes_accessed=1 << 22, transcendentals=0
        ),
        name="attention",
    )(q, g, k, v, logits, x)


def finish_body(
    heads, low_hbm, kv_hbm, w_hbm, dq_out, dk_out, dv_out, w_out, low, kv, w, dq, dk, dv, in_sem, out_sem
):
    halves = kv.shape[0] // heads
    hk = kv.shape[2]
    loads = [
        pltpu.make_async_copy(src, dst, in_sem.at[n])
        for n, (src, dst) in enumerate(((low_hbm, low), (kv_hbm, kv), (w_hbm, w)))
    ]
    for copy in loads:
        copy.start()
    stores = [
        pltpu.make_async_copy(src, dst, out_sem.at[n])
        for n, (src, dst) in enumerate(((dq, dq_out), (dk, dk_out), (dv, dv_out), (w, w_out)))
    ]
    loads[0].wait()
    dq[...] = low[...].astype(jnp.float32)
    stores[0].start()
    loads[1].wait()
    for i, grad in enumerate((dk, dv)):
        for h in range(heads):
            for m in range(halves):
                grad[m * hk : (m + 1) * hk, h * HEAD : (h + 1) * HEAD] = kv[h * halves + m, i].astype(jnp.float32)
        stores[1 + i].start()
    loads[2].wait()
    stores[3].start()
    for copy in stores:
        copy.wait()


def finish(heads, low, kv, w):
    anywhere = pl.BlockSpec(memory_space=pl.ANY)
    f32 = jnp.float32
    grad = jax.ShapeDtypeStruct(low.shape, f32)
    return pl.pallas_call(
        lambda *refs: finish_body(heads, *refs),
        out_shape=(grad, grad, grad, jax.ShapeDtypeStruct(w.shape, f32)),
        in_specs=[anywhere] * 3,
        out_specs=(anywhere,) * 4,
        scratch_shapes=[
            pltpu.VMEM(low.shape, LOW), pltpu.VMEM(kv.shape, LOW), pltpu.VMEM(w.shape, f32),
            pltpu.VMEM(low.shape, f32), pltpu.VMEM(low.shape, f32), pltpu.VMEM(low.shape, f32),
            pltpu.SemaphoreType.DMA((3,)), pltpu.SemaphoreType.DMA((4,)),
        ],
        compiler_params=pltpu.CompilerParams(vmem_limit_bytes=62 * 1024 * 1024),
        name="finish",
    )(low, kv, w)


def local(queries, keys, values, forget_logits, layer_input, out_grad):
    heads = queries.shape[1] // HEAD
    blocks = lax.axis_size("sp")
    wide = lax.axis_size("tp")
    pieces = attention(blocks, wide, queries, out_grad, keys, values, forget_logits.T, layer_input)
    return finish(heads, *pieces)


def solution(mesh):
    spec = P("sp", "tp")
    return jax.shard_map(
        local, mesh=mesh, in_specs=(spec,) * 6, out_specs=(spec,) * 4, check_vma=False
    )
```
